512 devices in a mesh: sp: 32 (over z, x), tp: 16 (over y, core).
Axes of the slice: x: 4, y: 8, z: 8, core: 2. Of those that a mesh axis runs over, the one named last changes fastest.
Arguments:
- expert_input: bfloat16 [4096, 2048], P('sp'), may hold values from -6 to 6
- cotangent: bfloat16 [4096, 2048], P('sp'), may hold values from -6 to 6
- routes: int32 [4096, 2], P('sp'), may hold values from 0 to 15, all different within a row; in each aligned block of 128 rows (0 to 127, 128 to 255, ...) at most 20 rows name the same one
- route_weight: float32 [4096, 2], P('sp'), may hold values from 0.1 to 1
- gate_weight: bfloat16 [32, 2048, 2048], P('sp', None, 'tp'), may hold values from -0.125 to 0.125
- up_weight: bfloat16 [32, 2048, 2048], P('sp', None, 'tp'), may hold values from -0.125 to 0.125
- down_weight: bfloat16 [32, 2048, 2048], P('sp', 'tp'), may hold values from -0.09375 to 0.09375
- out_weight: bfloat16 [2048, 2048], P(None, 'tp'), may hold values from -0.125 to 0.125
- queries: bfloat16 [4096, 16, 64], P('sp', 'tp'), may hold values from -6 to 6
- key_vectors: bfloat16 [4096, 16, 64], P('sp', 'tp'), may hold values from -6 to 6
- value_rows: bfloat16 [4096, 16, 128], P('sp', 'tp'), may hold values from -6 to 6
- log_decay: float32 [4096, 16, 64], P('sp', 'tp'), may hold values from -2 to 0
- start_state: float32 [32, 16, 64, 128], P('sp', 'tp'), may hold values from -24 to 24
Outputs:
- gate_grad: bfloat16 [32, 2048, 2048], P('sp', None, 'tp')
- up_grad: bfloat16 [32, 2048, 2048], P('sp', None, 'tp')
- down_grad: bfloat16 [32, 2048, 2048], P('sp', 'tp')
- out_grad: float32 [2048, 2048], P('sp', 'tp')
- query_grad: bfloat16 [4096, 16, 64], P('sp', 'tp')
- key_grad: bfloat16 [4096, 16, 64], P('sp', 'tp')
- value_grad: bfloat16 [4096, 16, 128], P('sp', 'tp')
- decay_grad: float32 [4096, 16, 64], P('sp', 'tp')
The draws below stay inside these ranges and needn't reach their ends.
Inputs may be any that keep to these rules, and one draw needn't show every extreme that they name: `routes`: in each aligned block of 128 rows, no number is named by more than 20 rows, and in some blocks one number is named by exactly 20 rows.
All inputs are finite; a program needn't handle non-finite values.
Results may differ from the reference program's by a relative error of at most 0.02.
Values may be sent and summed in bfloat16 or wider, within the bound.
No kernel may reach another device: no remote copies, remote signals or barrier semaphores. Data moves between devices by JAX's collectives and lax.ppermute only.
A program may use at most 64 MiB of HBM per device.

```python
import math
import jax
import jax.numpy as jnp
import numpy as np
from jax import lax

D = 2048
FF = 4096
HEADS = 16
DK = 64
DV = 128
TOPK = 2
TOK_DEV = 128
EXPERTS = 16
CAP = 20
FFD = 128
SPANS = 32
SEQUENCE_TOKENS = 4096
N_TP = 16


def draw_log_decay(key, part):
    every_key_row = jax.random.split(jax.random.fold_in(key, 17), 7)
    slow_share = 0.5
    slow_mask = jax.random.bernoulli(every_key_row[0], slow_share, (HEADS, DK))
    slow_rate = jax.random.uniform(every_key_row[1], (HEADS, DK), jnp.float32, 0.3, 1.0) / SEQUENCE_TOKENS
    fast_rate = jnp.exp(jax.random.uniform(every_key_row[2], (HEADS, DK), jnp.float32, math.log(0.02), math.log(0.05)))
    channel_decay_rate = jnp.where(slow_mask, slow_rate, fast_rate)
    span_factor = jnp.exp(jax.random.uniform(every_key_row[3], (SEQUENCE_TOKENS // TOK_DEV,), jnp.float32, -math.log(2.0), math.log(2.0)))
    position_weighting = jnp.repeat(span_factor, TOK_DEV)
    random_jitter_factor = jnp.exp(0.4 * jnp.clip(jax.random.normal(every_key_row[4], (SEQUENCE_TOKENS, HEADS, DK), jnp.float32), -3.0, 3.0))
    spike_location = jax.random.randint(every_key_row[5], (3,), 0, SEQUENCE_TOKENS)
    spike_penalty = jax.random.uniform(every_key_row[6], (3,), jnp.float32, 0.2, 0.4)
    spike_hit_count = (jnp.arange(SEQUENCE_TOKENS)[:, None] == spike_location[None, :]).astype(jnp.float32)
    spike_logarithm = jnp.sum(spike_hit_count * jnp.log(1.0 - spike_penalty)[None, :], axis=1)
    return -channel_decay_rate[None] * position_weighting[:, None, None] * random_jitter_factor + spike_logarithm[:, None, None]


def spiked(values, own_key, source, target, shards_of, factor):
    def block_of(position):
        return (jnp.arange(values.shape[position]) // (values.shape[position] // shards_of)).reshape((-1,) + (1,) * (values.ndim - 1 - position))

    one_side = jax.random.permutation(own_key, shards_of)[block_of(target)]
    other_side = (block_of(target) + shards_of // 2) % shards_of
    return jnp.where((block_of(source) == one_side) | (block_of(source) == other_side), factor * values, values)


def block_scale(own_key, dims, cuts, least, largest):
    loudness, own = 1.0, jax.random.fold_in(own_key, 6)
    for position, blocks in cuts:
        draws = jnp.exp(jax.random.uniform(jax.random.fold_in(own, position), (blocks,), jnp.float32, least / len(cuts), largest / len(cuts)))
        loudness = loudness * jnp.repeat(draws, dims[position] // blocks).reshape([-1 if axis == position else 1 for axis in range(len(dims))])
    return loudness


def shared_out(own_key, own, number, rows, amount, top, bound, slope):
    ranking = jax.random.permutation(own_key, amount)
    packed, usual = portions_of(amount, rows * top, bound, slope, True), portions_of(amount, rows * top, bound, slope, False)
    places = jnp.arange(amount)

    def named(lengths, rotation):
        used = int((lengths > 0).sum())
        fixed = max(1, used // 4)
        moved = fixed + (places - fixed + rotation * (used - fixed)) % max(1, amount - fixed)
        return jnp.zeros((amount,), jnp.int32).at[ranking[jnp.where(places < fixed, places, moved)]].set(jnp.asarray(lengths, jnp.int32))

    lengths = jnp.where(number % 4 == 0, named(packed, number // 4), named(usual, number - number // 4 - 1))
    mixed = jax.random.permutation(jax.random.fold_in(own, 3), amount)
    donor, receiver = mixed[0:amount // 2 * 2:2], mixed[1:amount // 2 * 2:2]
    margin = jnp.minimum(lengths[donor] - 1, bound - lengths[receiver]) // 2
    margin = jnp.where((donor == ranking[0]) | (receiver == ranking[0]) | (lengths[receiver] == 0), 0, jnp.maximum(margin, 0))
    moved = jax.random.randint(jax.random.fold_in(own, 4), (amount // 2,), 0, 1 << 20) % (margin + 1)
    lengths = lengths.at[donor].add(-moved).at[receiver].add(moved)
    labels = jnp.searchsorted(jnp.cumsum(lengths), jnp.arange(rows * top), side="right").astype(jnp.int32)
    grid = labels.reshape(top, rows).T
    grid = grid[jax.random.permutation(jax.random.fold_in(own, 1), rows)]
    rotation = jax.random.randint(jax.random.fold_in(own, 2), (rows, 1), 0, top)
    return jnp.take_along_axis(grid, (jnp.arange(top)[None, :] + rotation) % top, axis=1)


def portions_of(count, total, bound, slope, full):
    weights = [(1 << 20) // math.isqrt(grade ** slope) + 1 for grade in range(1, count + 1)]
    largest = bound if full else min(bound, max(-(-total // count), total * weights[0] // sum(weights)))
    least = 1 if total - largest >= count - 1 else 0
    counts, spare = [largest] + [least] * (count - 1), total - largest - least * (count - 1)
    while spare > 0:
        movable = [i for i in range(1, count) if counts[i] < largest] or [i for i in range(1, count) if counts[i] < bound]
        mass, budget = sum([weights[i] for i in movable]), spare
        for i in movable:
            addition = min(bound - counts[i], max(1, budget * weights[i] // mass), spare)
            counts[i] = counts[i] + addition
            spare = spare - addition
    return np.array(counts)


def centred(own_key, shape, spread, most, cuts=(), held_as=jnp.bfloat16):
    result = spread * jax.random.normal(own_key, shape, jnp.float32)
    if cuts:
        result = result * block_scale(own_key, shape, cuts, -0.22, 0.18)
    return jnp.clip(result, -most, most).astype(held_as)


def noise_with(key, shape, scale, most, cuts, heavy, held_as=jnp.bfloat16):
    result = scale * jax.random.normal(key, shape, jnp.float32)
    if cuts:
        result = result * block_scale(key, shape, cuts, -0.22, 0.18)
    return jnp.clip(spiked(result, jax.random.fold_in(key, 3), *heavy), -most, most).astype(held_as)


def setup_inputs(seed: int = 0) -> dict:
    arg_keys = jax.random.split(jax.random.key(seed), 14)
    expert_input = centred(arg_keys[0], (SEQUENCE_TOKENS, D), 1.0, 6.0, ((0, 32),))
    cotangent = noise_with(arg_keys[1], (SEQUENCE_TOKENS, D), 1.0, 6.0, ((0, 32),), (0, 1, 32, 2.75))
    routes_keys = jax.random.split(jax.random.fold_in(arg_keys[2], 1), SEQUENCE_TOKENS // TOK_DEV)
    routes_turns = jax.random.permutation(jax.random.fold_in(arg_keys[2], 3), SEQUENCE_TOKENS // TOK_DEV)
    routes = jax.vmap(lambda own, number: shared_out(jax.random.fold_in(arg_keys[2], 2), own, number, TOK_DEV, EXPERTS, TOPK, CAP, 1))(routes_keys, routes_turns).reshape((SEQUENCE_TOKENS, TOPK))
    route_weight = jnp.clip(0.1 + 0.9 * jax.random.uniform(arg_keys[3], (SEQUENCE_TOKENS, TOPK), jnp.float32) ** block_scale(arg_keys[3], (SEQUENCE_TOKENS, TOPK), ((0, 32),), -0.2, 0.2), 0.1, 1.0)
    gate_weight = centred(arg_keys[4], (2 * EXPERTS, D, FF // 2), D ** -0.5, 0.125, ((0, 32), (2, 16)))
    up_weight = centred(arg_keys[5], (2 * EXPERTS, D, FF // 2), D ** -0.5, 0.125, ((0, 32), (2, 16)))
    down_weight = centred(arg_keys[6], (2 * EXPERTS, FF // 2, D), FF ** -0.5, 0.09375, ((0, 32), (1, 16)))
    out_weight = centred(arg_keys[7], (D, HEADS * DV), (HEADS * DV) ** -0.5, 0.125, ((1, 16),))
    queries = centred(arg_keys[8], (SEQUENCE_TOKENS, HEADS, DK), 1.0, 6.0, ((0, 32), (1, 16)))
    key_vectors = centred(arg_keys[9], (SEQUENCE_TOKENS, HEADS, DK), 1.0, 6.0, ((0, 32), (1, 16)))
    value_rows = centred(arg_keys[10], (SEQUENCE_TOKENS, HEADS, DV), 1.0, 6.0, ((0, 32), (1, 16)))
    log_decay = draw_log_decay(jax.random.fold_in(arg_keys[13], 71), 0)
    start_state = centred(arg_keys[12], (SPANS, HEADS, DK, DV), 4.0, 24.0, ((0, 32), (1, 16)), jnp.float32)
    return {"expert_input": expert_input, "cotangent": cotangent, "routes": routes, "route_weight": route_weight, "gate_weight": gate_weight, "up_weight": up_weight, "down_weight": down_weight, "out_weight": out_weight, "queries": queries, "key_vectors": key_vectors, "value_rows": value_rows, "log_decay": log_decay, "start_state": start_state}


EXACT_ARITHMETIC = lax.Precision.HIGHEST


def slot_table(routes_span):
    flat_ids = routes_span.reshape(-1).astype(jnp.int32)
    onehot = (flat_ids[:, None] == jnp.arange(EXPERTS, dtype=jnp.int32)[None, :]).astype(jnp.int32)
    running = jnp.cumsum(onehot, axis=0).astype(jnp.int32)
    slot_rank = jnp.sum((running - 1) * onehot, axis=1).astype(jnp.int32)
    destination = (flat_ids * CAP + slot_rank).astype(jnp.int32)
    source = jnp.full((EXPERTS * CAP,), -1, jnp.int32).at[destination].set(
        jnp.arange(flat_ids.shape[0], dtype=jnp.int32))
    return destination, source


def span_slots(inputs_span, grads_span, weights_span, source):
    present = (source >= 0)[:, None]
    picked = jnp.maximum(source, 0).astype(jnp.int32)
    token_rows = (picked // TOPK).astype(jnp.int32)
    taken_input = jnp.take(inputs_span, token_rows, axis=0)
    taken_input = jnp.where(present, taken_input, jnp.zeros_like(taken_input))
    picked_weight = jnp.take(weights_span.reshape(-1), picked)
    taken_grad = jnp.take(grads_span, token_rows, axis=0).astype(jnp.float32) * picked_weight[:, None]
    taken_grad = jnp.where(present, taken_grad, 0.0).astype(jnp.bfloat16)
    return taken_input, taken_grad


def expert_pass(inputs):
    rows_in, rows_grad, gate_halves, up_halves, down_halves = inputs
    w_gate = gate_halves.transpose(1, 0, 2).reshape(D, FF)
    w_up = up_halves.transpose(1, 0, 2).reshape(D, FF)
    w_down = down_halves.reshape(FF, D)
    pre_gate = jnp.dot(rows_in, w_gate, preferred_element_type=jnp.float32)
    pre_up = jnp.dot(rows_in, w_up, preferred_element_type=jnp.float32)
    sigmoid_gate = jax.nn.sigmoid(pre_gate)
    activated = pre_gate * sigmoid_gate
    hidden = (activated * pre_up).astype(jnp.bfloat16)
    down_sum = lax.dot_general(hidden, rows_grad, (((0,), (0,)), ((), ())),
                               preferred_element_type=jnp.float32)
    hidden_grad = lax.dot_general(rows_grad, w_down, (((1,), (1,)), ((), ())),
                                  preferred_element_type=jnp.float32)
    gate_delta = (hidden_grad * pre_up * sigmoid_gate * (1.0 + pre_gate * (1.0 - sigmoid_gate))).astype(jnp.bfloat16)
    up_delta = (hidden_grad * activated).astype(jnp.bfloat16)
    gate_sum = lax.dot_general(rows_in, gate_delta, (((0,), (0,)), ((), ())),
                               preferred_element_type=jnp.float32)
    up_sum = lax.dot_general(rows_in, up_delta, (((0,), (0,)), ((), ())),
                             preferred_element_type=jnp.float32)
    row_count = rows_in.shape[0]
    gate_blocks = gate_delta.astype(jnp.float32).reshape(row_count, 2 * N_TP, FFD)
    up_blocks = up_delta.astype(jnp.float32).reshape(row_count, 2 * N_TP, FFD)
    gate_table = w_gate.astype(jnp.float32).reshape(D, 2 * N_TP, FFD)
    up_table = w_up.astype(jnp.float32).reshape(D, 2 * N_TP, FFD)
    block_terms = (jnp.einsum('rbf,dbf->brd', gate_blocks, gate_table, precision=EXACT_ARITHMETIC)
                   + jnp.einsum('rbf,dbf->brd', up_blocks, up_table, precision=EXACT_ARITHMETIC))
    block_round = lax.optimization_barrier(block_terms.astype(jnp.bfloat16)).astype(jnp.float32)
    half_sums = jnp.sum(block_round.reshape(2, N_TP, row_count, D), axis=1)
    half_round = lax.optimization_barrier(half_sums.astype(jnp.bfloat16)).astype(jnp.float32)
    pair_sum = half_round[0] + half_round[1]
    return (down_sum.astype(jnp.bfloat16), gate_sum.astype(jnp.bfloat16),
            up_sum.astype(jnp.bfloat16), pair_sum)


def reference(expert_input, cotangent, routes, route_weight, gate_weight, up_weight, down_weight,
              out_weight, queries, key_vectors, value_rows, log_decay, start_state):
    routes_span = routes.reshape(SPANS, TOK_DEV, TOPK)
    destination, source = jax.vmap(slot_table)(routes_span)
    taken_input, taken_grad = jax.vmap(span_slots)(
        expert_input.reshape(SPANS, TOK_DEV, D), cotangent.reshape(SPANS, TOK_DEV, D),
        route_weight.reshape(SPANS, TOK_DEV, TOPK), source)
    rows_in = taken_input.reshape(SPANS, EXPERTS, CAP, D).transpose(1, 0, 2, 3).reshape(EXPERTS, SPANS * CAP, D)
    rows_grad = taken_grad.reshape(SPANS, EXPERTS, CAP, D).transpose(1, 0, 2, 3).reshape(EXPERTS, SPANS * CAP, D)
    down_sum, gate_sum, up_sum, pair_sum = lax.map(
        expert_pass,
        (rows_in, rows_grad, gate_weight.reshape(EXPERTS, 2, D, FF // 2),
         up_weight.reshape(EXPERTS, 2, D, FF // 2), down_weight.reshape(EXPERTS, 2, FF // 2, D)))
    gate_grad = gate_sum.reshape(EXPERTS, D, 2, FF // 2).transpose(0, 2, 1, 3).reshape(2 * EXPERTS, D, FF // 2)
    up_grad = up_sum.reshape(EXPERTS, D, 2, FF // 2).transpose(0, 2, 1, 3).reshape(2 * EXPERTS, D, FF // 2)
    down_grad = down_sum.reshape(2 * EXPERTS, FF // 2, D)
    by_span = pair_sum.reshape(EXPERTS, SPANS, CAP, D).transpose(1, 0, 2, 3).reshape(SPANS, EXPERTS * CAP, D)
    per_pair = jax.vmap(lambda table, where_to: jnp.take(table, where_to, axis=0))(by_span, destination)
    moe_grad = jnp.sum(per_pair.reshape(SEQUENCE_TOKENS, TOPK, D), axis=1)
    total_grad = (cotangent.astype(jnp.float32) + moe_grad).astype(jnp.bfloat16)
    head_grad = jnp.dot(total_grad, out_weight, preferred_element_type=jnp.float32).astype(jnp.bfloat16)

    query_scale = DK ** -0.5
    q_all = queries.astype(jnp.float32).reshape(SPANS, TOK_DEV, HEADS, DK)
    k_all = key_vectors.astype(jnp.float32).reshape(SPANS, TOK_DEV, HEADS, DK)
    v_all = value_rows.astype(jnp.float32).reshape(SPANS, TOK_DEV, HEADS, DV)
    g_all = log_decay.reshape(SPANS, TOK_DEV, HEADS, DK)
    d_all = head_grad.astype(jnp.float32).reshape(SPANS, TOK_DEV, HEADS, DV)

    def span_forward(inputs):
        q_span, k_span, v_span, g_span, d_span, state_first = inputs

        def advance(current_state, item):
            query_current, key_current, value_current, g_now, decay_current = item
            following_state = jnp.exp(g_now)[:, :, None] * current_state + key_current[:, :, None] * value_current[:, None, :]
            mixed_current = jnp.einsum('ti,tir->tr', query_current * query_scale, following_state, precision=EXACT_ARITHMETIC)
            query_present_step = query_scale * jnp.einsum('dt,dst->ds', decay_current, following_state, precision=EXACT_ARITHMETIC)
            return following_state, (mixed_current, query_present_step)

        state_last, (mixed_span, query_span) = lax.scan(advance, state_first, (q_span, k_span, v_span, g_span, d_span))
        return mixed_span, query_span, state_last

    mixed_all, query_raw, state_ends = lax.map(span_forward, (q_all, k_all, v_all, g_all, d_all, start_state))

    def span_backward(carried_state, inputs):
        def retreat(later, item):
            query_current, key_current, value_current, g_now, decay_current = item
            adjoint_vector = (query_current * query_scale)[:, :, None] * decay_current[:, None, :] + later
            key_present_step = jnp.einsum('nfm,nm->nf', adjoint_vector, value_current, precision=EXACT_ARITHMETIC)
            value_present_step = jnp.einsum('ti,tir->tr', key_current, adjoint_vector, precision=EXACT_ARITHMETIC)
            return jnp.exp(g_now)[:, :, None] * adjoint_vector, (key_present_step, value_present_step)

        carried_next, (key_span, value_span) = lax.scan(retreat, carried_state, inputs, reverse=True)
        return carried_next, (key_span, value_span, carried_state)

    zero_state = jnp.zeros((HEADS, DK, DV), jnp.float32)
    _, (key_raw, value_raw, incoming) = lax.scan(span_backward, zero_state, (q_all, k_all, v_all, g_all, d_all),
                                                 reverse=True)
    local_terms = q_all * query_raw - k_all * key_raw
    reversed_sum = jnp.flip(jnp.cumsum(jnp.flip(local_terms, 1), axis=1), 1)
    cross_term = jnp.sum(state_ends * incoming, axis=-1)
    decay_grad = (reversed_sum + cross_term[:, None]).reshape(SEQUENCE_TOKENS, HEADS, DK)
    mixed = mixed_all.astype(jnp.bfloat16).reshape(SEQUENCE_TOKENS, HEADS * DV)
    out_grad = lax.dot_general(total_grad, mixed, (((0,), (0,)), ((), ())), preferred_element_type=jnp.float32)
    return (gate_grad, up_grad, down_grad, out_grad,
            query_raw.reshape(SEQUENCE_TOKENS, HEADS, DK).astype(jnp.bfloat16),
            key_raw.reshape(SEQUENCE_TOKENS, HEADS, DK).astype(jnp.bfloat16),
            value_raw.reshape(SEQUENCE_TOKENS, HEADS, DV).astype(jnp.bfloat16),
            decay_grad)
```

```python
from functools import partial

import jax
import jax.numpy as jnp
from jax import lax
from jax.experimental import pallas as pl
from jax.experimental.pallas import tpu as pltpu
from jax.sharding import Mesh
from jax.sharding import PartitionSpec as P

SP = ("z", "x")
TP = ("y", "c")
BF = jnp.bfloat16
F32 = jnp.float32
HI = lax.Precision.HIGHEST
BLOCK = 32
LIMIT = 56 * 1024 * 1024


def dot(a, b, precision=None):
    return lax.dot_general(
        a, b, (((1,), (0,)), ((), ())), precision=precision, preferred_element_type=F32
    )


def dot_nt(a, b, precision=None):
    return lax.dot_general(
        a, b, (((1,), (1,)), ((), ())), precision=precision, preferred_element_type=F32
    )


def dot_tn(a, b, precision=None):
    return lax.dot_general(
        a, b, (((0,), (0,)), ((), ())), precision=precision, preferred_element_type=F32
    )


def iota(shape, dim):
    return lax.broadcasted_iota(jnp.int32, shape, dim)


def params(**kw):
    return pltpu.CompilerParams(vmem_limit_bytes=LIMIT, **kw)


def call(kernel, name, outs, scalars, *args, blocks=None, scratch=(), after=()):
    blocks = blocks or {}
    specs = []
    used, waits = len(args), len(after)

    def body(at, *refs):
        kernel(at, *refs[:used], *refs[used + waits :])

    for n, a in enumerate(args):
        if n in blocks:
            specs.append(pl.BlockSpec(*blocks[n]))
        else:
            specs.append(pl.BlockSpec(a.shape, lambda i, s, nd=a.ndim: (0,) * nd))
    specs += [pl.BlockSpec(memory_space=pl.ANY)] * waits
    out_specs = tuple(pl.BlockSpec(o.shape, lambda i, s, nd=len(o.shape): (0,) * nd) for o in outs)
    return pl.pallas_call(
        body,
        name=name,
        out_shape=outs,
        grid_spec=pltpu.PrefetchScalarGridSpec(
            num_scalar_prefetch=1,
            grid=(1,),
            in_specs=specs,
            out_specs=out_specs,
            scratch_shapes=list(scratch),
        ),
        compiler_params=params(),
    )(scalars, *args, *after)


def sds(shape, dtype):
    return jax.ShapeDtypeStruct(shape, dtype)


def slots_of(routes):
    tokens = routes.shape[1]
    experts = iota((16, tokens), 0)
    r0, r1 = routes[0:1, :], routes[1:2, :]
    one0, one1 = r0 == experts, r1 == experts
    both = jnp.where(one0 | one1, 1.0, 0.0).astype(BF)
    earlier = jnp.where(iota((tokens, tokens), 0) < iota((tokens, tokens), 1), 1.0, 0.0).astype(BF)
    count = dot(both, earlier)
    s0 = jnp.sum(jnp.where(one0, count, 0.0), axis=0, keepdims=True)
    s1 = jnp.sum(jnp.where(one1, count, 0.0), axis=0, keepdims=True)
    return r0.astype(F32), r1.astype(F32), s0, s1


def column(row):
    return jnp.broadcast_to(row, (row.shape[1], row.shape[1])).T


def dispatch_kernel(at, routes_ref, weight_ref, x_ref, y_ref, out_ref):
    tokens = routes_ref.shape[1]
    r0, r1, s0, s1 = slots_of(routes_ref[...])
    key0 = r0 * 32.0 + s0
    key1 = r1 * 32.0 + s1
    y = y_ref[...].astype(F32)
    w = weight_ref[...]
    table = jnp.concatenate(
        [x_ref[...], (column(w[0:1]) * y).astype(BF), (column(w[1:2]) * y).astype(BF)], axis=0
    )
    q = iota((40, tokens), 0)
    is_input = q < 20
    slot = jnp.where(is_input, q, jnp.where(q < 24, q - 4, q - 24)).astype(F32)
    for e in range(out_ref.shape[0] // 2):
        key = slot + 32.0 * e
        m0, m1 = key0 == key, key1 == key
        a = jnp.concatenate(
            [
                jnp.where(is_input & (m0 | m1), 1.0, 0.0).astype(BF),
                jnp.where(is_input, 0.0, jnp.where(m0, 1.0, 0.0)).astype(BF),
                jnp.where(is_input, 0.0, jnp.where(m1, 1.0, 0.0)).astype(BF),
            ],
            axis=1,
        )
        rows = dot(a, table).astype(BF)
        out_ref[2 * e] = rows
        out_ref[2 * e + 1] = rows


def swap_halves(a):
    return jnp.concatenate([a[4:8], a[0:4]], axis=0)


def delta_kernel(at, g_ref, wg_ref, wu_ref, wd_ref, delta_ref, pack_ref, wgu_ref):
    slices, rows, _ = g_ref.shape
    wgu_ref[:, 0:128] = wg_ref[0]
    wgu_ref[:, 128:256] = wu_ref[0]
    low = iota((8, 128), 0) < 4
    zero8 = jnp.zeros((8, 128), F32)

    def step(i, carry):
        at_row = pl.multiple_of(i * 160, 32)
        a = jnp.concatenate([g_ref[t, pl.ds(at_row, 160), :] for t in range(slices)], axis=1)
        gu = dot(a, wgu_ref[...])
        yh = dot_nt(a, wd_ref[0])
        dgs, dus, dhs, pgs, pus = [], [], [], [], []
        mixed = []
        for d in range(4):
            b = 40 * d
            pg, pu = gu[b : b + 24, 0:128], gu[b : b + 24, 128:256]
            hg = jnp.concatenate([yh[b + 24 : b + 40], swap_halves(yh[b + 16 : b + 24])], axis=0)
            s = jax.nn.sigmoid(pg)
            act = pg * s
            hid = act * pu
            gd = hg * pu * s * (1.0 + pg * (1.0 - s))
            ud = hg * act
            dgs += [gd[0:16], jnp.where(low, gd[16:24], 0.0), zero8, zero8]
            dus += [ud[0:16], jnp.where(low, ud[16:24], 0.0), zero8, zero8]
            dhs += [zero8, zero8, jnp.where(low, 0.0, swap_halves(hid[16:24])), hid[0:16]]
            mixed.append((gd, ud))
        for d in (0, 2):
            for n, parts in ((0, pgs), (1, pus)):
                even, odd = mixed[d][n], mixed[d + 1][n]
                parts += [
                    even[0:16],
                    jnp.where(low, even[16:24], swap_halves(odd[16:24])),
                    odd[0:16],
                ]
        delta_ref[pl.ds(at_row, 160), 0:128] = jnp.concatenate(dgs, axis=0).astype(BF)
        delta_ref[pl.ds(at_row, 160), 128:256] = jnp.concatenate(dus, axis=0).astype(BF)
        delta_ref[pl.ds(at_row, 160), 256:384] = jnp.concatenate(dhs, axis=0).astype(BF)
        at_pack = pl.multiple_of(i * 80, 16)
        pack_ref[pl.ds(at_pack, 80), 0:128] = jnp.concatenate(pgs, axis=0).astype(BF)
        pack_ref[pl.ds(at_pack, 80), 128:256] = jnp.concatenate(pus, axis=0).astype(BF)
        return carry

    lax.fori_loop(0, rows // 160, step, 0)


def partial_kernel(at, pack_ref, wg_ref, wu_ref, woth_ref, out_ref):
    core = at[1]
    lhs = jnp.concatenate([pack_ref[core], pack_ref[1 - core]], axis=1)
    for y in range(0, out_ref.shape[0], 2):
        sides = []
        for v in (y, y + 1):
            first = pl.multiple_of((2 * v + core) * 128, 128)
            sides.append(
                jnp.concatenate(
                    [
                        wg_ref[0, pl.ds(first, 128), :],
                        wu_ref[0, pl.ds(first, 128), :],
                        woth_ref[0, v],
                        woth_ref[1, v],
                    ],
                    axis=1,
                )
            )
        o = dot_nt(lhs, jnp.concatenate(sides, axis=0)).astype(BF)
        out_ref[y] = o[:, 0:128]
        out_ref[y + 1] = o[:, 128:256]


def weight_kernel(at, delta_ref, g_ref, gate_ref, up_ref, down_ref, dt_ref):
    rows = delta_ref.shape[0]
    for r in range(0, rows, 128):
        dt_ref[:, r : r + 128] = delta_ref[r : r + 128, :].astype(F32).T.astype(BF)

    def step(p, carry):
        g2 = jnp.concatenate([g_ref[2 * p], g_ref[2 * p + 1]], axis=1)
        o = dot(dt_ref[...], g2)
        first = pl.multiple_of(p * 256, 256)
        gate_ref[0, pl.ds(first, 256), :] = o[0:128].T.astype(BF)
        up_ref[0, pl.ds(first, 256), :] = o[128:256].T.astype(BF)
        down_ref[0, :, pl.ds(first, 256)] = o[256:384].astype(BF)
        return carry

    lax.fori_loop(0, g_ref.shape[0] // 2, step, 0)


def sum_kernel(at, got_ref, out_ref):
    total = got_ref[0].astype(F32)
    for y in range(1, got_ref.shape[0]):
        total = total + got_ref[y].astype(F32)
    for p in range(out_ref.shape[0] // 2):
        b = 40 * p
        out_ref[2 * p] = total[b : b + 24].astype(BF)
        out_ref[2 * p + 1] = jnp.concatenate(
            [total[b + 24 : b + 40], total[b + 16 : b + 24]], axis=0
        ).astype(BF)


def collect_kernel(at, routes_ref, got_ref, cot_ref, out_ref):
    halves = got_ref.shape[0]
    r0, r1, s0, s1 = slots_of(routes_ref[...])
    shift = (at[2] % 2).astype(F32) * 4.0
    cols = halves * 24
    lanes = iota((routes_ref.shape[1], cols), 1).astype(F32)
    hit = None
    for r, s in ((r0, s0), (r1, s1)):
        first = column(r * 48.0 + s + jnp.where(s >= 16.0, shift, 0.0))[:, 0:1]
        match = (lanes == first) | (lanes == first + 24.0)
        hit = match if hit is None else hit | match
    pick = jnp.where(hit, 1.0, 0.0).astype(BF)
    table = got_ref[...].astype(F32).reshape(cols, 128).astype(BF)
    out_ref[...] = (cot_ref[...].astype(F32) + dot(pick, table)).astype(BF)


def block_of(shape):
    return iota(shape, 1) // BLOCK


def mids_of(gc):
    return [gc[:, b + BLOCK // 2 - 1 : b + BLOCK // 2] for b in range(0, gc.shape[1], BLOCK)]


def growth(gc):
    blocks = block_of(gc.shape)
    mid = jnp.zeros(gc.shape, F32)
    for n, m in enumerate(mids_of(gc)):
        mid = jnp.where(blocks == n, m, mid)
    return jnp.exp(gc - mid)


def causal(tokens):
    return iota((tokens, tokens), 1) <= iota((tokens, tokens), 0)


def forward_kernel(at, q_ref, k_ref, v_ref, g_ref, s_ref, mixed_ref, p_ref, last_ref, gc_ref, tot_ref):
    width, tokens = q_ref.shape
    g = g_ref[...]
    before = jnp.where(iota((tokens, tokens), 0) <= iota((tokens, tokens), 1), 1.0, 0.0)
    gc = dot(g, before, HI)
    gc_ref[...] = gc
    q = q_ref[...].astype(F32) * (width**-0.5)
    k = k_ref[...].astype(F32)
    v = v_ref[...].astype(F32)
    s0 = s_ref[0, 0]
    qt = q * growth(gc)
    parts = []
    for n, mid in enumerate(mids_of(gc)):
        whole = dot_tn(qt, k * jnp.exp(jnp.minimum(mid - gc, 40.0)), HI)
        parts.append(whole[n * BLOCK : (n + 1) * BLOCK])
    p = jnp.where(causal(tokens), jnp.concatenate(parts, axis=0), 0.0)
    p_ref[...] = p.astype(BF)
    mixed_ref[...] = (dot_tn(q * jnp.exp(gc), s0, HI) + dot(p, v, HI)).astype(BF)
    end = gc[:, tokens - 1 : tokens]
    last_ref[...] = jnp.exp(end) * s0 + dot(k * jnp.exp(end - gc), v, HI)
    row = dot_nt(jnp.ones((8, tokens), F32), g, HI)
    tot_ref[...] = jnp.zeros(tot_ref.shape, F32)
    for d in range(tot_ref.shape[0]):
        tot_ref[d, :, 0:width] = row


def decay_kernel(at, tot_ref, out_ref):
    spans = tot_ref.shape[0]
    z, x, nx = at[3], at[4], at[5]
    nz = spans // nx
    k = iota((128, spans), 0)
    u = iota((128, spans), 1)
    own = z * nx + x
    low = jnp.where((k >= nx) & (k < 2 * nx), z * nx - 1, own)
    high = jnp.where(k < nx, z * nx + k, jnp.where(k < 2 * nx, z * nx + k - nx, (k - 2 * nx) * nx))
    inside = jnp.where((u > low) & (u < high), 1.0, 0.0)
    sums = dot(inside, tot_ref[:, 0, :], HI)
    kk = iota((128, 128), 0)
    valid = (
        ((kk < nx) & (kk > x))
        | ((kk >= nx) & (kk < 2 * nx))
        | ((kk > 2 * nx + z) & (kk < 2 * nx + nz))
    )
    out_ref[...] = jnp.where(valid, jnp.exp(sums), 0.0).T


def head_kernel(piece, at, tg_ref, w_ref, q_ref, gc_ref, mixed_ref, rows_ref, send_ref):
    slices = tg_ref.shape[0]
    width = q_ref.shape[0]
    nx = send_ref.shape[0]
    tg = jnp.concatenate([tg_ref[t] for t in range(slices)], axis=1)
    rows = dot(tg, w_ref[...]).astype(BF)
    rows_ref[...] = rows
    qe = q_ref[...].astype(F32) * (width**-0.5) * jnp.exp(gc_ref[...])
    carry = dot(qe, rows.astype(F32), HI).astype(BF)
    own = send_ref.shape[1] - width
    for n in range(nx):
        send_ref[n, own : own + width, :] = carry
    mixed = mixed_ref[...]
    for t in range(slices):
        o = dot_tn(tg_ref[t], mixed).astype(BF)
        for r in range(0, 128, piece):
            d = (t * 128 + r) // piece
            send_ref[d % nx, (d // nx) * piece : (d // nx + 1) * piece, :] = o[r : r + piece]


def local_kernel(at, rows_ref, q_ref, k_ref, v_ref, gc_ref, s_ref, p_ref, qraw_ref, qq_ref, kl_ref, vl_ref):
    width, tokens = q_ref.shape
    scale = width**-0.5
    rows = rows_ref[...]
    gc = gc_ref[...]
    q = q_ref[...].astype(F32)
    k = k_ref[...].astype(F32)
    a = jnp.where(causal(tokens), dot_nt(rows, v_ref[...]), 0.0)
    grow = growth(gc)
    qt = q * scale * grow
    blocks = block_of(gc.shape)
    inner = jnp.zeros((width, tokens), F32)
    key_local = jnp.zeros((width, tokens), F32)
    for n, mid in enumerate(mids_of(gc)):
        fall = jnp.exp(jnp.minimum(mid - gc, 40.0))
        inner = jnp.where(blocks == n, dot_nt(k * fall, a, HI), inner)
        key_local = key_local + fall * dot(jnp.where(blocks == n, qt, 0.0), a, HI)
    qraw = scale * (jnp.exp(gc) * dot_nt(s_ref[0, 0], rows.astype(F32), HI) + grow * inner)
    qraw_ref[...] = qraw.astype(BF)
    qq_ref[...] = q * qraw
    kl_ref[...] = key_local
    vl_ref[...] = dot_tn(p_ref[...], rows)


def group_kernel(at, got_ref, cols_ref, inside_ref, send_ref):
    nx, rows, _ = got_ref.shape
    nz = send_ref.shape[0]
    width = inside_ref.shape[0]
    own = rows - width
    piece = own // nz
    inside = jnp.zeros((width, 128), F32)
    whole = jnp.zeros((width, 128), F32)
    for i in range(nx):
        part = got_ref[i, own:rows, :].astype(F32)
        inside = inside + cols_ref[0:width, i : i + 1] * part
        whole = whole + cols_ref[0:width, nx + i : nx + i + 1] * part
    inside_ref[...] = inside
    whole = whole.astype(BF)
    for i in range(nz):
        total = got_ref[0, i * piece : (i + 1) * piece, :].astype(F32)
        for j in range(1, nx):
            total = total + got_ref[j, i * piece : (i + 1) * piece, :].astype(F32)
        send_ref[i, 0:piece, :] = total.astype(BF)
        send_ref[i, piece : piece + width, :] = whole


def last_kernel(first, at, got_ref, cols_ref, inside_ref, k_ref, v_ref, gc_ref, last_ref, qq_ref, kl_ref, vl_ref, og_ref, key_ref, value_ref, decay_ref):
    width, tokens = k_ref.shape
    piece = og_ref.shape[0]
    incoming = inside_ref[...]
    total = jnp.zeros((piece, 128), F32)
    for i in range(got_ref.shape[0]):
        total = total + got_ref[i, 0:piece, :].astype(F32)
        part = got_ref[i, piece : piece + width, :].astype(F32)
        incoming = incoming + cols_ref[0:width, first + i : first + i + 1] * part
    og_ref[...] = total
    gc = gc_ref[...]
    k = k_ref[...].astype(F32)
    rest = jnp.exp(gc[:, tokens - 1 : tokens] - gc)
    key = kl_ref[...] + rest * dot_nt(incoming, v_ref[...].astype(F32), HI)
    key_ref[...] = key.astype(BF)
    value_ref[...] = (vl_ref[...] + dot_tn(k * rest, incoming, HI)).astype(BF)
    later = jnp.where(causal(tokens), 1.0, 0.0)
    cross = jnp.sum(last_ref[...] * incoming, axis=1, keepdims=True)
    decay_ref[...] = dot(qq_ref[...] - k * key, later, HI) + cross


def on_device(
    expert_input,
    cotangent,
    routes,
    route_weight,
    gate_weight,
    up_weight,
    down_weight,
    out_weight,
    queries,
    key_vectors,
    value_rows,
    log_decay,
    start_state,
):
    tokens = expert_input.shape[0]
    nz, nx, ny = lax.axis_size("z"), lax.axis_size("x"), lax.axis_size("y")
    spans = nz * nx
    slices = ny * 2
    core = lax.axis_index("c")
    at = jnp.stack(
        [
            lax.axis_index(TP),
            core,
            lax.axis_index(SP),
            lax.axis_index("z"),
            lax.axis_index("x"),
            jnp.int32(nx),
        ]
    ).astype(jnp.int32)
    width = queries.shape[2]
    piece_rows = slices * 128 // spans
    routes = routes.T
    route_weight = route_weight.T
    q = queries.reshape(tokens, width).T
    k = key_vectors.reshape(tokens, width).T
    v = value_rows.reshape(tokens, 128)
    g = log_decay.reshape(tokens, width).T
    slice_block = ((tokens, 128), lambda i, s: (0, s[0]))

    (sent,) = call(
        dispatch_kernel,
        "dispatch",
        (sds((spans, 40, 128), BF),),
        at,
        routes,
        route_weight,
        expert_input,
        cotangent,
        blocks={2: slice_block, 3: slice_block},
    )
    piece = lax.all_to_all(sent, SP, 0, 0, tiled=True)
    got = lax.all_gather(piece.reshape(spans * 40, 128), TP, axis=0)

    other = jnp.stack([gate_weight[0], up_weight[0]]).reshape(2, ny, 2, 128, 128)
    other = lax.dynamic_index_in_dim(other, 1 - core, 2, keepdims=False)
    other = lax.ppermute(other, "c", [(0, 1), (1, 0)])
    mixed, p, last, gc, totals = call(
        forward_kernel,
        "forward",
        (
            sds((tokens, 128), BF),
            sds((tokens, tokens), BF),
            sds((width, 128), F32),
            sds((width, tokens), F32),
            sds((spans, 8, 128), F32),
        ),
        at,
        q,
        k,
        v,
        g,
        start_state,
        after=(piece,),
    )
    totals = lax.all_to_all(totals, SP, 0, 0, tiled=True)
    (cols,) = call(decay_kernel, "decays", (sds((128, 128), F32),), at, totals)

    delta, pack = call(
        delta_kernel,
        "deltas",
        (sds((spans * 40, 384), BF), sds((spans * 20, 256), BF)),
        at,
        got,
        gate_weight,
        up_weight,
        down_weight,
        scratch=[pltpu.VMEM((slices * 128, 256), BF)],
        after=(cols, other),
    )
    packs = lax.all_gather(pack, "c", axis=0)
    (terms,) = call(
        partial_kernel,
        "partials",
        (sds((ny, spans * 20, 128), BF),),
        at,
        packs,
        gate_weight,
        up_weight,
        other,
    )
    partials = lax.all_to_all(terms, "y", 0, 0, tiled=True)
    gate_grad, up_grad, down_grad = call(
        weight_kernel,
        "weights",
        (
            sds((1, slices * 128, 128), BF),
            sds((1, slices * 128, 128), BF),
            sds((1, 128, slices * 128), BF),
        ),
        at,
        delta,
        got,
        scratch=[pltpu.VMEM((384, spans * 40), BF)],
        after=(terms,),
    )
    (summed,) = call(
        sum_kernel, "sums", (sds((spans, 24, 128), BF),), at, partials, after=(down_grad,)
    )
    returned = lax.all_to_all(summed, SP, 0, 0, tiled=True)
    (slice_grad,) = call(
        collect_kernel,
        "collect",
        (sds((tokens, 128), BF),),
        at,
        routes,
        returned,
        cotangent,
        blocks={2: slice_block},
    )
    total_grad = lax.all_gather(slice_grad, TP, axis=0)

    rows, leaving = call(
        partial(head_kernel, piece_rows),
        "head",
        (sds((tokens, 128), BF), sds((nx, nz * piece_rows + width, 128), BF)),
        at,
        total_grad,
        out_weight,
        q,
        gc,
        mixed,
    )
    crossing = lax.all_to_all(leaving, "x", 0, 0, tiled=True)
    qraw, qq, key_local, value_local = call(
        local_kernel,
        "local",
        (
            sds((width, tokens), BF),
            sds((width, tokens), F32),
            sds((width, tokens), F32),
            sds((tokens, 128), F32),
        ),
        at,
        rows,
        q,
        k,
        v,
        gc,
        start_state,
        p,
        after=(leaving,),
    )
    inside, group = call(
        group_kernel,
        "group",
        (sds((width, 128), F32), sds((nz, piece_rows + width, 128), BF)),
        at,
        crossing,
        cols,
        after=(qq,),
    )
    group = lax.all_to_all(group, "z", 0, 0, tiled=True)
    out_grad, key, value, decay = call(
        partial(last_kernel, 2 * nx),
        "last",
        (
            sds((piece_rows, 128), F32),
            sds((width, tokens), BF),
            sds((tokens, 128), BF),
            sds((width, tokens), F32),
        ),
        at,
        group,
        cols,
        inside,
        k,
        v,
        gc,
        last,
        qq,
        key_local,
        value_local,
    )
    return (
        gate_grad,
        up_grad,
        down_grad,
        out_grad,
        qraw.T[:, None, :],
        key.T[:, None, :],
        value[:, None, :],
        decay.T[:, None, :],
    )


def solution(mesh):
    torus = Mesh(mesh.devices.reshape(8, 4, mesh.shape["tp"] // 2, 2), ("z", "x", "y", "c"))
    in_specs = (
        P(SP, None),
        P(SP, None),
        P(SP, None),
        P(SP, None),
        P(SP, None, TP),
        P(SP, None, TP),
        P(SP, TP, None),
        P(None, TP),
        P(SP, TP, None),
        P(SP, TP, None),
        P(SP, TP, None),
        P(SP, TP, None),
        P(SP, TP, None, None),
    )
    out_specs = (
        P(SP, None, TP),
        P(SP, None, TP),
        P(SP, TP, None),
        P(SP, TP),
        P(SP, TP, None),
        P(SP, TP, None),
        P(SP, TP, None),
        P(SP, TP, None),
    )
    return jax.shard_map(
        on_device, mesh=torus, in_specs=in_specs, out_specs=out_specs, check_vma=False
    )
```

```python
from functools import partial

import jax
import jax.numpy as jnp
from jax import lax
from jax.experimental import pallas as pl
from jax.experimental.pallas import tpu as pltpu
from jax.sharding import Mesh
from jax.sharding import PartitionSpec as P

SP = ("z", "x")
TP = ("y", "c")
BF = jnp.bfloat16
F32 = jnp.float32
HI = lax.Precision.HIGHEST
BLOCK = 32
LIMIT = 56 * 1024 * 1024


def dot(a, b, precision=None):
    return lax.dot_general(
        a, b, (((1,), (0,)), ((), ())), precision=precision, preferred_element_type=F32
    )


def dot_nt(a, b, precision=None):
    return lax.dot_general(
        a, b, (((1,), (1,)), ((), ())), precision=precision, preferred_element_type=F32
    )


def dot_tn(a, b, precision=None):
    return lax.dot_general(
        a, b, (((0,), (0,)), ((), ())), precision=precision, preferred_element_type=F32
    )


def iota(shape, dim):
    return lax.broadcasted_iota(jnp.int32, shape, dim)


def params(**kw):
    return pltpu.CompilerParams(vmem_limit_bytes=LIMIT, **kw)


def call(
    kernel, name, outs, scalars, *args, blocks=None, out_blocks=None, scratch=(), after=(), grid=1
):
    blocks = blocks or {}
    out_blocks = out_blocks or {}
    specs = []
    used, waits = len(args), len(after)

    def body(at, *refs):
        kernel(at, *refs[:used], *refs[used + waits :])

    for n, a in enumerate(args):
        if n in blocks:
            specs.append(pl.BlockSpec(*blocks[n]))
        else:
            specs.append(pl.BlockSpec(a.shape, lambda i, s, nd=a.ndim: (0,) * nd))
    specs += [pl.BlockSpec(memory_space=pl.ANY)] * waits
    out_specs = tuple(
        pl.BlockSpec(*out_blocks[n])
        if n in out_blocks
        else pl.BlockSpec(o.shape, lambda i, s, nd=len(o.shape): (0,) * nd)
        for n, o in enumerate(outs)
    )
    return pl.pallas_call(
        body,
        name=name,
        out_shape=outs,
        grid_spec=pltpu.PrefetchScalarGridSpec(
            num_scalar_prefetch=1,
            grid=(grid,),
            in_specs=specs,
            out_specs=out_specs,
            scratch_shapes=list(scratch),
        ),
        compiler_params=params(),
    )(scalars, *args, *after)


def sds(shape, dtype):
    return jax.ShapeDtypeStruct(shape, dtype)


def slots_of(routes):
    tokens = routes.shape[1]
    experts = iota((16, tokens), 0)
    r0, r1 = routes[0:1, :], routes[1:2, :]
    one0, one1 = r0 == experts, r1 == experts
    both = jnp.where(one0 | one1, 1.0, 0.0).astype(BF)
    earlier = jnp.where(iota((tokens, tokens), 0) < iota((tokens, tokens), 1), 1.0, 0.0).astype(BF)
    count = dot(both, earlier)
    s0 = jnp.sum(jnp.where(one0, count, 0.0), axis=0, keepdims=True)
    s1 = jnp.sum(jnp.where(one1, count, 0.0), axis=0, keepdims=True)
    return r0.astype(F32), r1.astype(F32), s0, s1


def column(row):
    return jnp.broadcast_to(row, (row.shape[1], row.shape[1])).T


def dispatch_kernel(at, routes_ref, weight_ref, x_ref, y_ref, out_ref):
    tokens = routes_ref.shape[1]
    r0, r1, s0, s1 = slots_of(routes_ref[...])
    key0 = r0 * 32.0 + s0
    key1 = r1 * 32.0 + s1
    y = y_ref[...].astype(F32)
    w = weight_ref[...]
    table = jnp.concatenate(
        [
            x_ref[...],
            (column(w[0:1])[:, 0:1] * y).astype(BF),
            (column(w[1:2])[:, 0:1] * y).astype(BF),
        ],
        axis=0,
    )
    q = iota((40, tokens), 0)
    is_input = q < 20
    slot = jnp.where(is_input, q, jnp.where(q < 24, q - 4, q - 24)).astype(F32)
    experts = out_ref.shape[0] // 2
    picks = []
    for e in range(experts):
        key = slot + 32.0 * e
        m0, m1 = key0 == key, key1 == key
        picks.append(
            jnp.concatenate(
                [
                    jnp.where(is_input & (m0 | m1), 1.0, 0.0),
                    jnp.where(is_input, 0.0, jnp.where(m0, 1.0, 0.0)),
                    jnp.where(is_input, 0.0, jnp.where(m1, 1.0, 0.0)),
                ],
                axis=1,
            )
        )
    pick = jnp.concatenate(picks, axis=0).astype(BF)
    for f in range(0, out_ref.shape[2], 256):
        rows = dot(pick, table[:, f : f + 256])
        for e in range(experts):
            block = rows[40 * e : 40 * e + 40].astype(BF)
            out_ref[2 * e, :, f : f + 256] = block
            out_ref[2 * e + 1, :, f : f + 256] = block


def swap_halves(a):
    return jnp.concatenate([a[4:8], a[0:4]], axis=0)


def three_products(g_ref, wg_ref, wu_ref, wd_ref):
    g = g_ref[...]
    return dot(g, jnp.concatenate([wg_ref[0], wu_ref[0]], axis=1)), dot_nt(g, wd_ref[0])


def first_kernel(at, g_ref, wg_ref, wu_ref, wd_ref, gu_ref, yh_ref):
    gu, yh = three_products(g_ref, wg_ref, wu_ref, wd_ref)
    gu_ref[...] = gu
    yh_ref[...] = yh


def delta_kernel(at, g_ref, wg_ref, wu_ref, wd_ref, gu_ref, yh_ref, delta_ref, pack_ref):
    gu, yh = three_products(g_ref, wg_ref, wu_ref, wd_ref)
    gu = gu + gu_ref[...]
    yh = yh + yh_ref[...]
    low = iota((8, 128), 0) < 4
    zero8 = jnp.zeros((8, 128), F32)
    dgs, dus, dhs, pgs, pus = [], [], [], [], []
    mixed = []
    spans = g_ref.shape[0] // 40
    for d in range(spans):
        b = 40 * d
        pg, pu = gu[b : b + 24, 0:128], gu[b : b + 24, 128:256]
        hg = jnp.concatenate([yh[b + 24 : b + 40], swap_halves(yh[b + 16 : b + 24])], axis=0)
        s = jax.nn.sigmoid(pg)
        act = pg * s
        hid = act * pu
        gd = hg * pu * s * (1.0 + pg * (1.0 - s))
        ud = hg * act
        dgs += [gd[0:16], jnp.where(low, gd[16:24], 0.0), zero8, zero8]
        dus += [ud[0:16], jnp.where(low, ud[16:24], 0.0), zero8, zero8]
        dhs += [zero8, zero8, jnp.where(low, 0.0, swap_halves(hid[16:24])), hid[0:16]]
        mixed.append((gd, ud))
    for d in range(0, spans, 2):
        for n, parts in ((0, pgs), (1, pus)):
            even, odd = mixed[d][n], mixed[d + 1][n]
            parts += [
                even[0:16],
                jnp.where(low, even[16:24], swap_halves(odd[16:24])),
                odd[0:16],
            ]
    delta_ref[:, 0:128] = jnp.concatenate(dgs, axis=0).astype(BF)
    delta_ref[:, 128:256] = jnp.concatenate(dus, axis=0).astype(BF)
    delta_ref[:, 256:384] = jnp.concatenate(dhs, axis=0).astype(BF)
    pack_ref[:, 0:128] = jnp.concatenate(pgs, axis=0).astype(BF)
    pack_ref[:, 128:256] = jnp.concatenate(pus, axis=0).astype(BF)


def partial_kernel(at, pack_ref, wg_ref, wu_ref, woth_ref, out_ref):
    core = at[1]
    lhs = jnp.concatenate([pack_ref[core], pack_ref[1 - core]], axis=1)
    nz, ny, rows, _ = out_ref.shape
    for y in range(0, ny, 2):
        sides = []
        for v in (y, y + 1):
            first = pl.multiple_of((2 * v + core) * 128, 128)
            sides.append(
                jnp.concatenate(
                    [
                        wg_ref[0, pl.ds(first, 128), :],
                        wu_ref[0, pl.ds(first, 128), :],
                        woth_ref[0, v],
                        woth_ref[1, v],
                    ],
                    axis=1,
                )
            )
        o = dot_nt(lhs, jnp.concatenate(sides, axis=0)).astype(BF)
        for z in range(nz):
            out_ref[z, y] = o[z * rows : (z + 1) * rows, 0:128]
            out_ref[z, y + 1] = o[z * rows : (z + 1) * rows, 128:256]


def weight_kernel(at, delta_ref, own_ref, other_ref, gate_ref, up_ref, down_ref, dt_ref):
    rows, half = own_ref.shape
    for r in range(0, rows, 128):
        dt_ref[:, r : r + 128] = delta_ref[r : r + 128, :].astype(F32).T.astype(BF)
    for g_ref, core in ((own_ref, at[1]), (other_ref, 1 - at[1])):

        def step(p, carry, g_ref=g_ref, core=core):
            o = dot(dt_ref[...], g_ref[:, pl.ds(pl.multiple_of(p * 256, 256), 256)])
            first = pl.multiple_of(core * half + p * 256, 256)
            gate_ref[0, pl.ds(first, 256), :] = o[0:128].T.astype(BF)
            up_ref[0, pl.ds(first, 256), :] = o[128:256].T.astype(BF)
            down_ref[0, :, pl.ds(first, 256)] = o[256:384].astype(BF)
            return carry

        lax.fori_loop(0, half // 256, step, 0)


def sum_kernel(at, got_ref, out_ref):
    nz, ny, _, _ = got_ref.shape
    for z in range(nz):
        total = got_ref[z, 0].astype(F32)
        for y in range(1, ny):
            total = total + got_ref[z, y].astype(F32)
        for p in range(out_ref.shape[0] // 2):
            b = 40 * p
            out_ref[2 * p, z] = total[b : b + 24].astype(BF)
            out_ref[2 * p + 1, z] = jnp.concatenate(
                [total[b + 24 : b + 40], total[b + 16 : b + 24]], axis=0
            ).astype(BF)


def collect_kernel(at, routes_ref, got_ref, cot_ref, out_ref):
    nx, nz, _, _ = got_ref.shape
    routes = routes_ref[...]
    _, _, s0, s1 = slots_of(routes)
    shift = (at[4] % 2).astype(F32) * 4.0
    cols = nx * nz * 24
    lanes = iota((routes.shape[1], cols), 1).astype(F32)
    hit = None
    for n, s in ((0, s0), (1, s1)):
        half = routes[n : n + 1, :] * 2
        block = (half % nx) * nz + half // nx
        row = block.astype(F32) * 24.0 + s + jnp.where(s >= 16.0, shift, 0.0)
        first = column(row)[:, 0:1]
        match = (lanes == first) | (lanes == first + 24.0 * nz)
        hit = match if hit is None else hit | match
    pick = jnp.where(hit, 1.0, 0.0).astype(BF)
    table = got_ref[...].astype(F32).reshape(cols, 128).astype(BF)
    out_ref[...] = (cot_ref[...].astype(F32) + dot(pick, table)).astype(BF)


def block_of(shape):
    return iota(shape, 1) // BLOCK


def mids_of(gc):
    return [gc[:, b + BLOCK // 2 - 1 : b + BLOCK // 2] for b in range(0, gc.shape[1], BLOCK)]


def growth(gc):
    blocks = block_of(gc.shape)
    mid = jnp.zeros(gc.shape, F32)
    for n, m in enumerate(mids_of(gc)):
        mid = jnp.where(blocks == n, m, mid)
    return jnp.exp(gc - mid)


def causal(tokens):
    return iota((tokens, tokens), 1) <= iota((tokens, tokens), 0)


def forward_kernel(at, q_ref, k_ref, v_ref, g_ref, s_ref, mixed_ref, p_ref, last_ref, gc_ref, tot_ref):
    width, tokens = q_ref.shape
    g = g_ref[...]
    before = jnp.where(iota((tokens, tokens), 0) <= iota((tokens, tokens), 1), 1.0, 0.0)
    gc = dot(g, before, HI)
    gc_ref[...] = gc
    q = q_ref[...].astype(F32) * (width**-0.5)
    k = k_ref[...].astype(F32)
    v = v_ref[...].astype(F32)
    s0 = s_ref[0, 0]
    qt = q * growth(gc)
    parts = []
    for n, mid in enumerate(mids_of(gc)):
        whole = dot_tn(qt, k * jnp.exp(jnp.minimum(mid - gc, 40.0)), HI)
        parts.append(whole[n * BLOCK : (n + 1) * BLOCK])
    p = jnp.where(causal(tokens), jnp.concatenate(parts, axis=0), 0.0)
    p_ref[...] = p.astype(BF)
    mixed_ref[...] = (dot_tn(q * jnp.exp(gc), s0, HI) + dot(p, v, HI)).astype(BF)
    end = gc[:, tokens - 1 : tokens]
    last_ref[...] = jnp.exp(end) * s0 + dot(k * jnp.exp(end - gc), v, HI)
    row = dot_nt(jnp.ones((8, tokens), F32), g, HI)
    tot_ref[...] = jnp.zeros(tot_ref.shape, F32)
    tot_ref[:, 0:width] = row


def decay_kernel(at, tot_ref, out_ref):
    spans = tot_ref.shape[0]
    z, x, nx = at[3], at[4], at[5]
    nz = spans // nx
    k = iota((128, spans), 0)
    u = iota((128, spans), 1)
    own = z * nx + x
    low = jnp.where((k >= nx) & (k < 2 * nx), z * nx - 1, own)
    high = jnp.where(k < nx, z * nx + k, jnp.where(k < 2 * nx, z * nx + k - nx, (k - 2 * nx) * nx))
    inside = jnp.where((u > low) & (u < high), 1.0, 0.0)
    sums = dot(inside, tot_ref[:, 0, :], HI)
    kk = iota((128, 128), 0)
    valid = (
        ((kk < nx) & (kk > x))
        | ((kk >= nx) & (kk < 2 * nx))
        | ((kk > 2 * nx + z) & (kk < 2 * nx + nz))
    )
    out_ref[...] = jnp.where(valid, jnp.exp(sums), 0.0).T


def head_kernel(piece, at, tg_ref, w_ref, q_ref, gc_ref, mixed_ref, rows_ref, send_ref):
    slices = tg_ref.shape[0]
    width = q_ref.shape[0]
    nx = send_ref.shape[0]
    tg = jnp.concatenate([tg_ref[t] for t in range(slices)], axis=1)
    rows = dot(tg, w_ref[...]).astype(BF)
    rows_ref[...] = rows
    qe = q_ref[...].astype(F32) * (width**-0.5) * jnp.exp(gc_ref[...])
    carry = dot(qe, rows.astype(F32), HI).astype(BF)
    own = send_ref.shape[1] - width
    for n in range(nx):
        send_ref[n, own : own + width, :] = carry
    mixed = mixed_ref[...]
    for t in range(slices):
        o = dot_tn(tg_ref[t], mixed).astype(BF)
        for r in range(0, 128, piece):
            d = (t * 128 + r) // piece
            send_ref[d % nx, (d // nx) * piece : (d // nx + 1) * piece, :] = o[r : r + piece]


def local_kernel(at, rows_ref, q_ref, k_ref, v_ref, gc_ref, s_ref, p_ref, qraw_ref, qq_ref, kl_ref, vl_ref):
    width, tokens = q_ref.shape
    scale = width**-0.5
    rows = rows_ref[...]
    gc = gc_ref[...]
    q = q_ref[...].astype(F32)
    k = k_ref[...].astype(F32)
    a = jnp.where(causal(tokens), dot_nt(rows, v_ref[...]), 0.0)
    grow = growth(gc)
    qt = q * scale * grow
    blocks = block_of(gc.shape)
    inner = jnp.zeros((width, tokens), F32)
    key_local = jnp.zeros((width, tokens), F32)
    for n, mid in enumerate(mids_of(gc)):
        fall = jnp.exp(jnp.minimum(mid - gc, 40.0))
        inner = jnp.where(blocks == n, dot_nt(k * fall, a, HI), inner)
        key_local = key_local + fall * dot(jnp.where(blocks == n, qt, 0.0), a, HI)
    qraw = scale * (jnp.exp(gc) * dot_nt(s_ref[0, 0], rows.astype(F32), HI) + grow * inner)
    qraw_ref[...] = qraw.astype(BF)
    qq_ref[...] = q * qraw
    kl_ref[...] = key_local
    vl_ref[...] = dot_tn(p_ref[...], rows)


def group_kernel(at, got_ref, cols_ref, inside_ref, send_ref):
    nx, rows, _ = got_ref.shape
    nz = send_ref.shape[0]
    width = inside_ref.shape[0]
    own = rows - width
    piece = own // nz
    inside = jnp.zeros((width, 128), F32)
    whole = jnp.zeros((width, 128), F32)
    for i in range(nx):
        part = got_ref[i, own:rows, :].astype(F32)
        inside = inside + cols_ref[0:width, i : i + 1] * part
        whole = whole + cols_ref[0:width, nx + i : nx + i + 1] * part
    inside_ref[...] = inside
    whole = whole.astype(BF)
    for i in range(nz):
        total = got_ref[0, i * piece : (i + 1) * piece, :].astype(F32)
        for j in range(1, nx):
            total = total + got_ref[j, i * piece : (i + 1) * piece, :].astype(F32)
        send_ref[i, 0:piece, :] = total.astype(BF)
        send_ref[i, piece : piece + width, :] = whole


def last_kernel(first, at, got_ref, cols_ref, inside_ref, k_ref, v_ref, gc_ref, last_ref, qq_ref, kl_ref, vl_ref, og_ref, key_ref, value_ref, decay_ref):
    width, tokens = k_ref.shape
    piece = og_ref.shape[0]
    incoming = inside_ref[...]
    total = jnp.zeros((piece, 128), F32)
    for i in range(got_ref.shape[0]):
        total = total + got_ref[i, 0:piece, :].astype(F32)
        part = got_ref[i, piece : piece + width, :].astype(F32)
        incoming = incoming + cols_ref[0:width, first + i : first + i + 1] * part
    og_ref[...] = total
    gc = gc_ref[...]
    k = k_ref[...].astype(F32)
    rest = jnp.exp(gc[:, tokens - 1 : tokens] - gc)
    key = kl_ref[...] + rest * dot_nt(incoming, v_ref[...].astype(F32), HI)
    key_ref[...] = key.astype(BF)
    value_ref[...] = (vl_ref[...] + dot_tn(k * rest, incoming, HI)).astype(BF)
    later = jnp.where(causal(tokens), 1.0, 0.0)
    cross = jnp.sum(last_ref[...] * incoming, axis=1, keepdims=True)
    decay_ref[...] = dot(qq_ref[...] - k * key, later, HI) + cross


def on_device(
    expert_input,
    cotangent,
    routes,
    route_weight,
    gate_weight,
    up_weight,
    down_weight,
    out_weight,
    queries,
    key_vectors,
    value_rows,
    log_decay,
    start_state,
):
    tokens = expert_input.shape[0]
    nz, nx, ny = lax.axis_size("z"), lax.axis_size("x"), lax.axis_size("y")
    spans = nz * nx
    slices = ny * 2
    core = lax.axis_index("c")
    at = jnp.stack(
        [
            lax.axis_index(TP),
            core,
            lax.axis_index(SP),
            lax.axis_index("z"),
            lax.axis_index("x"),
            jnp.int32(nx),
        ]
    ).astype(jnp.int32)
    width = queries.shape[2]
    piece_rows = slices * 128 // spans
    routes = routes.T
    route_weight = route_weight.T
    q = queries.reshape(tokens, width).T
    k = key_vectors.reshape(tokens, width).T
    v = value_rows.reshape(tokens, 128)
    g = log_decay.reshape(tokens, width).T
    slice_block = ((tokens, 128), lambda i, s: (0, s[0]))
    half = slices * 64
    half_block = ((tokens, half), lambda i, s: (0, s[1]))

    (sent,) = call(
        dispatch_kernel,
        "dispatch",
        (sds((spans, 40, half), BF),),
        at,
        routes,
        route_weight,
        expert_input,
        cotangent,
        blocks={2: half_block, 3: half_block},
    )
    own = lax.all_to_all(sent, SP, 0, 0, tiled=True).reshape(spans * 40, half)

    weights = jnp.stack([gate_weight[0], up_weight[0]]).reshape(2, ny, 2, 128, 128)
    weights = lax.dynamic_index_in_dim(weights, 1 - core, 2, keepdims=False)
    weights = lax.ppermute(weights, "c", [(0, 1), (1, 0)])
    mixed, p, last, gc, totals = call(
        forward_kernel,
        "forward",
        (
            sds((tokens, 128), BF),
            sds((tokens, tokens), BF),
            sds((width, 128), F32),
            sds((width, tokens), F32),
            sds((8, 128), F32),
        ),
        at,
        q,
        k,
        v,
        g,
        start_state,
        after=(sent,),
    )
    totals = lax.all_gather(lax.all_gather(totals, "x"), "z").reshape(spans, 8, 128)
    (cols,) = call(decay_kernel, "decays", (sds((128, 128), F32),), at, totals)

    own, cols, weights = lax.optimization_barrier((own, cols, weights))
    tiles = spans // 8
    rows_block = ((320, half), lambda i, s: (i, 0))
    acc_blocks = (((320, 256), lambda i, s: (i, 0)), ((320, 128), lambda i, s: (i, 0)))
    gu, yh = call(
        first_kernel,
        "first",
        (sds((spans * 40, 256), F32), sds((spans * 40, 128), F32)),
        at,
        own,
        gate_weight,
        up_weight,
        down_weight,
        blocks={
            0: rows_block,
            1: ((1, half, 128), lambda i, s: (0, s[1], 0)),
            2: ((1, half, 128), lambda i, s: (0, s[1], 0)),
            3: ((1, 128, half), lambda i, s: (0, 0, s[1])),
        },
        out_blocks={0: acc_blocks[0], 1: acc_blocks[1]},
        grid=tiles,
    )
    other = lax.ppermute(own, "c", [(0, 1), (1, 0)])
    delta, pack = call(
        delta_kernel,
        "deltas",
        (sds((spans * 40, 384), BF), sds((spans * 20, 256), BF)),
        at,
        other,
        gate_weight,
        up_weight,
        down_weight,
        gu,
        yh,
        blocks={
            0: rows_block,
            1: ((1, half, 128), lambda i, s: (0, 1 - s[1], 0)),
            2: ((1, half, 128), lambda i, s: (0, 1 - s[1], 0)),
            3: ((1, 128, half), lambda i, s: (0, 0, 1 - s[1])),
            4: acc_blocks[0],
            5: acc_blocks[1],
        },
        out_blocks={
            0: ((320, 384), lambda i, s: (i, 0)),
            1: ((160, 256), lambda i, s: (i, 0)),
        },
        grid=tiles,
    )
    packs = lax.all_gather(pack, "c", axis=0)
    (terms,) = call(
        partial_kernel,
        "partials",
        (sds((nz, ny, nx * 20, 128), BF),),
        at,
        packs,
        gate_weight,
        up_weight,
        weights,
    )
    got = lax.all_to_all(
        terms.reshape(nz * ny, nx * 20, 128), ("z", "y"), 0, 0, tiled=True
    ).reshape(nz, ny, nx * 20, 128)
    gate_grad, up_grad, down_grad = call(
        weight_kernel,
        "weights",
        (
            sds((1, slices * 128, 128), BF),
            sds((1, slices * 128, 128), BF),
            sds((1, 128, slices * 128), BF),
        ),
        at,
        delta,
        own,
        other,
        scratch=[pltpu.VMEM((384, spans * 40), BF)],
        after=(terms,),
    )
    (summed,) = call(
        sum_kernel, "sums", (sds((nx, nz, 24, 128), BF),), at, got, after=(down_grad,)
    )
    returned = lax.all_to_all(summed.reshape(nx, nz * 24, 128), "x", 0, 0, tiled=True)
    (slice_grad,) = call(
        collect_kernel,
        "collect",
        (sds((tokens, 128), BF),),
        at,
        routes,
        returned.reshape(nx, nz, 24, 128),
        cotangent,
        blocks={2: slice_block},
    )
    total_grad = lax.all_gather(slice_grad, TP, axis=0)

    rows, leaving = call(
        partial(head_kernel, piece_rows),
        "head",
        (sds((tokens, 128), BF), sds((nx, nz * piece_rows + width, 128), BF)),
        at,
        total_grad,
        out_weight,
        q,
        gc,
        mixed,
    )
    crossing = lax.all_to_all(leaving, "x", 0, 0, tiled=True)
    qraw, qq, key_local, value_local = call(
        local_kernel,
        "local",
        (
            sds((width, tokens), BF),
            sds((width, tokens), F32),
            sds((width, tokens), F32),
            sds((tokens, 128), F32),
        ),
        at,
        rows,
        q,
        k,
        v,
        gc,
        start_state,
        p,
        after=(leaving,),
    )
    inside, group = call(
        group_kernel,
        "group",
        (sds((width, 128), F32), sds((nz, piece_rows + width, 128), BF)),
        at,
        crossing,
        cols,
        after=(qq,),
    )
    group = lax.all_to_all(group, "z", 0, 0, tiled=True)
    out_grad, key, value, decay = call(
        partial(last_kernel, 2 * nx),
        "last",
        (
            sds((piece_rows, 128), F32),
            sds((width, tokens), BF),
            sds((tokens, 128), BF),
            sds((width, tokens), F32),
        ),
        at,
        group,
        cols,
        inside,
        k,
        v,
        gc,
        last,
        qq,
        key_local,
        value_local,
    )
    return (
        gate_grad,
        up_grad,
        down_grad,
        out_grad,
        qraw.T[:, None, :],
        key.T[:, None, :],
        value[:, None, :],
        decay.T[:, None, :],
    )


def solution(mesh):
    torus = Mesh(mesh.devices.reshape(8, 4, mesh.shape["tp"] // 2, 2), ("z", "x", "y", "c"))
    in_specs = (
        P(SP, None),
        P(SP, None),
        P(SP, None),
        P(SP, None),
        P(SP, None, TP),
        P(SP, None, TP),
        P(SP, TP, None),
        P(None, TP),
        P(SP, TP, None),
        P(SP, TP, None),
        P(SP, TP, None),
        P(SP, TP, None),
        P(SP, TP, None, None),
    )
    out_specs = (
        P(SP, None, TP),
        P(SP, None, TP),
        P(SP, TP, None),
        P(SP, TP),
        P(SP, TP, None),
        P(SP, TP, None),
        P(SP, TP, None),
        P(SP, TP, None),
    )
    return jax.shard_map(
        on_device, mesh=torus, in_specs=in_specs, out_specs=out_specs, check_vma=False
    )
```

```python
from functools import partial

import jax
import jax.numpy as jnp
from jax import lax
from jax.experimental import pallas as pl
from jax.experimental.pallas import tpu as pltpu
from jax.sharding import Mesh
from jax.sharding import PartitionSpec as P

SP = ("z", "x")
TP = ("y", "c")
BF = jnp.bfloat16
F32 = jnp.float32
HI = lax.Precision.HIGHEST
BLOCK = 32
LIMIT = 56 * 1024 * 1024


def dot(a, b, precision=None):
    return lax.dot_general(
        a, b, (((1,), (0,)), ((), ())), precision=precision, preferred_element_type=F32
    )


def dot_nt(a, b, precision=None):
    return lax.dot_general(
        a, b, (((1,), (1,)), ((), ())), precision=precision, preferred_element_type=F32
    )


def dot_tn(a, b, precision=None):
    return lax.dot_general(
        a, b, (((0,), (0,)), ((), ())), precision=precision, preferred_element_type=F32
    )


def iota(shape, dim):
    return lax.broadcasted_iota(jnp.int32, shape, dim)


def params(**kw):
    return pltpu.CompilerParams(vmem_limit_bytes=LIMIT, **kw)


def call(
    kernel, name, outs, scalars, *args, blocks=None, out_blocks=None, scratch=(), after=(), grid=1
):
    blocks = blocks or {}
    out_blocks = out_blocks or {}
    specs = []
    used, waits = len(args), len(after)

    def body(at, *refs):
        kernel(at, *refs[:used], *refs[used + waits :])

    for n, a in enumerate(args):
        if n in blocks:
            specs.append(pl.BlockSpec(*blocks[n]))
        else:
            specs.append(pl.BlockSpec(a.shape, lambda i, s, nd=a.ndim: (0,) * nd))
    specs += [pl.BlockSpec(memory_space=pl.ANY)] * waits
    out_specs = tuple(
        pl.BlockSpec(*out_blocks[n])
        if n in out_blocks
        else pl.BlockSpec(o.shape, lambda i, s, nd=len(o.shape): (0,) * nd)
        for n, o in enumerate(outs)
    )
    return pl.pallas_call(
        body,
        name=name,
        out_shape=outs,
        grid_spec=pltpu.PrefetchScalarGridSpec(
            num_scalar_prefetch=1,
            grid=(grid,),
            in_specs=specs,
            out_specs=out_specs,
            scratch_shapes=list(scratch),
        ),
        compiler_params=params(),
    )(scalars, *args, *after)


def sds(shape, dtype):
    return jax.ShapeDtypeStruct(shape, dtype)


def slots_of(routes):
    tokens = routes.shape[1]
    experts = iota((16, tokens), 0)
    r0, r1 = routes[0:1, :], routes[1:2, :]
    one0, one1 = r0 == experts, r1 == experts
    both = jnp.where(one0 | one1, 1.0, 0.0).astype(BF)
    earlier = jnp.where(iota((tokens, tokens), 0) < iota((tokens, tokens), 1), 1.0, 0.0).astype(BF)
    count = dot(both, earlier)
    s0 = jnp.sum(jnp.where(one0, count, 0.0), axis=0, keepdims=True)
    s1 = jnp.sum(jnp.where(one1, count, 0.0), axis=0, keepdims=True)
    return r0.astype(F32), r1.astype(F32), s0, s1


def column(row):
    return jnp.broadcast_to(row, (row.shape[1], row.shape[1])).T


def dispatch_kernel(at, routes_ref, weight_ref, x_ref, y_ref, out_ref):
    tokens = routes_ref.shape[1]
    r0, r1, s0, s1 = slots_of(routes_ref[...])
    key0 = r0 * 32.0 + s0
    key1 = r1 * 32.0 + s1
    y = y_ref[...].astype(F32)
    w = weight_ref[...]
    table = jnp.concatenate(
        [
            x_ref[...],
            (column(w[0:1])[:, 0:1] * y).astype(BF),
            (column(w[1:2])[:, 0:1] * y).astype(BF),
        ],
        axis=0,
    )
    q = iota((40, tokens), 0)
    is_input = q < 20
    slot = jnp.where(is_input, q, jnp.where(q < 24, q - 4, q - 24)).astype(F32)
    experts = out_ref.shape[0] // 2
    picks = []
    for e in range(experts):
        key = slot + 32.0 * e
        m0, m1 = key0 == key, key1 == key
        picks.append(
            jnp.concatenate(
                [
                    jnp.where(is_input & (m0 | m1), 1.0, 0.0),
                    jnp.where(is_input, 0.0, jnp.where(m0, 1.0, 0.0)),
                    jnp.where(is_input, 0.0, jnp.where(m1, 1.0, 0.0)),
                ],
                axis=1,
            )
        )
    pick = jnp.concatenate(picks, axis=0).astype(BF)
    for f in range(0, out_ref.shape[2], 256):
        wide = slice(f, min(f + 256, out_ref.shape[2]))
        rows = dot(pick, table[:, wide])
        for e in range(experts):
            block = rows[40 * e : 40 * e + 40].astype(BF)
            out_ref[2 * e, :, wide] = block
            out_ref[2 * e + 1, :, wide] = block


def swap_halves(a):
    return jnp.concatenate([a[4:8], a[0:4]], axis=0)


def products(g, wg_ref, wu_ref, wd_ref):
    return dot(g, jnp.concatenate([wg_ref[0], wu_ref[0]], axis=1)), dot_nt(g, wd_ref[0])


def first_kernel(at, a_ref, b_ref, *refs):
    gu0, yh0 = products(a_ref[...], *refs[0:3])
    gu1, yh1 = products(b_ref[...], *refs[3:6])
    refs[6][...] = gu0 + gu1
    refs[7][...] = yh0 + yh1


def chosen(low_ref, high_ref):
    upper = pl.program_id(0) >= pl.num_programs(0) // 2
    return jnp.where(upper, high_ref[...], low_ref[...])


def second_kernel(at, low_ref, high_ref, wg_ref, wu_ref, wd_ref, gu_ref, yh_ref, gu_out, yh_out):
    gu, yh = products(chosen(low_ref, high_ref), wg_ref, wu_ref, wd_ref)
    gu_out[...] = gu + gu_ref[...]
    yh_out[...] = yh + yh_ref[...]


def delta_kernel(at, low_ref, high_ref, wg_ref, wu_ref, wd_ref, gu_ref, yh_ref, delta_ref, pack_ref):
    gu, yh = products(chosen(low_ref, high_ref), wg_ref, wu_ref, wd_ref)
    gu = gu + gu_ref[...]
    yh = yh + yh_ref[...]
    low = iota((8, 128), 0) < 4
    zero8 = jnp.zeros((8, 128), F32)
    dgs, dus, dhs, pgs, pus = [], [], [], [], []
    mixed = []
    spans = low_ref.shape[0] // 40
    for d in range(spans):
        b = 40 * d
        pg, pu = gu[b : b + 24, 0:128], gu[b : b + 24, 128:256]
        hg = jnp.concatenate([yh[b + 24 : b + 40], swap_halves(yh[b + 16 : b + 24])], axis=0)
        s = jax.nn.sigmoid(pg)
        act = pg * s
        hid = act * pu
        gd = hg * pu * s * (1.0 + pg * (1.0 - s))
        ud = hg * act
        dgs += [gd[0:16], jnp.where(low, gd[16:24], 0.0), zero8, zero8]
        dus += [ud[0:16], jnp.where(low, ud[16:24], 0.0), zero8, zero8]
        dhs += [zero8, zero8, jnp.where(low, 0.0, swap_halves(hid[16:24])), hid[0:16]]
        mixed.append((gd, ud))
    for d in range(0, spans, 2):
        for n, parts in ((0, pgs), (1, pus)):
            even, odd = mixed[d][n], mixed[d + 1][n]
            parts += [
                even[0:16],
                jnp.where(low, even[16:24], swap_halves(odd[16:24])),
                odd[0:16],
            ]
    delta_ref[:, 0:128] = jnp.concatenate(dgs, axis=0).astype(BF)
    delta_ref[:, 128:256] = jnp.concatenate(dus, axis=0).astype(BF)
    delta_ref[:, 256:384] = jnp.concatenate(dhs, axis=0).astype(BF)
    pack_ref[:, 0:128] = jnp.concatenate(pgs, axis=0).astype(BF)
    pack_ref[:, 128:256] = jnp.concatenate(pus, axis=0).astype(BF)


def partial_kernel(at, pack_ref, wg_ref, wu_ref, woth_ref, out_ref):
    core = at[1]
    lhs = jnp.concatenate([pack_ref[core], pack_ref[1 - core]], axis=1)
    nz, ny, rows, _ = out_ref.shape
    for y in range(0, ny, 2):
        sides = []
        for v in (y, y + 1):
            first = pl.multiple_of((2 * v + core) * 128, 128)
            sides.append(
                jnp.concatenate(
                    [
                        wg_ref[0, pl.ds(first, 128), :],
                        wu_ref[0, pl.ds(first, 128), :],
                        woth_ref[0, v],
                        woth_ref[1, v],
                    ],
                    axis=1,
                )
            )
        o = dot_nt(lhs, jnp.concatenate(sides, axis=0)).astype(BF)
        for z in range(nz):
            out_ref[z, y] = o[z * rows : (z + 1) * rows, 0:128]
            out_ref[z, y + 1] = o[z * rows : (z + 1) * rows, 128:256]


def weight_kernel(at, delta_ref, a_ref, b_ref, c0_ref, c1_ref, d0_ref, d1_ref, gate_ref, up_ref, down_ref, dt_ref):
    rows, part = a_ref.shape
    for r in range(0, rows, 128):
        dt_ref[:, r : r + 128] = delta_ref[r : r + 128, :].astype(F32).T.astype(BF)
    core, side = at[1], at[6]
    for refs, quarter in (
        ((a_ref,), 2 * side + core),
        ((b_ref,), 2 * side + 1 - core),
        ((c0_ref, c1_ref), 2 * (1 - side) + core),
        ((d0_ref, d1_ref), 2 * (1 - side) + 1 - core),
    ):
        size = rows // len(refs)
        for p in range(0, part, 256):
            o = dot(dt_ref[:, 0:size], refs[0][:, p : p + 256])
            for n in range(1, len(refs)):
                o = o + dot(dt_ref[:, n * size : (n + 1) * size], refs[n][:, p : p + 256])
            at_row = pl.multiple_of(quarter * part + p, 128)
            wide = min(256, part - p)
            gate_ref[0, pl.ds(at_row, wide), :] = o[0:128].T.astype(BF)
            up_ref[0, pl.ds(at_row, wide), :] = o[128:256].T.astype(BF)
            down_ref[0, :, pl.ds(at_row, wide)] = o[256:384].astype(BF)


def sum_kernel(at, got_ref, out_ref):
    nz, ny, _, _ = got_ref.shape
    for z in range(nz):
        total = got_ref[z, 0].astype(F32)
        for y in range(1, ny):
            total = total + got_ref[z, y].astype(F32)
        for p in range(out_ref.shape[0] // 2):
            b = 40 * p
            out_ref[2 * p, z] = total[b : b + 24].astype(BF)
            out_ref[2 * p + 1, z] = jnp.concatenate(
                [total[b + 24 : b + 40], total[b + 16 : b + 24]], axis=0
            ).astype(BF)


def collect_kernel(at, routes_ref, got_ref, cot_ref, out_ref):
    nx, nz, _, _ = got_ref.shape
    routes = routes_ref[...]
    _, _, s0, s1 = slots_of(routes)
    shift = (at[4] % 2).astype(F32) * 4.0
    cols = nx * nz * 24
    lanes = iota((routes.shape[1], cols), 1).astype(F32)
    hit = None
    for n, s in ((0, s0), (1, s1)):
        half = routes[n : n + 1, :] * 2
        block = (half % nx) * nz + half // nx
        row = block.astype(F32) * 24.0 + s + jnp.where(s >= 16.0, shift, 0.0)
        first = column(row)[:, 0:1]
        match = (lanes == first) | (lanes == first + 24.0 * nz)
        hit = match if hit is None else hit | match
    pick = jnp.where(hit, 1.0, 0.0).astype(BF)
    table = got_ref[...].astype(F32).reshape(cols, 128).astype(BF)
    out_ref[...] = (cot_ref[...].astype(F32) + dot(pick, table)).astype(BF)


def block_of(shape):
    return iota(shape, 1) // BLOCK


def mids_of(gc):
    return [gc[:, b + BLOCK // 2 - 1 : b + BLOCK // 2] for b in range(0, gc.shape[1], BLOCK)]


def growth(gc):
    blocks = block_of(gc.shape)
    mid = jnp.zeros(gc.shape, F32)
    for n, m in enumerate(mids_of(gc)):
        mid = jnp.where(blocks == n, m, mid)
    return jnp.exp(gc - mid)


def causal(tokens):
    return iota((tokens, tokens), 1) <= iota((tokens, tokens), 0)


def in_parts(rows):
    high = rows.astype(BF)
    rest = rows - high.astype(F32)
    mid = rest.astype(BF)
    low = (rest - mid.astype(F32)).astype(BF)
    n = iota(rows.shape, 0)
    parts = jnp.where(n == 0, high.astype(F32), jnp.where(n == 1, mid.astype(F32), low.astype(F32)))
    return jnp.where(n < 3, parts, 0.0).astype(BF)


def columns(rows):
    rows = rows + [jnp.zeros((128 - len(rows), 128), F32)]
    return jnp.concatenate(rows, axis=0).T


def forward_kernel(at, q_ref, k_ref, v_ref, g_ref, s_ref, mixed_ref, p_ref, last_ref, gc_ref, tot_ref):
    width, tokens = q_ref.shape
    g = g_ref[...]
    before = jnp.where(iota((tokens, tokens), 0) <= iota((tokens, tokens), 1), 1.0, 0.0)
    gc = dot(g, before, HI)
    gc_ref[...] = gc
    q = q_ref[...].astype(F32) * (width**-0.5)
    k = k_ref[...].astype(F32)
    v = v_ref[...].astype(F32)
    s0 = s_ref[0, 0]
    qt = q * growth(gc)
    parts = []
    for n, mid in enumerate(mids_of(gc)):
        whole = dot_tn(qt, k * jnp.exp(jnp.minimum(mid - gc, 40.0)), HI)
        parts.append(whole[n * BLOCK : (n + 1) * BLOCK])
    p = jnp.where(causal(tokens), jnp.concatenate(parts, axis=0), 0.0)
    p_ref[...] = p.astype(BF)
    mixed_ref[...] = (dot_tn(q * jnp.exp(gc), s0, HI) + dot(p, v, HI)).astype(BF)
    end = gc[:, tokens - 1 : tokens]
    last_ref[...] = jnp.exp(end) * s0 + dot(k * jnp.exp(end - gc), v, HI)
    row = dot_nt(jnp.ones((8, tokens), F32), g, HI)
    row = jnp.concatenate([row, jnp.zeros((8, 128 - width), F32)], axis=1)
    tot_ref[...] = in_parts(row)


def head_kernel(piece, at, tg_ref, w_ref, q_ref, gc_ref, mixed_ref, tot_ref, rows_ref, send_ref):
    slices = tg_ref.shape[0]
    width = q_ref.shape[0]
    nx = send_ref.shape[0]
    tg = jnp.concatenate([tg_ref[t] for t in range(slices)], axis=1)
    rows = dot(tg, w_ref[...]).astype(BF)
    rows_ref[...] = rows
    qe = q_ref[...].astype(F32) * (width**-0.5) * jnp.exp(gc_ref[...])
    carry = dot(qe, rows.astype(F32), HI).astype(BF)
    own = send_ref.shape[1] - width - 8
    for n in range(nx):
        send_ref[n, own : own + width, :] = carry
        send_ref[n, own + width : own + width + 8, :] = tot_ref[...]
    mixed = mixed_ref[...]
    for t in range(slices):
        o = dot_tn(tg_ref[t], mixed).astype(BF)
        for r in range(0, 128, piece):
            d = (t * 128 + r) // piece
            send_ref[d % nx, (d // nx) * piece : (d // nx + 1) * piece, :] = o[r : r + piece]


def local_kernel(at, rows_ref, q_ref, k_ref, v_ref, gc_ref, s_ref, p_ref, qraw_ref, qq_ref, kl_ref, vl_ref):
    width, tokens = q_ref.shape
    scale = width**-0.5
    rows = rows_ref[...]
    gc = gc_ref[...]
    q = q_ref[...].astype(F32)
    k = k_ref[...].astype(F32)
    a = jnp.where(causal(tokens), dot_nt(rows, v_ref[...]), 0.0)
    grow = growth(gc)
    qt = q * scale * grow
    blocks = block_of(gc.shape)
    inner = jnp.zeros((width, tokens), F32)
    key_local = jnp.zeros((width, tokens), F32)
    for n, mid in enumerate(mids_of(gc)):
        fall = jnp.exp(jnp.minimum(mid - gc, 40.0))
        inner = jnp.where(blocks == n, dot_nt(k * fall, a, HI), inner)
        key_local = key_local + fall * dot(jnp.where(blocks == n, qt, 0.0), a, HI)
    qraw = scale * (jnp.exp(gc) * dot_nt(s_ref[0, 0], rows.astype(F32), HI) + grow * inner)
    qraw_ref[...] = qraw.astype(BF)
    qq_ref[...] = q * qraw
    kl_ref[...] = key_local
    vl_ref[...] = dot_tn(p_ref[...], rows)


def group_kernel(at, got_ref, inside_ref, after_ref, send_ref):
    nx, rows, _ = got_ref.shape
    nz = send_ref.shape[0]
    width = inside_ref.shape[0]
    own = rows - width - 8
    piece = own // nz
    x = at[4]
    zero = jnp.zeros((1, 128), F32)
    before, later = zero, zero
    weights, wholes = [], []
    for i in range(nx):
        weights.append(jnp.where(x < i, jnp.exp(later), 0.0))
        wholes.append(jnp.exp(before))
        part = got_ref[i, own + width : own + width + 8, :].astype(F32)
        total = jnp.sum(part, axis=0, keepdims=True)
        before = before + total
        later = later + jnp.where(x < i, total, 0.0)
    after_ref[...] = jnp.broadcast_to(later, (8, 128))
    cols = columns(weights + wholes)
    inside = jnp.zeros((width, 128), F32)
    whole = jnp.zeros((width, 128), F32)
    for i in range(nx):
        part = got_ref[i, own : own + width, :].astype(F32)
        inside = inside + cols[0:width, i : i + 1] * part
        whole = whole + cols[0:width, nx + i : nx + i + 1] * part
    inside_ref[...] = inside
    whole = whole.astype(BF)
    parts = in_parts(jnp.broadcast_to(before, (8, 128)))
    for i in range(nz):
        total = got_ref[0, i * piece : (i + 1) * piece, :].astype(F32)
        for j in range(1, nx):
            total = total + got_ref[j, i * piece : (i + 1) * piece, :].astype(F32)
        send_ref[i, 0:piece, :] = total.astype(BF)
        send_ref[i, piece : piece + width, :] = whole
        send_ref[i, piece + width : piece + width + 8, :] = parts


def last_kernel(at, got_ref, inside_ref, after_ref, k_ref, v_ref, gc_ref, last_ref, qq_ref, kl_ref, vl_ref, og_ref, key_ref, value_ref, decay_ref):
    width, tokens = k_ref.shape
    piece = og_ref.shape[0]
    z = at[3]
    sums = after_ref[0:1, :]
    weights = []
    for i in range(got_ref.shape[0]):
        weights.append(jnp.where(z < i, jnp.exp(sums), 0.0))
        part = got_ref[i, piece + width : piece + width + 8, :].astype(F32)
        sums = sums + jnp.where(z < i, jnp.sum(part, axis=0, keepdims=True), 0.0)
    cols = columns(weights)
    incoming = inside_ref[...]
    total = jnp.zeros((piece, 128), F32)
    for i in range(got_ref.shape[0]):
        total = total + got_ref[i, 0:piece, :].astype(F32)
        part = got_ref[i, piece : piece + width, :].astype(F32)
        incoming = incoming + cols[0:width, i : i + 1] * part
    og_ref[...] = total
    gc = gc_ref[...]
    k = k_ref[...].astype(F32)
    rest = jnp.exp(gc[:, tokens - 1 : tokens] - gc)
    key = kl_ref[...] + rest * dot_nt(incoming, v_ref[...].astype(F32), HI)
    key_ref[...] = key.astype(BF)
    value_ref[...] = (vl_ref[...] + dot_tn(k * rest, incoming, HI)).astype(BF)
    later = jnp.where(causal(tokens), 1.0, 0.0)
    cross = jnp.sum(last_ref[...] * incoming, axis=1, keepdims=True)
    decay_ref[...] = dot(qq_ref[...] - k * key, later, HI) + cross


def on_device(
    expert_input,
    cotangent,
    routes,
    route_weight,
    gate_weight,
    up_weight,
    down_weight,
    out_weight,
    queries,
    key_vectors,
    value_rows,
    log_decay,
    start_state,
):
    tokens = expert_input.shape[0]
    nz, nx, ny = lax.axis_size("z"), lax.axis_size("x"), lax.axis_size("y")
    spans = nz * nx
    slices = ny * 2
    core = lax.axis_index("c")
    place = lax.axis_index(("z", "x", "y", "c"))
    divide = jnp.array([1, 1, slices, slices * nx, slices, 1, 2], jnp.int32)
    wrap = jnp.array([slices, 2, spans, nz, nx, 1, 2], jnp.int32)
    at = (place // divide) % wrap
    width = queries.shape[2]
    piece_rows = slices * 128 // spans
    routes = routes.T
    route_weight = route_weight.T
    q = queries.reshape(tokens, width).T
    k = key_vectors.reshape(tokens, width).T
    v = value_rows.reshape(tokens, 128)
    g = log_decay.reshape(tokens, width).T
    slice_block = ((tokens, 128), lambda i, s: (0, s[0]))
    part = slices * 32
    part_block = ((tokens, part), lambda i, s: (0, 2 * s[6] + s[1]))

    (sent,) = call(
        dispatch_kernel,
        "dispatch",
        (sds((spans, 40, part), BF),),
        at,
        routes,
        route_weight,
        expert_input,
        cotangent,
        blocks={2: part_block, 3: part_block},
    )
    own = lax.all_to_all(sent, SP, 0, 0, tiled=True).reshape(spans * 40, part)

    weights = jnp.stack([gate_weight[0], up_weight[0]]).reshape(2, ny, 2, 128, 128)
    weights = lax.dynamic_index_in_dim(weights, 1 - core, 2, keepdims=False)
    weights = lax.ppermute(weights, "c", [(0, 1), (1, 0)])
    mixed, p, last, gc, totals = call(
        forward_kernel,
        "forward",
        (
            sds((tokens, 128), BF),
            sds((tokens, tokens), BF),
            sds((width, 128), F32),
            sds((width, tokens), F32),
            sds((8, 128), BF),
        ),
        at,
        q,
        k,
        v,
        g,
        start_state,
        after=(sent,),
    )
    own, mixed, weights = lax.optimization_barrier((own, mixed, weights))

    swap = [(0, 1), (1, 0)]
    rows_all = spans * 40
    up = [(i, (i + 1) % ny) for i in range(ny)]
    down = [(i, (i - 1) % ny) for i in range(ny)]
    low = lax.ppermute(own[: rows_all // 2], "y", up)
    high = lax.ppermute(own[rows_all // 2 :], "y", down)
    beside = lax.ppermute(own, "c", swap)

    tiles = spans // 8
    last_low = tiles // 2 - 1
    rows_block = ((320, part), lambda i, s: (i, 0))
    low_block = ((320, part), lambda i, s: (jnp.minimum(i, last_low), 0))
    high_block = ((320, part), lambda i, s: (jnp.maximum(i - last_low - 1, 0), 0))
    acc_blocks = (((320, 256), lambda i, s: (i, 0)), ((320, 128), lambda i, s: (i, 0)))
    acc = (sds((rows_all, 256), F32), sds((rows_all, 128), F32))

    def weight_blocks(first, quarter):
        return {
            first: ((1, part, 128), lambda i, s: (0, quarter(s), 0)),
            first + 1: ((1, part, 128), lambda i, s: (0, quarter(s), 0)),
            first + 2: ((1, 128, part), lambda i, s: (0, 0, quarter(s))),
        }

    experts = (gate_weight, up_weight, down_weight)
    gu, yh = call(
        first_kernel,
        "first",
        acc,
        at,
        own,
        beside,
        *experts,
        *experts,
        blocks={
            0: rows_block,
            1: rows_block,
            **weight_blocks(2, lambda s: 2 * s[6] + s[1]),
            **weight_blocks(5, lambda s: 2 * s[6] + 1 - s[1]),
        },
        out_blocks={0: acc_blocks[0], 1: acc_blocks[1]},
        grid=tiles,
    )
    low, high, gu, yh = lax.optimization_barrier((low, high, gu, yh))
    low_beside = lax.ppermute(low, "c", swap)
    high_beside = lax.ppermute(high, "c", swap)
    gu, yh = call(
        second_kernel,
        "second",
        acc,
        at,
        low,
        high,
        *experts,
        gu,
        yh,
        blocks={
            0: low_block,
            1: high_block,
            **weight_blocks(2, lambda s: 2 * (1 - s[6]) + s[1]),
            5: acc_blocks[0],
            6: acc_blocks[1],
        },
        out_blocks={0: acc_blocks[0], 1: acc_blocks[1]},
        grid=tiles,
    )
    delta, pack = call(
        delta_kernel,
        "deltas",
        (sds((rows_all, 384), BF), sds((rows_all // 2, 256), BF)),
        at,
        low_beside,
        high_beside,
        *experts,
        gu,
        yh,
        blocks={
            0: low_block,
            1: high_block,
            **weight_blocks(2, lambda s: 2 * (1 - s[6]) + 1 - s[1]),
            5: acc_blocks[0],
            6: acc_blocks[1],
        },
        out_blocks={
            0: ((320, 384), lambda i, s: (i, 0)),
            1: ((160, 256), lambda i, s: (i, 0)),
        },
        grid=tiles,
    )
    packs = lax.all_gather(pack, "c", axis=0)
    (terms,) = call(
        partial_kernel,
        "partials",
        (sds((nz, ny, nx * 20, 128), BF),),
        at,
        packs,
        gate_weight,
        up_weight,
        weights,
    )
    got = lax.all_to_all(
        terms.reshape(nz * ny, nx * 20, 128), ("z", "y"), 0, 0, tiled=True
    ).reshape(nz, ny, nx * 20, 128)
    gate_grad, up_grad, down_grad = call(
        weight_kernel,
        "weights",
        (
            sds((1, slices * 128, 128), BF),
            sds((1, slices * 128, 128), BF),
            sds((1, 128, slices * 128), BF),
        ),
        at,
        delta,
        own,
        beside,
        low,
        high,
        low_beside,
        high_beside,
        scratch=[pltpu.VMEM((384, spans * 40), BF)],
        after=(terms,),
    )
    (summed,) = call(
        sum_kernel, "sums", (sds((nx, nz, 24, 128), BF),), at, got, after=(down_grad,)
    )
    returned = lax.all_to_all(summed.reshape(nx, nz * 24, 128), "x", 0, 0, tiled=True)
    (slice_grad,) = call(
        collect_kernel,
        "collect",
        (sds((tokens, 128), BF),),
        at,
        routes,
        returned.reshape(nx, nz, 24, 128),
        cotangent,
        blocks={2: slice_block},
    )
    total_grad = lax.all_gather(slice_grad, TP, axis=0)

    rows, leaving = call(
        partial(head_kernel, piece_rows),
        "head",
        (sds((tokens, 128), BF), sds((nx, nz * piece_rows + width + 8, 128), BF)),
        at,
        total_grad,
        out_weight,
        q,
        gc,
        mixed,
        totals,
    )
    crossing = lax.all_to_all(leaving, "x", 0, 0, tiled=True)
    qraw, qq, key_local, value_local = call(
        local_kernel,
        "local",
        (
            sds((width, tokens), BF),
            sds((width, tokens), F32),
            sds((width, tokens), F32),
            sds((tokens, 128), F32),
        ),
        at,
        rows,
        q,
        k,
        v,
        gc,
        start_state,
        p,
        after=(leaving,),
    )
    inside, later, group = call(
        group_kernel,
        "group",
        (
            sds((width, 128), F32),
            sds((8, 128), F32),
            sds((nz, piece_rows + width + 8, 128), BF),
        ),
        at,
        crossing,
        after=(qq,),
    )
    group = lax.all_to_all(group, "z", 0, 0, tiled=True)
    out_grad, key, value, decay = call(
        last_kernel,
        "last",
        (
            sds((piece_rows, 128), F32),
            sds((width, tokens), BF),
            sds((tokens, 128), BF),
            sds((width, tokens), F32),
        ),
        at,
        group,
        inside,
        later,
        k,
        v,
        gc,
        last,
        qq,
        key_local,
        value_local,
    )
    return (
        gate_grad,
        up_grad,
        down_grad,
        out_grad,
        qraw.T[:, None, :],
        key.T[:, None, :],
        value[:, None, :],
        decay.T[:, None, :],
    )


def solution(mesh):
    torus = Mesh(mesh.devices.reshape(8, 4, mesh.shape["tp"] // 2, 2), ("z", "x", "y", "c"))
    in_specs = (
        P(SP, None),
        P(SP, None),
        P(SP, None),
        P(SP, None),
        P(SP, None, TP),
        P(SP, None, TP),
        P(SP, TP, None),
        P(None, TP),
        P(SP, TP, None),
        P(SP, TP, None),
        P(SP, TP, None),
        P(SP, TP, None),
        P(SP, TP, None, None),
    )
    out_specs = (
        P(SP, None, TP),
        P(SP, None, TP),
        P(SP, TP, None),
        P(SP, TP),
        P(SP, TP, None),
        P(SP, TP, None),
        P(SP, TP, None),
        P(SP, TP, None),
    )
    return jax.shard_map(
        on_device, mesh=torus, in_specs=in_specs, out_specs=out_specs, check_vma=False
    )
```

```python
from functools import partial

import jax
import jax.numpy as jnp
from jax import lax
from jax.experimental import pallas as pl
from jax.experimental.pallas import tpu as pltpu
from jax.sharding import Mesh
from jax.sharding import PartitionSpec as P

SP = ("z", "x")
TP = ("y", "c")
BF = jnp.bfloat16
F32 = jnp.float32
HI = lax.Precision.HIGHEST
BLOCK = 32
LIMIT = 56 * 1024 * 1024
SMALL = 20 * 1024 * 1024
LEAN = ('first', 'deltas', 'partials', 'sums', 'collect', 'head', 'local', 'group', 'last')
TILES = 2


def dot(a, b, precision=None):
    return lax.dot_general(
        a, b, (((1,), (0,)), ((), ())), precision=precision, preferred_element_type=F32
    )


def dot_nt(a, b, precision=None):
    return lax.dot_general(
        a, b, (((1,), (1,)), ((), ())), precision=precision, preferred_element_type=F32
    )


def dot_tn(a, b, precision=None):
    return lax.dot_general(
        a, b, (((0,), (0,)), ((), ())), precision=precision, preferred_element_type=F32
    )


def iota(shape, dim):
    return lax.broadcasted_iota(jnp.int32, shape, dim)


def call(
    kernel, name, outs, scalars, *args, blocks=None, out_blocks=None, scratch=(), after=(), grid=1
):
    blocks = blocks or {}
    out_blocks = out_blocks or {}
    specs = []
    used, waits = len(args), len(after)

    def body(at, *refs):
        kernel(at, *refs[:used], *refs[used + waits :])

    for n, a in enumerate(args):
        if n in blocks:
            specs.append(pl.BlockSpec(*blocks[n]))
        else:
            specs.append(pl.BlockSpec(a.shape, lambda i, s, nd=a.ndim: (0,) * nd))
    specs += [pl.BlockSpec(memory_space=pl.ANY)] * waits
    out_specs = tuple(
        pl.BlockSpec(*out_blocks[n])
        if n in out_blocks
        else pl.BlockSpec(o.shape, lambda i, s, nd=len(o.shape): (0,) * nd)
        for n, o in enumerate(outs)
    )
    return pl.pallas_call(
        body,
        name=name,
        out_shape=outs,
        grid_spec=pltpu.PrefetchScalarGridSpec(
            num_scalar_prefetch=1,
            grid=(grid,),
            in_specs=specs,
            out_specs=out_specs,
            scratch_shapes=list(scratch),
        ),
        compiler_params=pltpu.CompilerParams(
            vmem_limit_bytes=(SMALL if name in LEAN else LIMIT)
        ),
    )(scalars, *args, *after)


def sds(shape, dtype):
    return jax.ShapeDtypeStruct(shape, dtype)


def slots_of(routes):
    tokens = routes.shape[1]
    experts = iota((16, tokens), 0)
    r0, r1 = routes[0:1, :], routes[1:2, :]
    one0, one1 = r0 == experts, r1 == experts
    both = jnp.where(one0 | one1, 1.0, 0.0).astype(BF)
    earlier = jnp.where(iota((tokens, tokens), 0) < iota((tokens, tokens), 1), 1.0, 0.0).astype(BF)
    count = dot(both, earlier)
    s0 = jnp.sum(jnp.where(one0, count, 0.0), axis=0, keepdims=True)
    s1 = jnp.sum(jnp.where(one1, count, 0.0), axis=0, keepdims=True)
    return r0.astype(F32), r1.astype(F32), s0, s1


def column(row):
    return jnp.broadcast_to(row, (row.shape[1], row.shape[1])).T


def dispatch_kernel(at, routes_ref, weight_ref, x_ref, y_ref, out_ref):
    tokens = routes_ref.shape[1]
    r0, r1, s0, s1 = slots_of(routes_ref[...])
    key0 = r0 * 32.0 + s0
    key1 = r1 * 32.0 + s1
    y = y_ref[...].astype(F32)
    w = weight_ref[...]
    table = jnp.concatenate(
        [
            x_ref[...],
            (column(w[0:1])[:, 0:1] * y).astype(BF),
            (column(w[1:2])[:, 0:1] * y).astype(BF),
        ],
        axis=0,
    )
    q = iota((40, tokens), 0)
    is_input = q < 20
    slot = jnp.where(is_input, q, jnp.where(q < 24, q - 4, q - 24)).astype(F32)
    experts = out_ref.shape[0] // 2
    picks = []
    for e in range(experts):
        key = slot + 32.0 * e
        m0, m1 = key0 == key, key1 == key
        picks.append(
            jnp.concatenate(
                [
                    jnp.where(is_input & (m0 | m1), 1.0, 0.0),
                    jnp.where(is_input, 0.0, jnp.where(m0, 1.0, 0.0)),
                    jnp.where(is_input, 0.0, jnp.where(m1, 1.0, 0.0)),
                ],
                axis=1,
            )
        )
    pick = jnp.concatenate(picks, axis=0).astype(BF)
    for f in range(0, out_ref.shape[2], 256):
        wide = slice(f, min(f + 256, out_ref.shape[2]))
        rows = dot(pick, table[:, wide])
        for e in range(experts):
            block = rows[40 * e : 40 * e + 40].astype(BF)
            out_ref[2 * e, :, wide] = block
            out_ref[2 * e + 1, :, wide] = block


def swap_halves(a):
    return jnp.concatenate([a[4:8], a[0:4]], axis=0)


def layout_kernel(at, wg_ref, wu_ref, wd_ref, woth_ref, side_ref, back_ref):
    side_ref[:, 0:128] = wg_ref[0]
    side_ref[:, 128:256] = wu_ref[0]
    for t in range(0, side_ref.shape[0], 128):
        side_ref[t : t + 128, 256:384] = wd_ref[0, :, t : t + 128].astype(F32).T.astype(BF)
    for y in range(back_ref.shape[1] // 128):
        first = pl.multiple_of((2 * y + at[1]) * 128, 128)
        for n, w in enumerate(
            (
                wg_ref[0, pl.ds(first, 128), :],
                wu_ref[0, pl.ds(first, 128), :],
                woth_ref[0, y],
                woth_ref[1, y],
            )
        ):
            back_ref[128 * n : 128 * n + 128, 128 * y : 128 * y + 128] = w.astype(F32).T.astype(BF)


def first_kernel(at, g_ref, w_ref, out_ref):
    out_ref[...] = dot(g_ref[...], w_ref[...])


def delta_kernel(at, g_ref, w_ref, acc_ref, delta_ref, pack_ref):
    sums = dot(g_ref[...], w_ref[...]) + acc_ref[...]
    gu, yh = sums[:, 0:256], sums[:, 256:384]
    low = iota((8, 128), 0) < 4
    zero8 = jnp.zeros((8, 128), F32)
    dgs, dus, dhs, pgs, pus = [], [], [], [], []
    mixed = []
    spans = g_ref.shape[0] // 40
    for d in range(spans):
        b = 40 * d
        pg, pu = gu[b : b + 24, 0:128], gu[b : b + 24, 128:256]
        hg = jnp.concatenate([yh[b + 24 : b + 40], swap_halves(yh[b + 16 : b + 24])], axis=0)
        s = jax.nn.sigmoid(pg)
        act = pg * s
        hid = act * pu
        gd = hg * pu * s * (1.0 + pg * (1.0 - s))
        ud = hg * act
        dgs += [gd[0:16], jnp.where(low, gd[16:24], 0.0), zero8, zero8]
        dus += [ud[0:16], jnp.where(low, ud[16:24], 0.0), zero8, zero8]
        dhs += [zero8, zero8, jnp.where(low, 0.0, swap_halves(hid[16:24])), hid[0:16]]
        mixed.append((gd, ud))
    for d in range(0, spans, 2):
        for n, parts in ((0, pgs), (1, pus)):
            even, odd = mixed[d][n], mixed[d + 1][n]
            parts += [
                even[0:16],
                jnp.where(low, even[16:24], swap_halves(odd[16:24])),
                odd[0:16],
            ]
    delta_ref[:, 0:128] = jnp.concatenate(dgs, axis=0).astype(BF)
    delta_ref[:, 128:256] = jnp.concatenate(dus, axis=0).astype(BF)
    delta_ref[:, 256:384] = jnp.concatenate(dhs, axis=0).astype(BF)
    pack_ref[:, 0:128] = jnp.concatenate(pgs, axis=0).astype(BF)
    pack_ref[:, 128:256] = jnp.concatenate(pus, axis=0).astype(BF)


def partial_kernel(at, pack_ref, back_ref, out_ref):
    core = at[1]
    nz, ny, rows, _ = out_ref.shape
    lhs = jnp.concatenate([pack_ref[core], pack_ref[1 - core]], axis=1)
    for y in range(0, ny, 2):
        o = dot(lhs, back_ref[:, 128 * y : 128 * y + 256]).astype(BF)
        for z in range(nz):
            out_ref[z, y] = o[z * rows : (z + 1) * rows, 0:128]
            out_ref[z, y + 1] = o[z * rows : (z + 1) * rows, 128:256]


def weight_kernel(at, delta_ref, own_ref, other_ref, gate_ref, up_ref, down_ref, token_ref, dt_ref):
    token_ref[...] = jnp.zeros(token_ref.shape, F32)
    rows, half = own_ref.shape
    for r in range(0, rows, 128):
        dt_ref[:, r : r + 128] = delta_ref[r : r + 128, :].astype(F32).T.astype(BF)
    for g_ref, core in ((own_ref, at[1]), (other_ref, 1 - at[1])):
        for p in range(0, half, 256):
            o = dot(dt_ref[...], g_ref[:, p : p + 256])
            first = pl.multiple_of(core * half + p, 256)
            gate_ref[0, pl.ds(first, 256), :] = o[0:128].T.astype(BF)
            up_ref[0, pl.ds(first, 256), :] = o[128:256].T.astype(BF)
            down_ref[0, :, pl.ds(first, 256)] = o[256:384].astype(BF)


def sum_kernel(at, got_ref, out_ref):
    nz, ny, _, _ = got_ref.shape
    for z in range(nz):
        total = got_ref[z, 0].astype(F32)
        for y in range(1, ny):
            total = total + got_ref[z, y].astype(F32)
        for p in range(out_ref.shape[0] // 2):
            b = 40 * p
            out_ref[2 * p, z] = total[b : b + 24].astype(BF)
            out_ref[2 * p + 1, z] = jnp.concatenate(
                [total[b + 24 : b + 40], total[b + 16 : b + 24]], axis=0
            ).astype(BF)


def collect_kernel(at, routes_ref, got_ref, cot_ref, out_ref):
    nx, nz, _, _ = got_ref.shape
    routes = routes_ref[...]
    _, _, s0, s1 = slots_of(routes)
    shift = (at[4] % 2).astype(F32) * 4.0
    cols = nx * nz * 24
    lanes = iota((routes.shape[1], cols), 1).astype(F32)
    hit = None
    for n, s in ((0, s0), (1, s1)):
        half = routes[n : n + 1, :] * 2
        block = (half % nx) * nz + half // nx
        row = block.astype(F32) * 24.0 + s + jnp.where(s >= 16.0, shift, 0.0)
        first = column(row)[:, 0:1]
        match = (lanes == first) | (lanes == first + 24.0 * nz)
        hit = match if hit is None else hit | match
    pick = jnp.where(hit, 1.0, 0.0).astype(BF)
    table = got_ref[...].astype(F32).reshape(cols, 128).astype(BF)
    out_ref[...] = (cot_ref[...].astype(F32) + dot(pick, table)).astype(BF)


def block_of(shape):
    return iota(shape, 1) // BLOCK


def mids_of(gc):
    return [gc[:, b + BLOCK // 2 - 1 : b + BLOCK // 2] for b in range(0, gc.shape[1], BLOCK)]


def growth(gc):
    blocks = block_of(gc.shape)
    mid = jnp.zeros(gc.shape, F32)
    for n, m in enumerate(mids_of(gc)):
        mid = jnp.where(blocks == n, m, mid)
    return jnp.exp(gc - mid)


def causal(tokens):
    return iota((tokens, tokens), 1) <= iota((tokens, tokens), 0)


def in_parts(rows):
    high = rows.astype(BF)
    rest = rows - high.astype(F32)
    mid = rest.astype(BF)
    low = (rest - mid.astype(F32)).astype(BF)
    n = iota(rows.shape, 0)
    parts = jnp.where(n == 0, high.astype(F32), jnp.where(n == 1, mid.astype(F32), low.astype(F32)))
    return jnp.where(n < 3, parts, 0.0).astype(BF)


def columns(rows):
    rows = rows + [jnp.zeros((128 - len(rows), 128), F32)]
    return jnp.concatenate(rows, axis=0).T


def forward_kernel(at, q_ref, k_ref, v_ref, g_ref, s_ref, mixed_ref, p_ref, last_ref, gc_ref, tot_ref):
    width, tokens = q_ref.shape
    g = g_ref[...]
    before = jnp.where(iota((tokens, tokens), 0) <= iota((tokens, tokens), 1), 1.0, 0.0)
    gc = dot(g, before, HI)
    gc_ref[...] = gc
    q = q_ref[...].astype(F32) * (width**-0.5)
    k = k_ref[...].astype(F32)
    v = v_ref[...].astype(F32)
    s0 = s_ref[0, 0]
    qt = q * growth(gc)
    parts = []
    for n, mid in enumerate(mids_of(gc)):
        whole = dot_tn(qt, k * jnp.exp(jnp.minimum(mid - gc, 40.0)), HI)
        parts.append(whole[n * BLOCK : (n + 1) * BLOCK])
    p = jnp.where(causal(tokens), jnp.concatenate(parts, axis=0), 0.0)
    p_ref[...] = p.astype(BF)
    mixed_ref[...] = (dot_tn(q * jnp.exp(gc), s0, HI) + dot(p, v, HI)).astype(BF)
    end = gc[:, tokens - 1 : tokens]
    last_ref[...] = jnp.exp(end) * s0 + dot(k * jnp.exp(end - gc), v, HI)
    row = dot_nt(jnp.ones((8, tokens), F32), g, HI)
    row = jnp.concatenate([row, jnp.zeros((8, 128 - width), F32)], axis=1)
    tot_ref[...] = in_parts(row)


def head_kernel(piece, at, tg_ref, w_ref, q_ref, gc_ref, mixed_ref, tot_ref, rows_ref, send_ref):
    slices = tg_ref.shape[0]
    width = q_ref.shape[0]
    nx = send_ref.shape[0]
    tg = jnp.concatenate([tg_ref[t] for t in range(slices)], axis=1)
    rows = dot(tg, w_ref[...]).astype(BF)
    rows_ref[...] = rows
    qe = q_ref[...].astype(F32) * (width**-0.5) * jnp.exp(gc_ref[...])
    carry = dot(qe, rows.astype(F32), HI).astype(BF)
    own = send_ref.shape[1] - width - 8
    for n in range(nx):
        send_ref[n, own : own + width, :] = carry
        send_ref[n, own + width : own + width + 8, :] = tot_ref[...]
    mixed = mixed_ref[...]
    for t in range(slices):
        o = dot_tn(tg_ref[t], mixed).astype(BF)
        for r in range(0, 128, piece):
            d = (t * 128 + r) // piece
            send_ref[d % nx, (d // nx) * piece : (d // nx + 1) * piece, :] = o[r : r + piece]


def local_kernel(at, rows_ref, q_ref, k_ref, v_ref, gc_ref, s_ref, p_ref, qraw_ref, qq_ref, kl_ref, vl_ref):
    width, tokens = q_ref.shape
    scale = width**-0.5
    rows = rows_ref[...]
    gc = gc_ref[...]
    q = q_ref[...].astype(F32)
    k = k_ref[...].astype(F32)
    a = jnp.where(causal(tokens), dot_nt(rows, v_ref[...]), 0.0)
    grow = growth(gc)
    qt = q * scale * grow
    blocks = block_of(gc.shape)
    inner = jnp.zeros((width, tokens), F32)
    key_local = jnp.zeros((width, tokens), F32)
    for n, mid in enumerate(mids_of(gc)):
        fall = jnp.exp(jnp.minimum(mid - gc, 40.0))
        inner = jnp.where(blocks == n, dot_nt(k * fall, a, HI), inner)
        key_local = key_local + fall * dot(jnp.where(blocks == n, qt, 0.0), a, HI)
    qraw = scale * (jnp.exp(gc) * dot_nt(s_ref[0, 0], rows.astype(F32), HI) + grow * inner)
    qraw_ref[...] = qraw.astype(BF)
    qq_ref[...] = q * qraw
    kl_ref[...] = key_local
    vl_ref[...] = dot_tn(p_ref[...], rows)


def group_kernel(at, got_ref, inside_ref, after_ref, send_ref):
    nx, rows, _ = got_ref.shape
    nz = send_ref.shape[0]
    width = inside_ref.shape[0]
    own = rows - width - 8
    piece = own // nz
    x = at[4]
    zero = jnp.zeros((1, 128), F32)
    before, later = zero, zero
    weights, wholes = [], []
    for i in range(nx):
        weights.append(jnp.where(x < i, jnp.exp(later), 0.0))
        wholes.append(jnp.exp(before))
        part = got_ref[i, own + width : own + width + 8, :].astype(F32)
        total = jnp.sum(part, axis=0, keepdims=True)
        before = before + total
        later = later + jnp.where(x < i, total, 0.0)
    after_ref[...] = jnp.broadcast_to(later, (8, 128))
    cols = columns(weights + wholes)
    inside = jnp.zeros((width, 128), F32)
    whole = jnp.zeros((width, 128), F32)
    for i in range(nx):
        part = got_ref[i, own : own + width, :].astype(F32)
        inside = inside + cols[0:width, i : i + 1] * part
        whole = whole + cols[0:width, nx + i : nx + i + 1] * part
    inside_ref[...] = inside
    whole = whole.astype(BF)
    parts = in_parts(jnp.broadcast_to(before, (8, 128)))
    for i in range(nz):
        total = got_ref[0, i * piece : (i + 1) * piece, :].astype(F32)
        for j in range(1, nx):
            total = total + got_ref[j, i * piece : (i + 1) * piece, :].astype(F32)
        send_ref[i, 0:piece, :] = total.astype(BF)
        send_ref[i, piece : piece + width, :] = whole
        send_ref[i, piece + width : piece + width + 8, :] = parts


def last_kernel(at, got_ref, inside_ref, after_ref, k_ref, v_ref, gc_ref, last_ref, qq_ref, kl_ref, vl_ref, og_ref, key_ref, value_ref, decay_ref):
    width, tokens = k_ref.shape
    piece = og_ref.shape[0]
    z = at[3]
    sums = after_ref[0:1, :]
    weights = []
    for i in range(got_ref.shape[0]):
        weights.append(jnp.where(z < i, jnp.exp(sums), 0.0))
        part = got_ref[i, piece + width : piece + width + 8, :].astype(F32)
        sums = sums + jnp.where(z < i, jnp.sum(part, axis=0, keepdims=True), 0.0)
    cols = columns(weights)
    incoming = inside_ref[...]
    total = jnp.zeros((piece, 128), F32)
    for i in range(got_ref.shape[0]):
        total = total + got_ref[i, 0:piece, :].astype(F32)
        part = got_ref[i, piece : piece + width, :].astype(F32)
        incoming = incoming + cols[0:width, i : i + 1] * part
    og_ref[...] = total
    gc = gc_ref[...]
    k = k_ref[...].astype(F32)
    rest = jnp.exp(gc[:, tokens - 1 : tokens] - gc)
    key = kl_ref[...] + rest * dot_nt(incoming, v_ref[...].astype(F32), HI)
    key_ref[...] = key.astype(BF)
    value_ref[...] = (vl_ref[...] + dot_tn(k * rest, incoming, HI)).astype(BF)
    later = jnp.where(causal(tokens), 1.0, 0.0)
    cross = jnp.sum(last_ref[...] * incoming, axis=1, keepdims=True)
    decay_ref[...] = dot(qq_ref[...] - k * key, later, HI) + cross


def on_device(
    expert_input,
    cotangent,
    routes,
    route_weight,
    gate_weight,
    up_weight,
    down_weight,
    out_weight,
    queries,
    key_vectors,
    value_rows,
    log_decay,
    start_state,
):
    tokens = expert_input.shape[0]
    nz, nx, ny = lax.axis_size("z"), lax.axis_size("x"), lax.axis_size("y")
    spans = nz * nx
    slices = ny * 2
    core = lax.axis_index("c")
    place = lax.axis_index(("z", "x", "y", "c"))
    divide = jnp.array([1, 1, slices, slices * nx, slices, 1, 2], jnp.int32)
    wrap = jnp.array([slices, 2, spans, nz, nx, 1, 2], jnp.int32)
    at = (place // divide) % wrap
    width = queries.shape[2]
    piece_rows = slices * 128 // spans
    routes = routes.T
    route_weight = route_weight.T
    q = queries.reshape(tokens, width).T
    k = key_vectors.reshape(tokens, width).T
    v = value_rows.reshape(tokens, 128)
    g = log_decay.reshape(tokens, width).T
    slice_block = ((tokens, 128), lambda i, s: (0, s[0]))
    half = slices * 64
    half_block = ((tokens, half), lambda i, s: (0, s[1]))

    (sent,) = call(
        dispatch_kernel,
        "dispatch",
        (sds((spans, 40, half), BF),),
        at,
        routes,
        route_weight,
        expert_input,
        cotangent,
        blocks={2: half_block, 3: half_block},
    )
    own = lax.all_to_all(sent, SP, 0, 0, tiled=True).reshape(spans * 40, half)

    weights = jnp.stack([gate_weight[0], up_weight[0]]).reshape(2, ny, 2, 128, 128)
    weights = lax.dynamic_index_in_dim(weights, 1 - core, 2, keepdims=False)
    weights = lax.ppermute(weights, "c", [(0, 1), (1, 0)])
    mixed, p, last, gc, totals = call(
        forward_kernel,
        "forward",
        (
            sds((tokens, 128), BF),
            sds((tokens, tokens), BF),
            sds((width, 128), F32),
            sds((width, tokens), F32),
            sds((8, 128), BF),
        ),
        at,
        q,
        k,
        v,
        g,
        start_state,
        after=(sent,),
    )
    side, back = call(
        layout_kernel,
        "layout",
        (sds((slices * 128, 384), BF), sds((512, half), BF)),
        at,
        gate_weight,
        up_weight,
        down_weight,
        weights,
        after=(mixed,),
    )
    own, mixed, side = lax.optimization_barrier((own, mixed, side))

    other = lax.ppermute(own, "c", [(0, 1), (1, 0)])
    rows_all = spans * 40
    tile = rows_all // TILES
    rows_block = ((tile, half), lambda i, s: (i, 0))
    acc_block = ((tile, 384), lambda i, s: (i, 0))
    (acc,) = call(
        first_kernel,
        "first",
        (sds((rows_all, 384), F32),),
        at,
        own,
        side,
        blocks={0: rows_block, 1: ((half, 384), lambda i, s: (s[1], 0))},
        out_blocks={0: acc_block},
        grid=TILES,
    )
    delta, pack = call(
        delta_kernel,
        "deltas",
        (sds((rows_all, 384), BF), sds((rows_all // 2, 256), BF)),
        at,
        other,
        side,
        acc,
        blocks={
            0: rows_block,
            1: ((half, 384), lambda i, s: (1 - s[1], 0)),
            2: acc_block,
        },
        out_blocks={0: acc_block, 1: ((tile // 2, 256), lambda i, s: (i, 0))},
        grid=TILES,
    )
    packs = lax.all_gather(pack, "c", axis=0)
    (terms,) = call(
        partial_kernel,
        "partials",
        (sds((nz, ny, nx * 20, 128), BF),),
        at,
        packs,
        back,
    )
    got = lax.all_to_all(
        terms.reshape(nz * ny, nx * 20, 128), ("z", "y"), 0, 0, tiled=True
    ).reshape(nz, ny, nx * 20, 128)
    gate_grad, up_grad, down_grad, token = call(
        weight_kernel,
        "weights",
        (
            sds((1, slices * 128, 128), BF),
            sds((1, slices * 128, 128), BF),
            sds((1, 128, slices * 128), BF),
            sds((8, 128), F32),
        ),
        at,
        delta,
        own,
        other,
        scratch=[pltpu.VMEM((384, spans * 40), BF)],
        after=(terms,),
    )
    (summed,) = call(
        sum_kernel, "sums", (sds((nx, nz, 24, 128), BF),), at, got, after=(token,)
    )
    returned = lax.all_to_all(summed.reshape(nx, nz * 24, 128), "x", 0, 0, tiled=True)
    (slice_grad,) = call(
        collect_kernel,
        "collect",
        (sds((tokens, 128), BF),),
        at,
        routes,
        returned.reshape(nx, nz, 24, 128),
        cotangent,
        blocks={2: slice_block},
    )
    total_grad = lax.all_gather(slice_grad, TP, axis=0)

    rows, leaving = call(
        partial(head_kernel, piece_rows),
        "head",
        (sds((tokens, 128), BF), sds((nx, nz * piece_rows + width + 8, 128), BF)),
        at,
        total_grad,
        out_weight,
        q,
        gc,
        mixed,
        totals,
    )
    crossing = lax.all_to_all(leaving, "x", 0, 0, tiled=True)
    qraw, qq, key_local, value_local = call(
        local_kernel,
        "local",
        (
            sds((width, tokens), BF),
            sds((width, tokens), F32),
            sds((width, tokens), F32),
            sds((tokens, 128), F32),
        ),
        at,
        rows,
        q,
        k,
        v,
        gc,
        start_state,
        p,
        after=(leaving,),
    )
    inside, later, group = call(
        group_kernel,
        "group",
        (
            sds((width, 128), F32),
            sds((8, 128), F32),
            sds((nz, piece_rows + width + 8, 128), BF),
        ),
        at,
        crossing,
        after=(qq,),
    )
    group = lax.all_to_all(group, "z", 0, 0, tiled=True)
    out_grad, key, value, decay = call(
        last_kernel,
        "last",
        (
            sds((piece_rows, 128), F32),
            sds((width, tokens), BF),
            sds((tokens, 128), BF),
            sds((width, tokens), F32),
        ),
        at,
        group,
        inside,
        later,
        k,
        v,
        gc,
        last,
        qq,
        key_local,
        value_local,
    )
    return (
        gate_grad,
        up_grad,
        down_grad,
        out_grad,
        qraw.T[:, None, :],
        key.T[:, None, :],
        value[:, None, :],
        decay.T[:, None, :],
    )


def solution(mesh):
    torus = Mesh(mesh.devices.reshape(8, 4, mesh.shape["tp"] // 2, 2), ("z", "x", "y", "c"))
    in_specs = (
        P(SP, None),
        P(SP, None),
        P(SP, None),
        P(SP, None),
        P(SP, None, TP),
        P(SP, None, TP),
        P(SP, TP, None),
        P(None, TP),
        P(SP, TP, None),
        P(SP, TP, None),
        P(SP, TP, None),
        P(SP, TP, None),
        P(SP, TP, None, None),
    )
    out_specs = (
        P(SP, None, TP),
        P(SP, None, TP),
        P(SP, TP, None),
        P(SP, TP),
        P(SP, TP, None),
        P(SP, TP, None),
        P(SP, TP, None),
        P(SP, TP, None),
    )
    return jax.shard_map(
        on_device, mesh=torus, in_specs=in_specs, out_specs=out_specs, check_vma=False
    )
```

```python
from functools import partial

import jax
import jax.numpy as jnp
from jax import lax
from jax.experimental import pallas as pl
from jax.experimental.pallas import tpu as pltpu
from jax.sharding import Mesh
from jax.sharding import PartitionSpec as P

SP = ("z", "x")
TP = ("y", "c")
BF = jnp.bfloat16
F32 = jnp.float32
HI = lax.Precision.HIGHEST
BLOCK = 32
LIMIT = 56 * 1024 * 1024
SMALL = 20 * 1024 * 1024
LEAN = ('first', 'deltas', 'partials', 'sums', 'collect', 'head', 'local', 'group', 'last')
TILES = 2


def dot(a, b, precision=None):
    return lax.dot_general(
        a, b, (((1,), (0,)), ((), ())), precision=precision, preferred_element_type=F32
    )


def dot_nt(a, b, precision=None):
    return lax.dot_general(
        a, b, (((1,), (1,)), ((), ())), precision=precision, preferred_element_type=F32
    )


def dot_tn(a, b, precision=None):
    return lax.dot_general(
        a, b, (((0,), (0,)), ((), ())), precision=precision, preferred_element_type=F32
    )


def iota(shape, dim):
    return lax.broadcasted_iota(jnp.int32, shape, dim)


def call(
    kernel, name, outs, scalars, *args, blocks=None, out_blocks=None, scratch=(), after=(), grid=1
):
    blocks = blocks or {}
    out_blocks = out_blocks or {}
    specs = []
    used, waits = len(args), len(after)

    def body(at, *refs):
        kernel(at, *refs[:used], *refs[used + waits :])

    for n, a in enumerate(args):
        if n in blocks:
            specs.append(pl.BlockSpec(*blocks[n]))
        else:
            specs.append(pl.BlockSpec(a.shape, lambda i, s, nd=a.ndim: (0,) * nd))
    specs += [pl.BlockSpec(memory_space=pl.ANY)] * waits
    out_specs = tuple(
        pl.BlockSpec(*out_blocks[n])
        if n in out_blocks
        else pl.BlockSpec(o.shape, lambda i, s, nd=len(o.shape): (0,) * nd)
        for n, o in enumerate(outs)
    )
    return pl.pallas_call(
        body,
        name=name,
        out_shape=outs,
        grid_spec=pltpu.PrefetchScalarGridSpec(
            num_scalar_prefetch=1,
            grid=(grid,),
            in_specs=specs,
            out_specs=out_specs,
            scratch_shapes=list(scratch),
        ),
        compiler_params=pltpu.CompilerParams(
            vmem_limit_bytes=(SMALL if name in LEAN else LIMIT)
        ),
    )(scalars, *args, *after)


def sds(shape, dtype):
    return jax.ShapeDtypeStruct(shape, dtype)


def slots_of(routes):
    tokens = routes.shape[1]
    experts = iota((16, tokens), 0)
    r0, r1 = routes[0:1, :], routes[1:2, :]
    one0, one1 = r0 == experts, r1 == experts
    both = jnp.where(one0 | one1, 1.0, 0.0).astype(BF)
    earlier = jnp.where(iota((tokens, tokens), 0) < iota((tokens, tokens), 1), 1.0, 0.0).astype(BF)
    count = dot(both, earlier)
    s0 = jnp.sum(jnp.where(one0, count, 0.0), axis=0, keepdims=True)
    s1 = jnp.sum(jnp.where(one1, count, 0.0), axis=0, keepdims=True)
    return r0.astype(F32), r1.astype(F32), s0, s1


def column(row):
    return jnp.broadcast_to(row, (row.shape[1], row.shape[1])).T


def dispatch_kernel(at, routes_ref, weight_ref, *refs):
    out_ref = refs[-1]
    blocks = (len(refs) - 1) // 2
    tokens = routes_ref.shape[1]
    r0, r1, s0, s1 = slots_of(routes_ref[...])
    key0 = r0 * 32.0 + s0
    key1 = r1 * 32.0 + s1
    w = weight_ref[...]
    w0, w1 = column(w[0:1])[:, 0:1], column(w[1:2])[:, 0:1]
    q = iota((40, tokens), 0)
    is_input = q < 20
    slot = jnp.where(is_input, q, jnp.where(q < 24, q - 4, q - 24)).astype(F32)
    experts = out_ref.shape[0] // 2
    picks = []
    for e in range(experts):
        key = slot + 32.0 * e
        m0, m1 = key0 == key, key1 == key
        picks.append(
            jnp.concatenate(
                [
                    jnp.where(is_input & (m0 | m1), 1.0, 0.0),
                    jnp.where(is_input, 0.0, jnp.where(m0, 1.0, 0.0)),
                    jnp.where(is_input, 0.0, jnp.where(m1, 1.0, 0.0)),
                ],
                axis=1,
            )
        )
    pick = jnp.concatenate(picks, axis=0).astype(BF)
    for n in range(blocks):
        y = refs[blocks + n][...].astype(F32)
        table = jnp.concatenate([refs[n][...], (w0 * y).astype(BF), (w1 * y).astype(BF)], axis=0)
        rows = dot(pick, table)
        wide = slice(n * rows.shape[1], (n + 1) * rows.shape[1])
        for e in range(experts):
            block = rows[40 * e : 40 * e + 40].astype(BF)
            out_ref[2 * e, :, wide] = block
            out_ref[2 * e + 1, :, wide] = block


def swap_halves(a):
    return jnp.concatenate([a[4:8], a[0:4]], axis=0)


def layout_kernel(at, wg_ref, wu_ref, wd_ref, woth_ref, side_ref, back_ref):
    quarter = side_ref.shape[0] // 8
    for n in range(8):
        core = at[1] if n < 4 else 1 - at[1]
        first = pl.multiple_of((core * 4 + quarter_at(n % 4, at[5])) * quarter, 128)
        to = slice(n * quarter, (n + 1) * quarter)
        side_ref[to, 0:128] = wg_ref[0, pl.ds(first, quarter), :]
        side_ref[to, 128:256] = wu_ref[0, pl.ds(first, quarter), :]
        side_ref[to, 256:384] = wd_ref[0, :, pl.ds(first, quarter)].astype(F32).T.astype(BF)
    for y in range(back_ref.shape[1] // 128):
        first = pl.multiple_of((2 * y + at[1]) * 128, 128)
        for n, w in enumerate(
            (
                wg_ref[0, pl.ds(first, 128), :],
                wu_ref[0, pl.ds(first, 128), :],
                woth_ref[0, y],
                woth_ref[1, y],
            )
        ):
            back_ref[128 * n : 128 * n + 128, 128 * y : 128 * y + 128] = w.astype(F32).T.astype(BF)


def quarter_at(n, side):
    if n == 0:
        return 3 - 3 * side
    return 3 * side if n == 3 else n


def first_kernel(at, own_ref, other_ref, w_ref, out_ref):
    most = own_ref.shape[1]
    half = w_ref.shape[0] // 2
    out_ref[...] = dot(own_ref[...], w_ref[0:most, :]) + dot(
        other_ref[...], w_ref[half : half + most, :]
    )


def delta_kernel(at, rest_ref, beside_ref, w_ref, acc_ref, delta_ref, pack_ref):
    half = w_ref.shape[0] // 2
    most = half - rest_ref.shape[1]
    sums = acc_ref[...] + dot(rest_ref[...], w_ref[most:half, :])
    sums = sums + dot(beside_ref[...], w_ref[half + most :, :])
    gu, yh = sums[:, 0:256], sums[:, 256:384]
    low = iota((8, 128), 0) < 4
    zero8 = jnp.zeros((8, 128), F32)
    dgs, dus, dhs, pgs, pus = [], [], [], [], []
    mixed = []
    spans = rest_ref.shape[0] // 40
    for d in range(spans):
        b = 40 * d
        pg, pu = gu[b : b + 24, 0:128], gu[b : b + 24, 128:256]
        hg = jnp.concatenate([yh[b + 24 : b + 40], swap_halves(yh[b + 16 : b + 24])], axis=0)
        s = jax.nn.sigmoid(pg)
        act = pg * s
        hid = act * pu
        gd = hg * pu * s * (1.0 + pg * (1.0 - s))
        ud = hg * act
        dgs += [gd[0:16], jnp.where(low, gd[16:24], 0.0), zero8, zero8]
        dus += [ud[0:16], jnp.where(low, ud[16:24], 0.0), zero8, zero8]
        dhs += [zero8, zero8, jnp.where(low, 0.0, swap_halves(hid[16:24])), hid[0:16]]
        mixed.append((gd, ud))
    for d in range(0, spans, 2):
        for n, parts in ((0, pgs), (1, pus)):
            even, odd = mixed[d][n], mixed[d + 1][n]
            parts += [
                even[0:16],
                jnp.where(low, even[16:24], swap_halves(odd[16:24])),
                odd[0:16],
            ]
    delta_ref[:, 0:128] = jnp.concatenate(dgs, axis=0).astype(BF)
    delta_ref[:, 128:256] = jnp.concatenate(dus, axis=0).astype(BF)
    delta_ref[:, 256:384] = jnp.concatenate(dhs, axis=0).astype(BF)
    pack_ref[:, 0:128] = jnp.concatenate(pgs, axis=0).astype(BF)
    pack_ref[:, 128:256] = jnp.concatenate(pus, axis=0).astype(BF)


def partial_kernel(at, pack_ref, back_ref, out_ref):
    core = at[1]
    nz, ny, rows, _ = out_ref.shape
    lhs = jnp.concatenate([pack_ref[core], pack_ref[1 - core]], axis=1)
    for y in range(0, ny, 2):
        o = dot(lhs, back_ref[:, 128 * y : 128 * y + 256]).astype(BF)
        for z in range(nz):
            out_ref[z, y] = o[z * rows : (z + 1) * rows, 0:128]
            out_ref[z, y + 1] = o[z * rows : (z + 1) * rows, 128:256]


def weight_kernel(at, delta_ref, own_ref, other_ref, rest_ref, beside_ref, gate_ref, up_ref, down_ref, token_ref, dt_ref):
    token_ref[...] = jnp.zeros(token_ref.shape, F32)
    rows, quarter = rest_ref.shape
    for r in range(0, rows, 128):
        dt_ref[:, r : r + 128] = delta_ref[r : r + 128, :].astype(F32).T.astype(BF)
    for most_ref, last_ref, core in ((own_ref, rest_ref, at[1]), (other_ref, beside_ref, 1 - at[1])):
        for n in range(4):
            g = last_ref[...] if n == 3 else most_ref[:, n * quarter : (n + 1) * quarter]
            o = dot(dt_ref[...], g)
            first = pl.multiple_of((core * 4 + quarter_at(n, at[5])) * quarter, 128)
            gate_ref[0, pl.ds(first, quarter), :] = o[0:128].T.astype(BF)
            up_ref[0, pl.ds(first, quarter), :] = o[128:256].T.astype(BF)
            down_ref[0, :, pl.ds(first, quarter)] = o[256:384].astype(BF)


def sum_kernel(at, got_ref, out_ref):
    nz, ny, _, _ = got_ref.shape
    for z in range(nz):
        total = got_ref[z, 0].astype(F32)
        for y in range(1, ny):
            total = total + got_ref[z, y].astype(F32)
        for p in range(out_ref.shape[0] // 2):
            b = 40 * p
            out_ref[2 * p, z] = total[b : b + 24].astype(BF)
            out_ref[2 * p + 1, z] = jnp.concatenate(
                [total[b + 24 : b + 40], total[b + 16 : b + 24]], axis=0
            ).astype(BF)


def collect_kernel(at, routes_ref, got_ref, cot_ref, out_ref):
    nx, nz, _, _ = got_ref.shape
    routes = routes_ref[...]
    _, _, s0, s1 = slots_of(routes)
    shift = (at[4] % 2).astype(F32) * 4.0
    cols = nx * nz * 24
    lanes = iota((routes.shape[1], cols), 1).astype(F32)
    hit = None
    for n, s in ((0, s0), (1, s1)):
        half = routes[n : n + 1, :] * 2
        block = (half % nx) * nz + half // nx
        row = block.astype(F32) * 24.0 + s + jnp.where(s >= 16.0, shift, 0.0)
        first = column(row)[:, 0:1]
        match = (lanes == first) | (lanes == first + 24.0 * nz)
        hit = match if hit is None else hit | match
    pick = jnp.where(hit, 1.0, 0.0).astype(BF)
    table = got_ref[...].astype(F32).reshape(cols, 128).astype(BF)
    out_ref[...] = (cot_ref[...].astype(F32) + dot(pick, table)).astype(BF)


def block_of(shape):
    return iota(shape, 1) // BLOCK


def mids_of(gc):
    return [gc[:, b + BLOCK // 2 - 1 : b + BLOCK // 2] for b in range(0, gc.shape[1], BLOCK)]


def growth(gc):
    blocks = block_of(gc.shape)
    mid = jnp.zeros(gc.shape, F32)
    for n, m in enumerate(mids_of(gc)):
        mid = jnp.where(blocks == n, m, mid)
    return jnp.exp(gc - mid)


def causal(tokens):
    return iota((tokens, tokens), 1) <= iota((tokens, tokens), 0)


def in_parts(rows):
    high = rows.astype(BF)
    rest = rows - high.astype(F32)
    mid = rest.astype(BF)
    low = (rest - mid.astype(F32)).astype(BF)
    n = iota(rows.shape, 0)
    parts = jnp.where(n == 0, high.astype(F32), jnp.where(n == 1, mid.astype(F32), low.astype(F32)))
    return jnp.where(n < 3, parts, 0.0).astype(BF)


def columns(rows):
    rows = rows + [jnp.zeros((128 - len(rows), 128), F32)]
    return jnp.concatenate(rows, axis=0).T


def forward_kernel(at, q_ref, k_ref, v_ref, g_ref, s_ref, mixed_ref, p_ref, last_ref, gc_ref, tot_ref):
    width, tokens = q_ref.shape
    g = g_ref[...]
    before = jnp.where(iota((tokens, tokens), 0) <= iota((tokens, tokens), 1), 1.0, 0.0)
    gc = dot(g, before, HI)
    gc_ref[...] = gc
    q = q_ref[...].astype(F32) * (width**-0.5)
    k = k_ref[...].astype(F32)
    v = v_ref[...].astype(F32)
    s0 = s_ref[0, 0]
    qt = q * growth(gc)
    parts = []
    for n, mid in enumerate(mids_of(gc)):
        whole = dot_tn(qt, k * jnp.exp(jnp.minimum(mid - gc, 40.0)), HI)
        parts.append(whole[n * BLOCK : (n + 1) * BLOCK])
    p = jnp.where(causal(tokens), jnp.concatenate(parts, axis=0), 0.0)
    p_ref[...] = p.astype(BF)
    mixed_ref[...] = (dot_tn(q * jnp.exp(gc), s0, HI) + dot(p, v, HI)).astype(BF)
    end = gc[:, tokens - 1 : tokens]
    last_ref[...] = jnp.exp(end) * s0 + dot(k * jnp.exp(end - gc), v, HI)
    row = dot_nt(jnp.ones((8, tokens), F32), g, HI)
    row = jnp.concatenate([row, jnp.zeros((8, 128 - width), F32)], axis=1)
    tot_ref[...] = in_parts(row)


def head_kernel(piece, at, tg_ref, w_ref, q_ref, gc_ref, mixed_ref, tot_ref, rows_ref, send_ref):
    slices = tg_ref.shape[0]
    width = q_ref.shape[0]
    nx = send_ref.shape[0]
    tg = jnp.concatenate([tg_ref[t] for t in range(slices)], axis=1)
    rows = dot(tg, w_ref[...]).astype(BF)
    rows_ref[...] = rows
    qe = q_ref[...].astype(F32) * (width**-0.5) * jnp.exp(gc_ref[...])
    carry = dot(qe, rows.astype(F32), HI).astype(BF)
    own = send_ref.shape[1] - width - 8
    for n in range(nx):
        send_ref[n, own : own + width, :] = carry
        send_ref[n, own + width : own + width + 8, :] = tot_ref[...]
    mixed = mixed_ref[...]
    for t in range(slices):
        o = dot_tn(tg_ref[t], mixed).astype(BF)
        for r in range(0, 128, piece):
            d = (t * 128 + r) // piece
            send_ref[d % nx, (d // nx) * piece : (d // nx + 1) * piece, :] = o[r : r + piece]


def local_kernel(at, rows_ref, q_ref, k_ref, v_ref, gc_ref, s_ref, p_ref, qraw_ref, qq_ref, kl_ref, vl_ref):
    width, tokens = q_ref.shape
    scale = width**-0.5
    rows = rows_ref[...]
    gc = gc_ref[...]
    q = q_ref[...].astype(F32)
    k = k_ref[...].astype(F32)
    a = jnp.where(causal(tokens), dot_nt(rows, v_ref[...]), 0.0)
    grow = growth(gc)
    qt = q * scale * grow
    blocks = block_of(gc.shape)
    inner = jnp.zeros((width, tokens), F32)
    key_local = jnp.zeros((width, tokens), F32)
    for n, mid in enumerate(mids_of(gc)):
        fall = jnp.exp(jnp.minimum(mid - gc, 40.0))
        inner = jnp.where(blocks == n, dot_nt(k * fall, a, HI), inner)
        key_local = key_local + fall * dot(jnp.where(blocks == n, qt, 0.0), a, HI)
    qraw = scale * (jnp.exp(gc) * dot_nt(s_ref[0, 0], rows.astype(F32), HI) + grow * inner)
    qraw_ref[...] = qraw.astype(BF)
    qq_ref[...] = q * qraw
    kl_ref[...] = key_local
    vl_ref[...] = dot_tn(p_ref[...], rows)


def group_kernel(at, got_ref, inside_ref, after_ref, send_ref):
    nx, rows, _ = got_ref.shape
    nz = send_ref.shape[0]
    width = inside_ref.shape[0]
    own = rows - width - 8
    piece = own // nz
    x = at[4]
    zero = jnp.zeros((1, 128), F32)
    before, later = zero, zero
    weights, wholes = [], []
    for i in range(nx):
        weights.append(jnp.where(x < i, jnp.exp(later), 0.0))
        wholes.append(jnp.exp(before))
        part = got_ref[i, own + width : own + width + 8, :].astype(F32)
        total = jnp.sum(part, axis=0, keepdims=True)
        before = before + total
        later = later + jnp.where(x < i, total, 0.0)
    after_ref[...] = jnp.broadcast_to(later, (8, 128))
    cols = columns(weights + wholes)
    inside = jnp.zeros((width, 128), F32)
    whole = jnp.zeros((width, 128), F32)
    for i in range(nx):
        part = got_ref[i, own : own + width, :].astype(F32)
        inside = inside + cols[0:width, i : i + 1] * part
        whole = whole + cols[0:width, nx + i : nx + i + 1] * part
    inside_ref[...] = inside
    whole = whole.astype(BF)
    parts = in_parts(jnp.broadcast_to(before, (8, 128)))
    for i in range(nz):
        total = got_ref[0, i * piece : (i + 1) * piece, :].astype(F32)
        for j in range(1, nx):
            total = total + got_ref[j, i * piece : (i + 1) * piece, :].astype(F32)
        send_ref[i, 0:piece, :] = total.astype(BF)
        send_ref[i, piece : piece + width, :] = whole
        send_ref[i, piece + width : piece + width + 8, :] = parts


def last_kernel(at, got_ref, inside_ref, after_ref, k_ref, v_ref, gc_ref, last_ref, qq_ref, kl_ref, vl_ref, og_ref, key_ref, value_ref, decay_ref):
    width, tokens = k_ref.shape
    piece = og_ref.shape[0]
    z = at[3]
    sums = after_ref[0:1, :]
    weights = []
    for i in range(got_ref.shape[0]):
        weights.append(jnp.where(z < i, jnp.exp(sums), 0.0))
        part = got_ref[i, piece + width : piece + width + 8, :].astype(F32)
        sums = sums + jnp.where(z < i, jnp.sum(part, axis=0, keepdims=True), 0.0)
    cols = columns(weights)
    incoming = inside_ref[...]
    total = jnp.zeros((piece, 128), F32)
    for i in range(got_ref.shape[0]):
        total = total + got_ref[i, 0:piece, :].astype(F32)
        part = got_ref[i, piece : piece + width, :].astype(F32)
        incoming = incoming + cols[0:width, i : i + 1] * part
    og_ref[...] = total
    gc = gc_ref[...]
    k = k_ref[...].astype(F32)
    rest = jnp.exp(gc[:, tokens - 1 : tokens] - gc)
    key = kl_ref[...] + rest * dot_nt(incoming, v_ref[...].astype(F32), HI)
    key_ref[...] = key.astype(BF)
    value_ref[...] = (vl_ref[...] + dot_tn(k * rest, incoming, HI)).astype(BF)
    later = jnp.where(causal(tokens), 1.0, 0.0)
    cross = jnp.sum(last_ref[...] * incoming, axis=1, keepdims=True)
    decay_ref[...] = dot(qq_ref[...] - k * key, later, HI) + cross


def on_device(
    expert_input,
    cotangent,
    routes,
    route_weight,
    gate_weight,
    up_weight,
    down_weight,
    out_weight,
    queries,
    key_vectors,
    value_rows,
    log_decay,
    start_state,
):
    tokens = expert_input.shape[0]
    nz, nx, ny = lax.axis_size("z"), lax.axis_size("x"), lax.axis_size("y")
    spans = nz * nx
    slices = ny * 2
    core = lax.axis_index("c")
    place = lax.axis_index(("z", "x", "y", "c"))
    sizes = ((1, slices), (1, 2), (slices, spans), (slices * nx, nz), (slices, nx), (2, 2))
    shifts = jnp.array([(d).bit_length() - 1 for d, _ in sizes], jnp.int32)
    masks = jnp.array([n - 1 for _, n in sizes], jnp.int32)
    at = lax.shift_right_logical(jnp.broadcast_to(place, shifts.shape), shifts) & masks
    width = queries.shape[2]
    piece_rows = slices * 128 // spans
    routes = routes.T
    route_weight = route_weight.T
    q = queries.reshape(tokens, width).T
    k = key_vectors.reshape(tokens, width).T
    v = value_rows.reshape(tokens, 128)
    g = log_decay.reshape(tokens, width).T
    slice_block = ((tokens, 128), lambda i, s: (0, s[0]))
    half = slices * 64
    quarter = half // 4
    most = half - quarter

    def features(n):
        return ((tokens, quarter), lambda i, s: (0, s[1] * 4 + quarter_at(n, s[5])))


    (sent,) = call(
        dispatch_kernel,
        "dispatch",
        (sds((spans, 40, most), BF),),
        at,
        routes,
        route_weight,
        *[expert_input] * 3,
        *[cotangent] * 3,
        blocks={2 + n: features(n % 3) for n in range(6)},
    )
    own = lax.all_to_all(sent, SP, 0, 0, tiled=True).reshape(spans * 40, most)

    weights = jnp.stack([gate_weight[0], up_weight[0]]).reshape(2, ny, 2, 128, 128)
    weights = lax.dynamic_index_in_dim(weights, 1 - core, 2, keepdims=False)
    weights = lax.ppermute(weights, "c", [(0, 1), (1, 0)])
    mixed, p, last, gc, totals = call(
        forward_kernel,
        "forward",
        (
            sds((tokens, 128), BF),
            sds((tokens, tokens), BF),
            sds((width, 128), F32),
            sds((width, tokens), F32),
            sds((8, 128), BF),
        ),
        at,
        q,
        k,
        v,
        g,
        start_state,
        after=(sent,),
    )
    side, back = call(
        layout_kernel,
        "layout",
        (sds((slices * 128, 384), BF), sds((512, half), BF)),
        at,
        gate_weight,
        up_weight,
        down_weight,
        weights,
        after=(mixed,),
    )
    own, mixed, side = lax.optimization_barrier((own, mixed, side))

    rows_all = spans * 40
    swap = [(0, 1), (1, 0)]
    up = [(i, (i + 1) % ny) for i in range(ny)]
    down = [(i, (i - 1) % ny) for i in range(ny)]
    low = lax.ppermute(own[: rows_all // 2, :quarter], "y", up)
    high = lax.ppermute(own[rows_all // 2 :, :quarter], "y", down)
    other = lax.ppermute(own, "c", swap)
    tile = rows_all // TILES
    most_block = ((tile, most), lambda i, s: (i, 0))
    rest_block = ((tile, quarter), lambda i, s: (i, 0))
    acc_block = ((tile, 384), lambda i, s: (i, 0))
    (acc,) = call(
        first_kernel,
        "first",
        (sds((rows_all, 384), F32),),
        at,
        own,
        other,
        side,
        blocks={0: most_block, 1: most_block},
        out_blocks={0: acc_block},
        grid=TILES,
    )
    low, high, acc = lax.optimization_barrier((low, high, acc))
    rest = jnp.concatenate([low, high], axis=0)
    beside = lax.ppermute(rest, "c", swap)
    delta, pack = call(
        delta_kernel,
        "deltas",
        (sds((rows_all, 384), BF), sds((rows_all // 2, 256), BF)),
        at,
        rest,
        beside,
        side,
        acc,
        blocks={0: rest_block, 1: rest_block, 3: acc_block},
        out_blocks={0: acc_block, 1: ((tile // 2, 256), lambda i, s: (i, 0))},
        grid=TILES,
    )
    packs = lax.all_gather(pack, "c", axis=0)
    (terms,) = call(
        partial_kernel,
        "partials",
        (sds((nz, ny, nx * 20, 128), BF),),
        at,
        packs,
        back,
    )
    got = lax.all_to_all(
        terms.reshape(nz * ny, nx * 20, 128), ("z", "y"), 0, 0, tiled=True
    ).reshape(nz, ny, nx * 20, 128)
    gate_grad, up_grad, down_grad, token = call(
        weight_kernel,
        "weights",
        (
            sds((1, slices * 128, 128), BF),
            sds((1, slices * 128, 128), BF),
            sds((1, 128, slices * 128), BF),
            sds((8, 128), F32),
        ),
        at,
        delta,
        own,
        other,
        rest,
        beside,
        scratch=[pltpu.VMEM((384, spans * 40), BF)],
        after=(terms,),
    )
    got, token = lax.optimization_barrier((got, token))
    (summed,) = call(sum_kernel, "sums", (sds((nx, nz, 24, 128), BF),), at, got)
    returned = lax.all_to_all(summed.reshape(nx, nz * 24, 128), "x", 0, 0, tiled=True)
    (slice_grad,) = call(
        collect_kernel,
        "collect",
        (sds((tokens, 128), BF),),
        at,
        routes,
        returned.reshape(nx, nz, 24, 128),
        cotangent,
        blocks={2: slice_block},
    )
    total_grad = lax.all_gather(slice_grad, TP, axis=0)

    rows, leaving = call(
        partial(head_kernel, piece_rows),
        "head",
        (sds((tokens, 128), BF), sds((nx, nz * piece_rows + width + 8, 128), BF)),
        at,
        total_grad,
        out_weight,
        q,
        gc,
        mixed,
        totals,
    )
    crossing = lax.all_to_all(leaving, "x", 0, 0, tiled=True)
    qraw, qq, key_local, value_local = call(
        local_kernel,
        "local",
        (
            sds((width, tokens), BF),
            sds((width, tokens), F32),
            sds((width, tokens), F32),
            sds((tokens, 128), F32),
        ),
        at,
        rows,
        q,
        k,
        v,
        gc,
        start_state,
        p,
        after=(leaving,),
    )
    inside, later, group = call(
        group_kernel,
        "group",
        (
            sds((width, 128), F32),
            sds((8, 128), F32),
            sds((nz, piece_rows + width + 8, 128), BF),
        ),
        at,
        crossing,
        after=(qq,),
    )
    group = lax.all_to_all(group, "z", 0, 0, tiled=True)
    out_grad, key, value, decay = call(
        last_kernel,
        "last",
        (
            sds((piece_rows, 128), F32),
            sds((width, tokens), BF),
            sds((tokens, 128), BF),
            sds((width, tokens), F32),
        ),
        at,
        group,
        inside,
        later,
        k,
        v,
        gc,
        last,
        qq,
        key_local,
        value_local,
    )
    return (
        gate_grad,
        up_grad,
        down_grad,
        out_grad,
        qraw.T[:, None, :],
        key.T[:, None, :],
        value[:, None, :],
        decay.T[:, None, :],
    )


def solution(mesh):
    torus = Mesh(mesh.devices.reshape(8, 4, mesh.shape["tp"] // 2, 2), ("z", "x", "y", "c"))
    in_specs = (
        P(SP, None),
        P(SP, None),
        P(SP, None),
        P(SP, None),
        P(SP, None, TP),
        P(SP, None, TP),
        P(SP, TP, None),
        P(None, TP),
        P(SP, TP, None),
        P(SP, TP, None),
        P(SP, TP, None),
        P(SP, TP, None),
        P(SP, TP, None, None),
    )
    out_specs = (
        P(SP, None, TP),
        P(SP, None, TP),
        P(SP, TP, None),
        P(SP, TP),
        P(SP, TP, None),
        P(SP, TP, None),
        P(SP, TP, None),
        P(SP, TP, None),
    )
    return jax.shard_map(
        on_device, mesh=torus, in_specs=in_specs, out_specs=out_specs, check_vma=False
    )
```

```python
from functools import partial

import jax
import jax.numpy as jnp
from jax import lax
from jax.experimental import pallas as pl
from jax.experimental.pallas import tpu as pltpu
from jax.sharding import Mesh
from jax.sharding import PartitionSpec as P

SP = ("z", "x")
TP = ("y", "c")
BF = jnp.bfloat16
F32 = jnp.float32
HI = lax.Precision.HIGHEST
BLOCK = 32
LIMIT = 56 * 1024 * 1024
SMALL = 20 * 1024 * 1024
LEAN = ('first', 'deltas', 'partials', 'sums', 'collect', 'head', 'local', 'group', 'last')
TILES = 2


def dot(a, b, precision=None):
    return lax.dot_general(
        a, b, (((1,), (0,)), ((), ())), precision=precision, preferred_element_type=F32
    )


def dot_nt(a, b, precision=None):
    return lax.dot_general(
        a, b, (((1,), (1,)), ((), ())), precision=precision, preferred_element_type=F32
    )


def dot_tn(a, b, precision=None):
    return lax.dot_general(
        a, b, (((0,), (0,)), ((), ())), precision=precision, preferred_element_type=F32
    )


def iota(shape, dim):
    return lax.broadcasted_iota(jnp.int32, shape, dim)


class Place:
    def __init__(self, number, sizes):
        self.number, self.sizes = number, sizes

    def __getitem__(self, k):
        step, count = self.sizes[k]
        return lax.shift_right_logical(self.number[0], step.bit_length() - 1) & (count - 1)


def call(
    kernel, name, outs, scalars, *args, blocks=None, out_blocks=None, scratch=(), after=(), grid=1
):
    blocks = blocks or {}
    out_blocks = out_blocks or {}
    specs = []
    used, waits = len(args), len(after)

    def body(number, *refs):
        kernel(Place(number, scalars.sizes), *refs[:used], *refs[used + waits :])

    def placed(index):
        return lambda i, s: index(i, Place(s, scalars.sizes))

    for n, a in enumerate(args):
        if n in blocks:
            specs.append(pl.BlockSpec(blocks[n][0], placed(blocks[n][1])))
        else:
            specs.append(pl.BlockSpec(a.shape, lambda i, s, nd=a.ndim: (0,) * nd))
    specs += [pl.BlockSpec(memory_space=pl.ANY)] * waits
    out_specs = tuple(
        pl.BlockSpec(out_blocks[n][0], placed(out_blocks[n][1]))
        if n in out_blocks
        else pl.BlockSpec(o.shape, lambda i, s, nd=len(o.shape): (0,) * nd)
        for n, o in enumerate(outs)
    )
    return pl.pallas_call(
        body,
        name=name,
        out_shape=outs,
        grid_spec=pltpu.PrefetchScalarGridSpec(
            num_scalar_prefetch=1,
            grid=(grid,),
            in_specs=specs,
            out_specs=out_specs,
            scratch_shapes=list(scratch),
        ),
        compiler_params=pltpu.CompilerParams(
            vmem_limit_bytes=(SMALL if name in LEAN else LIMIT)
        ),
    )(scalars.number, *args, *after)


def sds(shape, dtype):
    return jax.ShapeDtypeStruct(shape, dtype)


def slots_of(routes):
    tokens = routes.shape[1]
    experts = iota((16, tokens), 0)
    r0, r1 = routes[0:1, :], routes[1:2, :]
    one0, one1 = r0 == experts, r1 == experts
    both = jnp.where(one0 | one1, 1.0, 0.0).astype(BF)
    earlier = jnp.where(iota((tokens, tokens), 0) < iota((tokens, tokens), 1), 1.0, 0.0).astype(BF)
    count = dot(both, earlier)
    s0 = jnp.sum(jnp.where(one0, count, 0.0), axis=0, keepdims=True)
    s1 = jnp.sum(jnp.where(one1, count, 0.0), axis=0, keepdims=True)
    return r0.astype(F32), r1.astype(F32), s0, s1


def column(row):
    return jnp.broadcast_to(row, (row.shape[1], row.shape[1])).T


def dispatch_kernel(at, routes_ref, weight_ref, x_ref, y_ref, out_ref):
    tokens = routes_ref.shape[1]
    r0, r1, s0, s1 = slots_of(routes_ref[...])
    key0 = r0 * 32.0 + s0
    key1 = r1 * 32.0 + s1
    w = weight_ref[...]
    w0, w1 = column(w[0:1])[:, 0:1], column(w[1:2])[:, 0:1]
    q = iota((40, tokens), 0)
    is_input = q < 20
    slot = jnp.where(is_input, q, jnp.where(q < 24, q - 4, q - 24)).astype(F32)
    experts = out_ref.shape[0] // 2
    picks = []
    for e in range(experts):
        key = slot + 32.0 * e
        m0, m1 = key0 == key, key1 == key
        picks.append(
            jnp.concatenate(
                [
                    jnp.where(is_input & (m0 | m1), 1.0, 0.0),
                    jnp.where(is_input, 0.0, jnp.where(m0, 1.0, 0.0)),
                    jnp.where(is_input, 0.0, jnp.where(m1, 1.0, 0.0)),
                ],
                axis=1,
            )
        )
    pick = jnp.concatenate(picks, axis=0).astype(BF)
    for f in range(0, out_ref.shape[2], 256):
        wide = slice(f, min(f + 256, out_ref.shape[2]))
        y = y_ref[:, wide].astype(F32)
        table = jnp.concatenate([x_ref[:, wide], (w0 * y).astype(BF), (w1 * y).astype(BF)], axis=0)
        rows = dot(pick, table)
        for e in range(experts):
            block = rows[40 * e : 40 * e + 40].astype(BF)
            out_ref[2 * e, :, wide] = block
            out_ref[2 * e + 1, :, wide] = block


def swap_halves(a):
    return jnp.concatenate([a[4:8], a[0:4]], axis=0)


def layout_kernel(at, wg_ref, wu_ref, wd_ref, woth_ref, side_ref, back_ref):
    side_ref[:, 0:128] = wg_ref[0]
    side_ref[:, 128:256] = wu_ref[0]
    for t in range(0, side_ref.shape[0], 128):
        side_ref[t : t + 128, 256:384] = wd_ref[0, :, t : t + 128].astype(F32).T.astype(BF)
    for y in range(back_ref.shape[1] // 128):
        first = pl.multiple_of((2 * y + at[1]) * 128, 128)
        for n, w in enumerate(
            (
                wg_ref[0, pl.ds(first, 128), :],
                wu_ref[0, pl.ds(first, 128), :],
                woth_ref[0, y],
                woth_ref[1, y],
            )
        ):
            back_ref[128 * n : 128 * n + 128, 128 * y : 128 * y + 128] = w.astype(F32).T.astype(BF)


def first_kernel(at, g_ref, w_ref, out_ref):
    out_ref[...] = dot(g_ref[...], w_ref[...])


def delta_kernel(at, g_ref, w_ref, acc_ref, delta_ref, pack_ref):
    sums = dot(g_ref[...], w_ref[...]) + acc_ref[...]
    gu, yh = sums[:, 0:256], sums[:, 256:384]
    low = iota((8, 128), 0) < 4
    zero8 = jnp.zeros((8, 128), F32)
    dgs, dus, dhs, pgs, pus = [], [], [], [], []
    mixed = []
    spans = g_ref.shape[0] // 40
    for d in range(spans):
        b = 40 * d
        pg, pu = gu[b : b + 24, 0:128], gu[b : b + 24, 128:256]
        hg = jnp.concatenate([yh[b + 24 : b + 40], swap_halves(yh[b + 16 : b + 24])], axis=0)
        s = jax.nn.sigmoid(pg)
        act = pg * s
        hid = act * pu
        gd = hg * pu * s * (1.0 + pg * (1.0 - s))
        ud = hg * act
        dgs += [gd[0:16], jnp.where(low, gd[16:24], 0.0), zero8, zero8]
        dus += [ud[0:16], jnp.where(low, ud[16:24], 0.0), zero8, zero8]
        dhs += [zero8, zero8, jnp.where(low, 0.0, swap_halves(hid[16:24])), hid[0:16]]
        mixed.append((gd, ud))
    for d in range(0, spans, 2):
        for n, parts in ((0, pgs), (1, pus)):
            even, odd = mixed[d][n], mixed[d + 1][n]
            parts += [
                even[0:16],
                jnp.where(low, even[16:24], swap_halves(odd[16:24])),
                odd[0:16],
            ]
    delta_ref[:, 0:128] = jnp.concatenate(dgs, axis=0).astype(BF)
    delta_ref[:, 128:256] = jnp.concatenate(dus, axis=0).astype(BF)
    delta_ref[:, 256:384] = jnp.concatenate(dhs, axis=0).astype(BF)
    pack_ref[:, 0:128] = jnp.concatenate(pgs, axis=0).astype(BF)
    pack_ref[:, 128:256] = jnp.concatenate(pus, axis=0).astype(BF)


def partial_kernel(at, pack_ref, back_ref, out_ref):
    core = at[1]
    nz, ny, rows, _ = out_ref.shape
    lhs = jnp.concatenate([pack_ref[core], pack_ref[1 - core]], axis=1)
    for y in range(0, ny, 2):
        o = dot(lhs, back_ref[:, 128 * y : 128 * y + 256]).astype(BF)
        for z in range(nz):
            out_ref[z, y] = o[z * rows : (z + 1) * rows, 0:128]
            out_ref[z, y + 1] = o[z * rows : (z + 1) * rows, 128:256]


def weight_kernel(at, delta_ref, own_ref, other_ref, gate_ref, up_ref, down_ref, dt_ref):
    rows, half = own_ref.shape
    for r in range(0, rows, 128):
        dt_ref[:, r : r + 128] = delta_ref[r : r + 128, :].astype(F32).T.astype(BF)
    for g_ref, core in ((own_ref, at[1]), (other_ref, 1 - at[1])):
        for p in range(0, half, 256):
            o = dot(dt_ref[...], g_ref[:, p : p + 256])
            first = pl.multiple_of(core * half + p, 256)
            gate_ref[0, pl.ds(first, 256), :] = o[0:128].T.astype(BF)
            up_ref[0, pl.ds(first, 256), :] = o[128:256].T.astype(BF)
            down_ref[0, :, pl.ds(first, 256)] = o[256:384].astype(BF)


def sum_kernel(at, got_ref, out_ref):
    nz, ny, _, _ = got_ref.shape
    for z in range(nz):
        total = got_ref[z, 0].astype(F32)
        for y in range(1, ny):
            total = total + got_ref[z, y].astype(F32)
        for p in range(out_ref.shape[0] // 2):
            b = 40 * p
            out_ref[2 * p, z] = total[b : b + 24].astype(BF)
            out_ref[2 * p + 1, z] = jnp.concatenate(
                [total[b + 24 : b + 40], total[b + 16 : b + 24]], axis=0
            ).astype(BF)


def collect_kernel(at, routes_ref, got_ref, cot_ref, out_ref):
    nx, nz, _, _ = got_ref.shape
    routes = routes_ref[...]
    _, _, s0, s1 = slots_of(routes)
    shift = (at[4] % 2).astype(F32) * 4.0
    cols = nx * nz * 24
    lanes = iota((routes.shape[1], cols), 1).astype(F32)
    hit = None
    for n, s in ((0, s0), (1, s1)):
        half = routes[n : n + 1, :] * 2
        block = (half % nx) * nz + half // nx
        row = block.astype(F32) * 24.0 + s + jnp.where(s >= 16.0, shift, 0.0)
        first = column(row)[:, 0:1]
        match = (lanes == first) | (lanes == first + 24.0 * nz)
        hit = match if hit is None else hit | match
    pick = jnp.where(hit, 1.0, 0.0).astype(BF)
    table = got_ref[...].astype(F32).reshape(cols, 128).astype(BF)
    out_ref[...] = (cot_ref[...].astype(F32) + dot(pick, table)).astype(BF)


def block_of(shape):
    return iota(shape, 1) // BLOCK


def mids_of(gc):
    return [gc[:, b + BLOCK // 2 - 1 : b + BLOCK // 2] for b in range(0, gc.shape[1], BLOCK)]


def growth(gc):
    blocks = block_of(gc.shape)
    mid = jnp.zeros(gc.shape, F32)
    for n, m in enumerate(mids_of(gc)):
        mid = jnp.where(blocks == n, m, mid)
    return jnp.exp(gc - mid)


def causal(tokens):
    return iota((tokens, tokens), 1) <= iota((tokens, tokens), 0)


def in_parts(rows):
    high = rows.astype(BF)
    rest = rows - high.astype(F32)
    mid = rest.astype(BF)
    low = (rest - mid.astype(F32)).astype(BF)
    n = iota(rows.shape, 0)
    parts = jnp.where(n == 0, high.astype(F32), jnp.where(n == 1, mid.astype(F32), low.astype(F32)))
    return jnp.where(n < 3, parts, 0.0).astype(BF)


def columns(rows):
    rows = rows + [jnp.zeros((128 - len(rows), 128), F32)]
    return jnp.concatenate(rows, axis=0).T


def forward_kernel(at, q_ref, k_ref, v_ref, g_ref, s_ref, mixed_ref, p_ref, last_ref, gc_ref, tot_ref):
    width, tokens = q_ref.shape
    g = g_ref[...]
    before = jnp.where(iota((tokens, tokens), 0) <= iota((tokens, tokens), 1), 1.0, 0.0)
    gc = dot(g, before, HI)
    gc_ref[...] = gc
    q = q_ref[...].astype(F32) * (width**-0.5)
    k = k_ref[...].astype(F32)
    v = v_ref[...].astype(F32)
    s0 = s_ref[0, 0]
    qt = q * growth(gc)
    parts = []
    for n, mid in enumerate(mids_of(gc)):
        whole = dot_tn(qt, k * jnp.exp(jnp.minimum(mid - gc, 40.0)), HI)
        parts.append(whole[n * BLOCK : (n + 1) * BLOCK])
    p = jnp.where(causal(tokens), jnp.concatenate(parts, axis=0), 0.0)
    p_ref[...] = p.astype(BF)
    mixed_ref[...] = (dot_tn(q * jnp.exp(gc), s0, HI) + dot(p, v, HI)).astype(BF)
    end = gc[:, tokens - 1 : tokens]
    last_ref[...] = jnp.exp(end) * s0 + dot(k * jnp.exp(end - gc), v, HI)
    row = dot_nt(jnp.ones((8, tokens), F32), g, HI)
    row = jnp.concatenate([row, jnp.zeros((8, 128 - width), F32)], axis=1)
    tot_ref[...] = in_parts(row)


def head_kernel(piece, at, tg_ref, w_ref, q_ref, gc_ref, mixed_ref, tot_ref, rows_ref, send_ref):
    slices = tg_ref.shape[0]
    width = q_ref.shape[0]
    nx = send_ref.shape[0]
    tg = jnp.concatenate([tg_ref[t] for t in range(slices)], axis=1)
    rows = dot(tg, w_ref[...]).astype(BF)
    rows_ref[...] = rows
    qe = q_ref[...].astype(F32) * (width**-0.5) * jnp.exp(gc_ref[...])
    carry = dot(qe, rows.astype(F32), HI).astype(BF)
    own = send_ref.shape[1] - width - 8
    for n in range(nx):
        send_ref[n, own : own + width, :] = carry
        send_ref[n, own + width : own + width + 8, :] = tot_ref[...]
    mixed = mixed_ref[...]
    for t in range(slices):
        o = dot_tn(tg_ref[t], mixed).astype(BF)
        for r in range(0, 128, piece):
            d = (t * 128 + r) // piece
            send_ref[d % nx, (d // nx) * piece : (d // nx + 1) * piece, :] = o[r : r + piece]


def local_kernel(at, rows_ref, q_ref, k_ref, v_ref, gc_ref, s_ref, p_ref, qraw_ref, qq_ref, kl_ref, vl_ref):
    width, tokens = q_ref.shape
    scale = width**-0.5
    rows = rows_ref[...]
    gc = gc_ref[...]
    q = q_ref[...].astype(F32)
    k = k_ref[...].astype(F32)
    a = jnp.where(causal(tokens), dot_nt(rows, v_ref[...]), 0.0)
    grow = growth(gc)
    qt = q * scale * grow
    blocks = block_of(gc.shape)
    inner = jnp.zeros((width, tokens), F32)
    key_local = jnp.zeros((width, tokens), F32)
    for n, mid in enumerate(mids_of(gc)):
        fall = jnp.exp(jnp.minimum(mid - gc, 40.0))
        inner = jnp.where(blocks == n, dot_nt(k * fall, a, HI), inner)
        key_local = key_local + fall * dot(jnp.where(blocks == n, qt, 0.0), a, HI)
    qraw = scale * (jnp.exp(gc) * dot_nt(s_ref[0, 0], rows.astype(F32), HI) + grow * inner)
    qraw_ref[...] = qraw.astype(BF)
    qq_ref[...] = q * qraw
    kl_ref[...] = key_local
    vl_ref[...] = dot_tn(p_ref[...], rows)


def group_kernel(at, got_ref, inside_ref, after_ref, send_ref, token_ref):
    token_ref[...] = jnp.zeros(token_ref.shape, F32)
    nx, rows, _ = got_ref.shape
    nz = send_ref.shape[0]
    width = inside_ref.shape[0]
    own = rows - width - 8
    piece = own // nz
    x = at[4]
    zero = jnp.zeros((1, 128), F32)
    before, later = zero, zero
    weights, wholes = [], []
    for i in range(nx):
        weights.append(jnp.where(x < i, jnp.exp(later), 0.0))
        wholes.append(jnp.exp(before))
        part = got_ref[i, own + width : own + width + 8, :].astype(F32)
        total = jnp.sum(part, axis=0, keepdims=True)
        before = before + total
        later = later + jnp.where(x < i, total, 0.0)
    after_ref[...] = jnp.broadcast_to(later, (8, 128))
    cols = columns(weights + wholes)
    inside = jnp.zeros((width, 128), F32)
    whole = jnp.zeros((width, 128), F32)
    for i in range(nx):
        part = got_ref[i, own : own + width, :].astype(F32)
        inside = inside + cols[0:width, i : i + 1] * part
        whole = whole + cols[0:width, nx + i : nx + i + 1] * part
    inside_ref[...] = inside
    whole = whole.astype(BF)
    parts = in_parts(jnp.broadcast_to(before, (8, 128)))
    for i in range(nz):
        total = got_ref[0, i * piece : (i + 1) * piece, :].astype(F32)
        for j in range(1, nx):
            total = total + got_ref[j, i * piece : (i + 1) * piece, :].astype(F32)
        send_ref[i, 0:piece, :] = total.astype(BF)
        send_ref[i, piece : piece + width, :] = whole
        send_ref[i, piece + width : piece + width + 8, :] = parts


def last_kernel(at, got_ref, inside_ref, after_ref, k_ref, v_ref, gc_ref, last_ref, qq_ref, kl_ref, vl_ref, og_ref, key_ref, value_ref, decay_ref):
    width, tokens = k_ref.shape
    piece = og_ref.shape[0]
    z = at[3]
    sums = after_ref[0:1, :]
    weights = []
    for i in range(got_ref.shape[0]):
        weights.append(jnp.where(z < i, jnp.exp(sums), 0.0))
        part = got_ref[i, piece + width : piece + width + 8, :].astype(F32)
        sums = sums + jnp.where(z < i, jnp.sum(part, axis=0, keepdims=True), 0.0)
    cols = columns(weights)
    incoming = inside_ref[...]
    total = jnp.zeros((piece, 128), F32)
    for i in range(got_ref.shape[0]):
        total = total + got_ref[i, 0:piece, :].astype(F32)
        part = got_ref[i, piece : piece + width, :].astype(F32)
        incoming = incoming + cols[0:width, i : i + 1] * part
    og_ref[...] = total
    gc = gc_ref[...]
    k = k_ref[...].astype(F32)
    rest = jnp.exp(gc[:, tokens - 1 : tokens] - gc)
    key = kl_ref[...] + rest * dot_nt(incoming, v_ref[...].astype(F32), HI)
    key_ref[...] = key.astype(BF)
    value_ref[...] = (vl_ref[...] + dot_tn(k * rest, incoming, HI)).astype(BF)
    later = jnp.where(causal(tokens), 1.0, 0.0)
    cross = jnp.sum(last_ref[...] * incoming, axis=1, keepdims=True)
    decay_ref[...] = dot(qq_ref[...] - k * key, later, HI) + cross


def on_device(
    expert_input,
    cotangent,
    routes,
    route_weight,
    gate_weight,
    up_weight,
    down_weight,
    out_weight,
    queries,
    key_vectors,
    value_rows,
    log_decay,
    start_state,
):
    tokens = expert_input.shape[0]
    nz, nx, ny = lax.axis_size("z"), lax.axis_size("x"), lax.axis_size("y")
    spans = nz * nx
    slices = ny * 2
    core = lax.axis_index("c")
    place = lax.axis_index(("z", "x", "y", "c")).astype(jnp.int32)
    sizes = ((1, slices), (1, 2), (slices, spans), (slices * nx, nz), (slices, nx))
    at = Place(place.reshape(1), sizes)
    width = queries.shape[2]
    piece_rows = slices * 128 // spans
    routes = routes.T
    route_weight = route_weight.T
    q = queries.reshape(tokens, width).T
    k = key_vectors.reshape(tokens, width).T
    v = value_rows.reshape(tokens, 128)
    g = log_decay.reshape(tokens, width).T
    slice_block = ((tokens, 128), lambda i, s: (0, s[0]))
    half = slices * 64
    half_block = ((tokens, half), lambda i, s: (0, s[1]))

    (sent,) = call(
        dispatch_kernel,
        "dispatch",
        (sds((spans, 40, half), BF),),
        at,
        routes,
        route_weight,
        expert_input,
        cotangent,
        blocks={2: half_block, 3: half_block},
    )
    own = lax.all_to_all(sent, SP, 0, 0, tiled=True).reshape(spans * 40, half)

    weights = jnp.stack([gate_weight[0], up_weight[0]]).reshape(2, ny, 2, 128, 128)
    weights = lax.dynamic_index_in_dim(weights, 1 - core, 2, keepdims=False)
    weights = lax.ppermute(weights, "c", [(0, 1), (1, 0)])
    mixed, p, last, gc, totals = call(
        forward_kernel,
        "forward",
        (
            sds((tokens, 128), BF),
            sds((tokens, tokens), BF),
            sds((width, 128), F32),
            sds((width, tokens), F32),
            sds((8, 128), BF),
        ),
        at,
        q,
        k,
        v,
        g,
        start_state,
        after=(sent,),
    )
    side, back = call(
        layout_kernel,
        "layout",
        (sds((slices * 128, 384), BF), sds((512, half), BF)),
        at,
        gate_weight,
        up_weight,
        down_weight,
        weights,
        after=(mixed,),
    )
    own, mixed, side = lax.optimization_barrier((own, mixed, side))

    other = lax.ppermute(own, "c", [(0, 1), (1, 0)])
    rows_all = spans * 40
    tile = rows_all // TILES
    rows_block = ((tile, half), lambda i, s: (i, 0))
    acc_block = ((tile, 384), lambda i, s: (i, 0))
    (acc,) = call(
        first_kernel,
        "first",
        (sds((rows_all, 384), F32),),
        at,
        own,
        side,
        blocks={0: rows_block, 1: ((half, 384), lambda i, s: (s[1], 0))},
        out_blocks={0: acc_block},
        grid=TILES,
    )
    delta, pack = call(
        delta_kernel,
        "deltas",
        (sds((rows_all, 384), BF), sds((rows_all // 2, 256), BF)),
        at,
        other,
        side,
        acc,
        blocks={
            0: rows_block,
            1: ((half, 384), lambda i, s: (1 - s[1], 0)),
            2: acc_block,
        },
        out_blocks={0: acc_block, 1: ((tile // 2, 256), lambda i, s: (i, 0))},
        grid=TILES,
    )
    packs = lax.all_gather(pack, "c", axis=0)
    (terms,) = call(
        partial_kernel,
        "partials",
        (sds((nz, ny, nx * 20, 128), BF),),
        at,
        packs,
        back,
    )
    got = lax.all_to_all(
        terms.reshape(nz * ny, nx * 20, 128), ("z", "y"), 0, 0, tiled=True
    ).reshape(nz, ny, nx * 20, 128)
    (summed,) = call(sum_kernel, "sums", (sds((nx, nz, 24, 128), BF),), at, got)
    returned = lax.all_to_all(summed.reshape(nx, nz * 24, 128), "x", 0, 0, tiled=True)
    (slice_grad,) = call(
        collect_kernel,
        "collect",
        (sds((tokens, 128), BF),),
        at,
        routes,
        returned.reshape(nx, nz, 24, 128),
        cotangent,
        blocks={2: slice_block},
    )
    total_grad = lax.all_gather(slice_grad, TP, axis=0)

    rows, leaving = call(
        partial(head_kernel, piece_rows),
        "head",
        (sds((tokens, 128), BF), sds((nx, nz * piece_rows + width + 8, 128), BF)),
        at,
        total_grad,
        out_weight,
        q,
        gc,
        mixed,
        totals,
    )
    crossing = lax.all_to_all(leaving, "x", 0, 0, tiled=True)
    inside, later, group, token = call(
        group_kernel,
        "group",
        (
            sds((width, 128), F32),
            sds((8, 128), F32),
            sds((nz, piece_rows + width + 8, 128), BF),
            sds((8, 128), F32),
        ),
        at,
        crossing,
    )
    group = lax.all_to_all(group, "z", 0, 0, tiled=True)
    gate_grad, up_grad, down_grad = call(
        weight_kernel,
        "weights",
        (
            sds((1, slices * 128, 128), BF),
            sds((1, slices * 128, 128), BF),
            sds((1, 128, slices * 128), BF),
        ),
        at,
        delta,
        own,
        other,
        scratch=[pltpu.VMEM((384, spans * 40), BF)],
        after=(token,),
    )
    qraw, qq, key_local, value_local = call(
        local_kernel,
        "local",
        (
            sds((width, tokens), BF),
            sds((width, tokens), F32),
            sds((width, tokens), F32),
            sds((tokens, 128), F32),
        ),
        at,
        rows,
        q,
        k,
        v,
        gc,
        start_state,
        p,
        after=(token,),
    )
    out_grad, key, value, decay = call(
        last_kernel,
        "last",
        (
            sds((piece_rows, 128), F32),
            sds((width, tokens), BF),
            sds((tokens, 128), BF),
            sds((width, tokens), F32),
        ),
        at,
        group,
        inside,
        later,
        k,
        v,
        gc,
        last,
        qq,
        key_local,
        value_local,
    )
    return (
        gate_grad,
        up_grad,
        down_grad,
        out_grad,
        qraw.T[:, None, :],
        key.T[:, None, :],
        value[:, None, :],
        decay.T[:, None, :],
    )


def solution(mesh):
    torus = Mesh(mesh.devices.reshape(8, 4, mesh.shape["tp"] // 2, 2), ("z", "x", "y", "c"))
    in_specs = (
        P(SP, None),
        P(SP, None),
        P(SP, None),
        P(SP, None),
        P(SP, None, TP),
        P(SP, None, TP),
        P(SP, TP, None),
        P(None, TP),
        P(SP, TP, None),
        P(SP, TP, None),
        P(SP, TP, None),
        P(SP, TP, None),
        P(SP, TP, None, None),
    )
    out_specs = (
        P(SP, None, TP),
        P(SP, None, TP),
        P(SP, TP, None),
        P(SP, TP),
        P(SP, TP, None),
        P(SP, TP, None),
        P(SP, TP, None),
        P(SP, TP, None),
    )
    return jax.shard_map(
        on_device, mesh=torus, in_specs=in_specs, out_specs=out_specs, check_vma=False
    )
```

```python
from functools import partial

import jax
import jax.numpy as jnp
from jax import lax
from jax.experimental import pallas as pl
from jax.experimental.pallas import tpu as pltpu
from jax.sharding import Mesh
from jax.sharding import PartitionSpec as P

SP = ("z", "x")
TP = ("y", "c")
BF = jnp.bfloat16
F32 = jnp.float32
HI = lax.Precision.HIGHEST
BLOCK = 32
LIMIT = 56 * 1024 * 1024
SMALL = 20 * 1024 * 1024
LEAN = ('first', 'deltas', 'partials', 'sums', 'collect', 'head', 'local', 'group', 'last')
TILES = 2


def dot(a, b, precision=None):
    return lax.dot_general(
        a, b, (((1,), (0,)), ((), ())), precision=precision, preferred_element_type=F32
    )


def dot_nt(a, b, precision=None):
    return lax.dot_general(
        a, b, (((1,), (1,)), ((), ())), precision=precision, preferred_element_type=F32
    )


def dot_tn(a, b, precision=None):
    return lax.dot_general(
        a, b, (((0,), (0,)), ((), ())), precision=precision, preferred_element_type=F32
    )


def iota(shape, dim):
    return lax.broadcasted_iota(jnp.int32, shape, dim)


class Place:
    def __init__(self, number, sizes):
        self.number, self.sizes = number, sizes

    def __getitem__(self, k):
        step, count = self.sizes[k]
        return lax.shift_right_logical(self.number[0], step.bit_length() - 1) & (count - 1)


def call(
    kernel, name, outs, scalars, *args, blocks=None, out_blocks=None, scratch=(), after=(), grid=1
):
    blocks = blocks or {}
    out_blocks = out_blocks or {}
    specs = []
    used, waits = len(args), len(after)

    def body(number, *refs):
        kernel(Place(number, scalars.sizes), *refs[:used], *refs[used + waits :])

    def placed(index):
        return lambda i, s: index(i, Place(s, scalars.sizes))

    for n, a in enumerate(args):
        if n in blocks:
            specs.append(pl.BlockSpec(blocks[n][0], placed(blocks[n][1])))
        else:
            specs.append(pl.BlockSpec(a.shape, lambda i, s, nd=a.ndim: (0,) * nd))
    specs += [pl.BlockSpec(memory_space=pl.ANY)] * waits
    out_specs = tuple(
        pl.BlockSpec(out_blocks[n][0], placed(out_blocks[n][1]))
        if n in out_blocks
        else pl.BlockSpec(o.shape, lambda i, s, nd=len(o.shape): (0,) * nd)
        for n, o in enumerate(outs)
    )
    return pl.pallas_call(
        body,
        name=name,
        out_shape=outs,
        grid_spec=pltpu.PrefetchScalarGridSpec(
            num_scalar_prefetch=1,
            grid=(grid,),
            in_specs=specs,
            out_specs=out_specs,
            scratch_shapes=list(scratch),
        ),
        compiler_params=pltpu.CompilerParams(
            vmem_limit_bytes=(SMALL if name in LEAN else LIMIT)
        ),
    )(scalars.number, *args, *after)


def sds(shape, dtype):
    return jax.ShapeDtypeStruct(shape, dtype)


def slots_of(routes):
    tokens = routes.shape[1]
    experts = iota((16, tokens), 0)
    r0, r1 = routes[0:1, :], routes[1:2, :]
    one0, one1 = r0 == experts, r1 == experts
    both = jnp.where(one0 | one1, 1.0, 0.0).astype(BF)
    earlier = jnp.where(iota((tokens, tokens), 0) < iota((tokens, tokens), 1), 1.0, 0.0).astype(BF)
    count = dot(both, earlier)
    s0 = jnp.sum(jnp.where(one0, count, 0.0), axis=0, keepdims=True)
    s1 = jnp.sum(jnp.where(one1, count, 0.0), axis=0, keepdims=True)
    return r0.astype(F32), r1.astype(F32), s0, s1


def column(row):
    return jnp.broadcast_to(row, (row.shape[1], row.shape[1])).T


def dispatch_kernel(at, routes_ref, weight_ref, x_ref, y_ref, out_ref):
    tokens = routes_ref.shape[1]
    r0, r1, s0, s1 = slots_of(routes_ref[...])
    key0 = r0 * 32.0 + s0
    key1 = r1 * 32.0 + s1
    w = weight_ref[...]
    w0, w1 = column(w[0:1])[:, 0:1], column(w[1:2])[:, 0:1]
    q = iota((40, tokens), 0)
    is_input = q < 20
    slot = jnp.where(is_input, q, jnp.where(q < 24, q - 4, q - 24)).astype(F32)
    experts = out_ref.shape[0] // 2
    picks = []
    for e in range(experts):
        key = slot + 32.0 * e
        m0, m1 = key0 == key, key1 == key
        picks.append(
            jnp.concatenate(
                [
                    jnp.where(is_input & (m0 | m1), 1.0, 0.0),
                    jnp.where(is_input, 0.0, jnp.where(m0, 1.0, 0.0)),
                    jnp.where(is_input, 0.0, jnp.where(m1, 1.0, 0.0)),
                ],
                axis=1,
            )
        )
    pick = jnp.concatenate(picks, axis=0).astype(BF)
    for f in range(0, out_ref.shape[2], 256):
        wide = slice(f, min(f + 256, out_ref.shape[2]))
        y = y_ref[:, wide].astype(F32)
        table = jnp.concatenate([x_ref[:, wide], (w0 * y).astype(BF), (w1 * y).astype(BF)], axis=0)
        rows = dot(pick, table)
        for e in range(experts):
            block = rows[40 * e : 40 * e + 40].astype(BF)
            out_ref[2 * e, :, wide] = block
            out_ref[2 * e + 1, :, wide] = block


def swap_halves(a):
    return jnp.concatenate([a[4:8], a[0:4]], axis=0)


def part_at(at, n):
    core = at[1] if n < 2 else 1 - at[1]
    return 2 * core + (at[5] if n % 2 == 0 else 1 - at[5])


def layout_kernel(at, wg_ref, wu_ref, wd_ref, woth_ref, side_ref, back_ref):
    part = side_ref.shape[0] // 4
    for n in range(4):
        first = pl.multiple_of(part_at(at, n) * part, 128)
        to = slice(n * part, (n + 1) * part)
        side_ref[to, 0:128] = wg_ref[0, pl.ds(first, part), :]
        side_ref[to, 128:256] = wu_ref[0, pl.ds(first, part), :]
        side_ref[to, 256:384] = wd_ref[0, :, pl.ds(first, part)].astype(F32).T.astype(BF)
    for y in range(back_ref.shape[1] // 128):
        first = pl.multiple_of((2 * y + at[1]) * 128, 128)
        for n, w in enumerate(
            (
                wg_ref[0, pl.ds(first, 128), :],
                wu_ref[0, pl.ds(first, 128), :],
                woth_ref[0, y],
                woth_ref[1, y],
            )
        ):
            back_ref[128 * n : 128 * n + 128, 128 * y : 128 * y + 128] = w.astype(F32).T.astype(BF)


def first_kernel(at, g_ref, w_ref, out_ref):
    out_ref[...] = dot(g_ref[...], w_ref[...])


def delta_kernel(at, other_ref, rest_ref, beside_ref, w_ref, acc_ref, delta_ref, pack_ref):
    part = rest_ref.shape[1]
    sums = acc_ref[...] + dot(rest_ref[...], w_ref[part : 2 * part, :])
    sums = sums + dot(other_ref[...], w_ref[2 * part : 3 * part, :])
    sums = sums + dot(beside_ref[...], w_ref[3 * part : 4 * part, :])
    gu, yh = sums[:, 0:256], sums[:, 256:384]
    low = iota((8, 128), 0) < 4
    zero8 = jnp.zeros((8, 128), F32)
    dgs, dus, dhs, pgs, pus = [], [], [], [], []
    mixed = []
    spans = rest_ref.shape[0] // 40
    for d in range(spans):
        b = 40 * d
        pg, pu = gu[b : b + 24, 0:128], gu[b : b + 24, 128:256]
        hg = jnp.concatenate([yh[b + 24 : b + 40], swap_halves(yh[b + 16 : b + 24])], axis=0)
        s = jax.nn.sigmoid(pg)
        act = pg * s
        hid = act * pu
        gd = hg * pu * s * (1.0 + pg * (1.0 - s))
        ud = hg * act
        dgs += [gd[0:16], jnp.where(low, gd[16:24], 0.0), zero8, zero8]
        dus += [ud[0:16], jnp.where(low, ud[16:24], 0.0), zero8, zero8]
        dhs += [zero8, zero8, jnp.where(low, 0.0, swap_halves(hid[16:24])), hid[0:16]]
        mixed.append((gd, ud))
    for d in range(0, spans, 2):
        for n, parts in ((0, pgs), (1, pus)):
            even, odd = mixed[d][n], mixed[d + 1][n]
            parts += [
                even[0:16],
                jnp.where(low, even[16:24], swap_halves(odd[16:24])),
                odd[0:16],
            ]
    delta_ref[:, 0:128] = jnp.concatenate(dgs, axis=0).astype(BF)
    delta_ref[:, 128:256] = jnp.concatenate(dus, axis=0).astype(BF)
    delta_ref[:, 256:384] = jnp.concatenate(dhs, axis=0).astype(BF)
    pack_ref[:, 0:128] = jnp.concatenate(pgs, axis=0).astype(BF)
    pack_ref[:, 128:256] = jnp.concatenate(pus, axis=0).astype(BF)


def partial_kernel(at, pack_ref, back_ref, out_ref):
    core = at[1]
    nz, ny, rows, _ = out_ref.shape
    lhs = jnp.concatenate([pack_ref[core], pack_ref[1 - core]], axis=1)
    for y in range(0, ny, 2):
        o = dot(lhs, back_ref[:, 128 * y : 128 * y + 256]).astype(BF)
        for z in range(nz):
            out_ref[z, y] = o[z * rows : (z + 1) * rows, 0:128]
            out_ref[z, y + 1] = o[z * rows : (z + 1) * rows, 128:256]


def weight_kernel(at, delta_ref, a_ref, b_ref, c_ref, d_ref, gate_ref, up_ref, down_ref, dt_ref):
    rows, part = a_ref.shape
    for r in range(0, rows, 128):
        dt_ref[:, r : r + 128] = delta_ref[r : r + 128, :].astype(F32).T.astype(BF)
    for n, g_ref in enumerate((a_ref, b_ref, c_ref, d_ref)):
        wide = min(256, part)
        for p in range(0, part, wide):
            o = dot(dt_ref[...], g_ref[:, p : p + wide])
            first = pl.multiple_of(part_at(at, n) * part + p, 128)
            gate_ref[0, pl.ds(first, wide), :] = o[0:128].T.astype(BF)
            up_ref[0, pl.ds(first, wide), :] = o[128:256].T.astype(BF)
            down_ref[0, :, pl.ds(first, wide)] = o[256:384].astype(BF)


def sum_kernel(at, got_ref, out_ref):
    nz, ny, _, _ = got_ref.shape
    for z in range(nz):
        total = got_ref[z, 0].astype(F32)
        for y in range(1, ny):
            total = total + got_ref[z, y].astype(F32)
        for p in range(out_ref.shape[0] // 2):
            b = 40 * p
            out_ref[2 * p, z] = total[b : b + 24].astype(BF)
            out_ref[2 * p + 1, z] = jnp.concatenate(
                [total[b + 24 : b + 40], total[b + 16 : b + 24]], axis=0
            ).astype(BF)


def collect_kernel(at, routes_ref, got_ref, cot_ref, out_ref):
    nx, nz, _, _ = got_ref.shape
    routes = routes_ref[...]
    _, _, s0, s1 = slots_of(routes)
    shift = (at[4] % 2).astype(F32) * 4.0
    cols = nx * nz * 24
    lanes = iota((routes.shape[1], cols), 1).astype(F32)
    hit = None
    for n, s in ((0, s0), (1, s1)):
        half = routes[n : n + 1, :] * 2
        block = (half % nx) * nz + half // nx
        row = block.astype(F32) * 24.0 + s + jnp.where(s >= 16.0, shift, 0.0)
        first = column(row)[:, 0:1]
        match = (lanes == first) | (lanes == first + 24.0 * nz)
        hit = match if hit is None else hit | match
    pick = jnp.where(hit, 1.0, 0.0).astype(BF)
    table = got_ref[...].astype(F32).reshape(cols, 128).astype(BF)
    out_ref[...] = (cot_ref[...].astype(F32) + dot(pick, table)).astype(BF)


def block_of(shape):
    return iota(shape, 1) // BLOCK


def mids_of(gc):
    return [gc[:, b + BLOCK // 2 - 1 : b + BLOCK // 2] for b in range(0, gc.shape[1], BLOCK)]


def growth(gc):
    blocks = block_of(gc.shape)
    mid = jnp.zeros(gc.shape, F32)
    for n, m in enumerate(mids_of(gc)):
        mid = jnp.where(blocks == n, m, mid)
    return jnp.exp(gc - mid)


def causal(tokens):
    return iota((tokens, tokens), 1) <= iota((tokens, tokens), 0)


def in_parts(rows):
    high = rows.astype(BF)
    rest = rows - high.astype(F32)
    mid = rest.astype(BF)
    low = (rest - mid.astype(F32)).astype(BF)
    n = iota(rows.shape, 0)
    parts = jnp.where(n == 0, high.astype(F32), jnp.where(n == 1, mid.astype(F32), low.astype(F32)))
    return jnp.where(n < 3, parts, 0.0).astype(BF)


def columns(rows):
    rows = rows + [jnp.zeros((128 - len(rows), 128), F32)]
    return jnp.concatenate(rows, axis=0).T


def forward_kernel(at, q_ref, k_ref, v_ref, g_ref, s_ref, mixed_ref, p_ref, last_ref, gc_ref, tot_ref):
    width, tokens = q_ref.shape
    g = g_ref[...]
    before = jnp.where(iota((tokens, tokens), 0) <= iota((tokens, tokens), 1), 1.0, 0.0)
    gc = dot(g, before, HI)
    gc_ref[...] = gc
    q = q_ref[...].astype(F32) * (width**-0.5)
    k = k_ref[...].astype(F32)
    v = v_ref[...].astype(F32)
    s0 = s_ref[0, 0]
    qt = q * growth(gc)
    parts = []
    for n, mid in enumerate(mids_of(gc)):
        whole = dot_tn(qt, k * jnp.exp(jnp.minimum(mid - gc, 40.0)), HI)
        parts.append(whole[n * BLOCK : (n + 1) * BLOCK])
    p = jnp.where(causal(tokens), jnp.concatenate(parts, axis=0), 0.0)
    p_ref[...] = p.astype(BF)
    mixed_ref[...] = (dot_tn(q * jnp.exp(gc), s0, HI) + dot(p, v, HI)).astype(BF)
    end = gc[:, tokens - 1 : tokens]
    last_ref[...] = jnp.exp(end) * s0 + dot(k * jnp.exp(end - gc), v, HI)
    row = dot_nt(jnp.ones((8, tokens), F32), g, HI)
    row = jnp.concatenate([row, jnp.zeros((8, 128 - width), F32)], axis=1)
    tot_ref[...] = in_parts(row)


def head_kernel(piece, at, tg_ref, w_ref, q_ref, gc_ref, mixed_ref, tot_ref, rows_ref, send_ref):
    slices = tg_ref.shape[0]
    width = q_ref.shape[0]
    nx = send_ref.shape[0]
    tg = jnp.concatenate([tg_ref[t] for t in range(slices)], axis=1)
    rows = dot(tg, w_ref[...]).astype(BF)
    rows_ref[...] = rows
    qe = q_ref[...].astype(F32) * (width**-0.5) * jnp.exp(gc_ref[...])
    carry = dot(qe, rows.astype(F32), HI).astype(BF)
    own = send_ref.shape[1] - width - 8
    for n in range(nx):
        send_ref[n, own : own + width, :] = carry
        send_ref[n, own + width : own + width + 8, :] = tot_ref[...]
    mixed = mixed_ref[...]
    for t in range(slices):
        o = dot_tn(tg_ref[t], mixed).astype(BF)
        for r in range(0, 128, piece):
            d = (t * 128 + r) // piece
            send_ref[d % nx, (d // nx) * piece : (d // nx + 1) * piece, :] = o[r : r + piece]


def local_kernel(at, rows_ref, q_ref, k_ref, v_ref, gc_ref, s_ref, p_ref, qraw_ref, qq_ref, kl_ref, vl_ref):
    width, tokens = q_ref.shape
    scale = width**-0.5
    rows = rows_ref[...]
    gc = gc_ref[...]
    q = q_ref[...].astype(F32)
    k = k_ref[...].astype(F32)
    a = jnp.where(causal(tokens), dot_nt(rows, v_ref[...]), 0.0)
    grow = growth(gc)
    qt = q * scale * grow
    blocks = block_of(gc.shape)
    inner = jnp.zeros((width, tokens), F32)
    key_local = jnp.zeros((width, tokens), F32)
    for n, mid in enumerate(mids_of(gc)):
        fall = jnp.exp(jnp.minimum(mid - gc, 40.0))
        inner = jnp.where(blocks == n, dot_nt(k * fall, a, HI), inner)
        key_local = key_local + fall * dot(jnp.where(blocks == n, qt, 0.0), a, HI)
    qraw = scale * (jnp.exp(gc) * dot_nt(s_ref[0, 0], rows.astype(F32), HI) + grow * inner)
    qraw_ref[...] = qraw.astype(BF)
    qq_ref[...] = q * qraw
    kl_ref[...] = key_local
    vl_ref[...] = dot_tn(p_ref[...], rows)


def group_kernel(at, got_ref, inside_ref, after_ref, send_ref, token_ref):
    token_ref[...] = jnp.zeros(token_ref.shape, F32)
    nx, rows, _ = got_ref.shape
    nz = send_ref.shape[0]
    width = inside_ref.shape[0]
    own = rows - width - 8
    piece = own // nz
    x = at[4]
    zero = jnp.zeros((1, 128), F32)
    before, later = zero, zero
    weights, wholes = [], []
    for i in range(nx):
        weights.append(jnp.where(x < i, jnp.exp(later), 0.0))
        wholes.append(jnp.exp(before))
        part = got_ref[i, own + width : own + width + 8, :].astype(F32)
        total = jnp.sum(part, axis=0, keepdims=True)
        before = before + total
        later = later + jnp.where(x < i, total, 0.0)
    after_ref[...] = jnp.broadcast_to(later, (8, 128))
    cols = columns(weights + wholes)
    inside = jnp.zeros((width, 128), F32)
    whole = jnp.zeros((width, 128), F32)
    for i in range(nx):
        part = got_ref[i, own : own + width, :].astype(F32)
        inside = inside + cols[0:width, i : i + 1] * part
        whole = whole + cols[0:width, nx + i : nx + i + 1] * part
    inside_ref[...] = inside
    whole = whole.astype(BF)
    parts = in_parts(jnp.broadcast_to(before, (8, 128)))
    for i in range(nz):
        total = got_ref[0, i * piece : (i + 1) * piece, :].astype(F32)
        for j in range(1, nx):
            total = total + got_ref[j, i * piece : (i + 1) * piece, :].astype(F32)
        send_ref[i, 0:piece, :] = total.astype(BF)
        send_ref[i, piece : piece + width, :] = whole
        send_ref[i, piece + width : piece + width + 8, :] = parts


def last_kernel(at, got_ref, inside_ref, after_ref, k_ref, v_ref, gc_ref, last_ref, qq_ref, kl_ref, vl_ref, og_ref, key_ref, value_ref, decay_ref):
    width, tokens = k_ref.shape
    piece = og_ref.shape[0]
    z = at[3]
    sums = after_ref[0:1, :]
    weights = []
    for i in range(got_ref.shape[0]):
        weights.append(jnp.where(z < i, jnp.exp(sums), 0.0))
        part = got_ref[i, piece + width : piece + width + 8, :].astype(F32)
        sums = sums + jnp.where(z < i, jnp.sum(part, axis=0, keepdims=True), 0.0)
    cols = columns(weights)
    incoming = inside_ref[...]
    total = jnp.zeros((piece, 128), F32)
    for i in range(got_ref.shape[0]):
        total = total + got_ref[i, 0:piece, :].astype(F32)
        part = got_ref[i, piece : piece + width, :].astype(F32)
        incoming = incoming + cols[0:width, i : i + 1] * part
    og_ref[...] = total
    gc = gc_ref[...]
    k = k_ref[...].astype(F32)
    rest = jnp.exp(gc[:, tokens - 1 : tokens] - gc)
    key = kl_ref[...] + rest * dot_nt(incoming, v_ref[...].astype(F32), HI)
    key_ref[...] = key.astype(BF)
    value_ref[...] = (vl_ref[...] + dot_tn(k * rest, incoming, HI)).astype(BF)
    later = jnp.where(causal(tokens), 1.0, 0.0)
    cross = jnp.sum(last_ref[...] * incoming, axis=1, keepdims=True)
    decay_ref[...] = dot(qq_ref[...] - k * key, later, HI) + cross


def on_device(
    expert_input,
    cotangent,
    routes,
    route_weight,
    gate_weight,
    up_weight,
    down_weight,
    out_weight,
    queries,
    key_vectors,
    value_rows,
    log_decay,
    start_state,
):
    tokens = expert_input.shape[0]
    nz, nx, ny = lax.axis_size("z"), lax.axis_size("x"), lax.axis_size("y")
    spans = nz * nx
    slices = ny * 2
    core = lax.axis_index("c")
    place = lax.axis_index(("z", "x", "y", "c")).astype(jnp.int32)
    sizes = ((1, slices), (1, 2), (slices, spans), (slices * nx, nz), (slices, nx), (2, 2))
    at = Place(place.reshape(1), sizes)
    width = queries.shape[2]
    piece_rows = slices * 128 // spans
    routes = routes.T
    route_weight = route_weight.T
    q = queries.reshape(tokens, width).T
    k = key_vectors.reshape(tokens, width).T
    v = value_rows.reshape(tokens, 128)
    g = log_decay.reshape(tokens, width).T
    slice_block = ((tokens, 128), lambda i, s: (0, s[0]))
    half = slices * 64
    part = half // 2
    part_block = ((tokens, part), lambda i, s: (0, part_at(s, 0)))

    (sent,) = call(
        dispatch_kernel,
        "dispatch",
        (sds((spans, 40, part), BF),),
        at,
        routes,
        route_weight,
        expert_input,
        cotangent,
        blocks={2: part_block, 3: part_block},
    )
    own = lax.all_to_all(sent, SP, 0, 0, tiled=True).reshape(spans * 40, part)

    weights = jnp.stack([gate_weight[0], up_weight[0]]).reshape(2, ny, 2, 128, 128)
    weights = lax.dynamic_index_in_dim(weights, 1 - core, 2, keepdims=False)
    weights = lax.ppermute(weights, "c", [(0, 1), (1, 0)])
    mixed, p, last, gc, totals = call(
        forward_kernel,
        "forward",
        (
            sds((tokens, 128), BF),
            sds((tokens, tokens), BF),
            sds((width, 128), F32),
            sds((width, tokens), F32),
            sds((8, 128), BF),
        ),
        at,
        q,
        k,
        v,
        g,
        start_state,
        after=(sent,),
    )
    side, back = call(
        layout_kernel,
        "layout",
        (sds((slices * 128, 384), BF), sds((512, half), BF)),
        at,
        gate_weight,
        up_weight,
        down_weight,
        weights,
        after=(mixed,),
    )
    own, mixed, side = lax.optimization_barrier((own, mixed, side))

    rows_all = spans * 40
    swap = [(0, 1), (1, 0)]
    up = [(i, (i + 1) % ny) for i in range(ny)]
    down = [(i, (i - 1) % ny) for i in range(ny)]
    low = lax.ppermute(own[: rows_all // 2], "y", up)
    high = lax.ppermute(own[rows_all // 2 :], "y", down)
    other = lax.ppermute(own, "c", swap)
    tile = rows_all // TILES
    part_rows = ((tile, part), lambda i, s: (i, 0))
    acc_block = ((tile, 384), lambda i, s: (i, 0))
    (acc,) = call(
        first_kernel,
        "first",
        (sds((rows_all, 384), F32),),
        at,
        own,
        side,
        blocks={0: part_rows, 1: ((part, 384), lambda i, s: (0, 0))},
        out_blocks={0: acc_block},
        grid=TILES,
    )
    low, high, acc, other = lax.optimization_barrier((low, high, acc, other))
    rest = jnp.concatenate([low, high], axis=0)
    beside = lax.ppermute(rest, "c", swap)
    delta, pack = call(
        delta_kernel,
        "deltas",
        (sds((rows_all, 384), BF), sds((rows_all // 2, 256), BF)),
        at,
        other,
        rest,
        beside,
        side,
        acc,
        blocks={0: part_rows, 1: part_rows, 2: part_rows, 4: acc_block},
        out_blocks={0: acc_block, 1: ((tile // 2, 256), lambda i, s: (i, 0))},
        grid=TILES,
    )
    packs = lax.all_gather(pack, "c", axis=0)
    (terms,) = call(
        partial_kernel,
        "partials",
        (sds((nz, ny, nx * 20, 128), BF),),
        at,
        packs,
        back,
    )
    got = lax.all_to_all(
        terms.reshape(nz * ny, nx * 20, 128), ("z", "y"), 0, 0, tiled=True
    ).reshape(nz, ny, nx * 20, 128)
    (summed,) = call(sum_kernel, "sums", (sds((nx, nz, 24, 128), BF),), at, got)
    returned = lax.all_to_all(summed.reshape(nx, nz * 24, 128), "x", 0, 0, tiled=True)
    (slice_grad,) = call(
        collect_kernel,
        "collect",
        (sds((tokens, 128), BF),),
        at,
        routes,
        returned.reshape(nx, nz, 24, 128),
        cotangent,
        blocks={2: slice_block},
    )
    total_grad = lax.all_gather(slice_grad, TP, axis=0)

    rows, leaving = call(
        partial(head_kernel, piece_rows),
        "head",
        (sds((tokens, 128), BF), sds((nx, nz * piece_rows + width + 8, 128), BF)),
        at,
        total_grad,
        out_weight,
        q,
        gc,
        mixed,
        totals,
    )
    crossing = lax.all_to_all(leaving, "x", 0, 0, tiled=True)
    inside, later, group, token = call(
        group_kernel,
        "group",
        (
            sds((width, 128), F32),
            sds((8, 128), F32),
            sds((nz, piece_rows + width + 8, 128), BF),
            sds((8, 128), F32),
        ),
        at,
        crossing,
    )
    group = lax.all_to_all(group, "z", 0, 0, tiled=True)
    gate_grad, up_grad, down_grad = call(
        weight_kernel,
        "weights",
        (
            sds((1, slices * 128, 128), BF),
            sds((1, slices * 128, 128), BF),
            sds((1, 128, slices * 128), BF),
        ),
        at,
        delta,
        own,
        rest,
        other,
        beside,
        scratch=[pltpu.VMEM((384, spans * 40), BF)],
        after=(token,),
    )
    qraw, qq, key_local, value_local = call(
        local_kernel,
        "local",
        (
            sds((width, tokens), BF),
            sds((width, tokens), F32),
            sds((width, tokens), F32),
            sds((tokens, 128), F32),
        ),
        at,
        rows,
        q,
        k,
        v,
        gc,
        start_state,
        p,
        after=(token,),
    )
    out_grad, key, value, decay = call(
        last_kernel,
        "last",
        (
            sds((piece_rows, 128), F32),
            sds((width, tokens), BF),
            sds((tokens, 128), BF),
            sds((width, tokens), F32),
        ),
        at,
        group,
        inside,
        later,
        k,
        v,
        gc,
        last,
        qq,
        key_local,
        value_local,
    )
    return (
        gate_grad,
        up_grad,
        down_grad,
        out_grad,
        qraw.T[:, None, :],
        key.T[:, None, :],
        value[:, None, :],
        decay.T[:, None, :],
    )


def solution(mesh):
    torus = Mesh(mesh.devices.reshape(8, 4, mesh.shape["tp"] // 2, 2), ("z", "x", "y", "c"))
    in_specs = (
        P(SP, None),
        P(SP, None),
        P(SP, None),
        P(SP, None),
        P(SP, None, TP),
        P(SP, None, TP),
        P(SP, TP, None),
        P(None, TP),
        P(SP, TP, None),
        P(SP, TP, None),
        P(SP, TP, None),
        P(SP, TP, None),
        P(SP, TP, None, None),
    )
    out_specs = (
        P(SP, None, TP),
        P(SP, None, TP),
        P(SP, TP, None),
        P(SP, TP),
        P(SP, TP, None),
        P(SP, TP, None),
        P(SP, TP, None),
        P(SP, TP, None),
    )
    return jax.shard_map(
        on_device, mesh=torus, in_specs=in_specs, out_specs=out_specs, check_vma=False
    )
```

```python
from functools import partial

import jax
import jax.numpy as jnp
from jax import lax
from jax.experimental import pallas as pl
from jax.experimental.pallas import tpu as pltpu
from jax.sharding import Mesh
from jax.sharding import PartitionSpec as P

SP = ("z", "x")
TP = ("y", "c")
BF = jnp.bfloat16
F32 = jnp.float32
HI = lax.Precision.HIGHEST
BLOCK = 32
LIMIT = 56 * 1024 * 1024
SMALL = 20 * 1024 * 1024
LEAN = ('first', 'deltas', 'partials', 'sums', 'collect', 'head', 'local', 'group', 'last')
TILES = 2


def dot(a, b, precision=None):
    return lax.dot_general(
        a, b, (((1,), (0,)), ((), ())), precision=precision, preferred_element_type=F32
    )


def dot_nt(a, b, precision=None):
    return lax.dot_general(
        a, b, (((1,), (1,)), ((), ())), precision=precision, preferred_element_type=F32
    )


def dot_tn(a, b, precision=None):
    return lax.dot_general(
        a, b, (((0,), (0,)), ((), ())), precision=precision, preferred_element_type=F32
    )


def iota(shape, dim):
    return lax.broadcasted_iota(jnp.int32, shape, dim)


class Place:
    def __init__(self, number, sizes):
        self.number, self.sizes = number, sizes

    def __getitem__(self, k):
        step, count = self.sizes[k]
        return lax.shift_right_logical(self.number[0], step.bit_length() - 1) & (count - 1)


def call(
    kernel, name, outs, scalars, *args, blocks=None, out_blocks=None, scratch=(), after=(), grid=1
):
    blocks = blocks or {}
    out_blocks = out_blocks or {}
    specs = []
    used, waits = len(args), len(after)

    def body(number, *refs):
        kernel(Place(number, scalars.sizes), *refs[:used], *refs[used + waits :])

    def placed(index):
        return lambda i, s: index(i, Place(s, scalars.sizes))

    for n, a in enumerate(args):
        if n in blocks:
            specs.append(pl.BlockSpec(blocks[n][0], placed(blocks[n][1])))
        else:
            specs.append(pl.BlockSpec(a.shape, lambda i, s, nd=a.ndim: (0,) * nd))
    specs += [pl.BlockSpec(memory_space=pl.ANY)] * waits
    out_specs = tuple(
        pl.BlockSpec(out_blocks[n][0], placed(out_blocks[n][1]))
        if n in out_blocks
        else pl.BlockSpec(o.shape, lambda i, s, nd=len(o.shape): (0,) * nd)
        for n, o in enumerate(outs)
    )
    return pl.pallas_call(
        body,
        name=name,
        out_shape=outs,
        grid_spec=pltpu.PrefetchScalarGridSpec(
            num_scalar_prefetch=1,
            grid=(grid,),
            in_specs=specs,
            out_specs=out_specs,
            scratch_shapes=list(scratch),
        ),
        compiler_params=pltpu.CompilerParams(
            vmem_limit_bytes=(SMALL if name in LEAN else LIMIT)
        ),
    )(scalars.number, *args, *after)


def sds(shape, dtype):
    return jax.ShapeDtypeStruct(shape, dtype)


def slots_of(routes):
    tokens = routes.shape[1]
    experts = iota((16, tokens), 0)
    r0, r1 = routes[0:1, :], routes[1:2, :]
    one0, one1 = r0 == experts, r1 == experts
    both = jnp.where(one0 | one1, 1.0, 0.0).astype(BF)
    earlier = jnp.where(iota((tokens, tokens), 0) < iota((tokens, tokens), 1), 1.0, 0.0).astype(BF)
    count = dot(both, earlier)
    s0 = jnp.sum(jnp.where(one0, count, 0.0), axis=0, keepdims=True)
    s1 = jnp.sum(jnp.where(one1, count, 0.0), axis=0, keepdims=True)
    return r0.astype(F32), r1.astype(F32), s0, s1


def column(row):
    return jnp.broadcast_to(row, (row.shape[1], row.shape[1])).T


def dispatch_kernel(at, routes_ref, weight_ref, x_ref, y_ref, out_ref):
    tokens = routes_ref.shape[1]
    r0, r1, s0, s1 = slots_of(routes_ref[...])
    key0 = r0 * 32.0 + s0
    key1 = r1 * 32.0 + s1
    w = weight_ref[...]
    w0, w1 = column(w[0:1])[:, 0:1], column(w[1:2])[:, 0:1]
    q = iota((40, tokens), 0)
    is_input = q < 20
    slot = jnp.where(is_input, q, jnp.where(q < 24, q - 4, q - 24)).astype(F32)
    experts = out_ref.shape[0] // 2
    picks = []
    for e in range(experts):
        key = slot + 32.0 * e
        m0, m1 = key0 == key, key1 == key
        picks.append(
            jnp.concatenate(
                [
                    jnp.where(is_input & (m0 | m1), 1.0, 0.0),
                    jnp.where(is_input, 0.0, jnp.where(m0, 1.0, 0.0)),
                    jnp.where(is_input, 0.0, jnp.where(m1, 1.0, 0.0)),
                ],
                axis=1,
            )
        )
    pick = jnp.concatenate(picks, axis=0).astype(BF)
    for f in range(0, out_ref.shape[2], 256):
        wide = slice(f, min(f + 256, out_ref.shape[2]))
        y = y_ref[:, wide].astype(F32)
        table = jnp.concatenate([x_ref[:, wide], (w0 * y).astype(BF), (w1 * y).astype(BF)], axis=0)
        rows = dot(pick, table)
        for e in range(experts):
            block = rows[40 * e : 40 * e + 40].astype(BF)
            out_ref[2 * e, :, wide] = block
            out_ref[2 * e + 1, :, wide] = block


def swap_halves(a):
    return jnp.concatenate([a[4:8], a[0:4]], axis=0)


def part_at(at, n):
    core = at[1] if n < 2 else 1 - at[1]
    return 2 * core + (at[5] if n % 2 == 0 else 1 - at[5])


def layout_kernel(at, wg_ref, wu_ref, wd_ref, woth_ref, side_ref, back_ref):
    part = side_ref.shape[0] // 4
    for n in range(4):
        first = pl.multiple_of(part_at(at, n) * part, 128)
        to = slice(n * part, (n + 1) * part)
        side_ref[to, 0:128] = wg_ref[0, pl.ds(first, part), :]
        side_ref[to, 128:256] = wu_ref[0, pl.ds(first, part), :]
        side_ref[to, 256:384] = wd_ref[0, :, pl.ds(first, part)].astype(F32).T.astype(BF)
    for y in range(back_ref.shape[1] // 128):
        first = pl.multiple_of((2 * y + at[1]) * 128, 128)
        for n, w in enumerate(
            (
                wg_ref[0, pl.ds(first, 128), :],
                wu_ref[0, pl.ds(first, 128), :],
                woth_ref[0, y],
                woth_ref[1, y],
            )
        ):
            back_ref[128 * n : 128 * n + 128, 128 * y : 128 * y + 128] = w.astype(F32).T.astype(BF)


def first_kernel(at, g_ref, w_ref, out_ref):
    out_ref[...] = dot(g_ref[...], w_ref[...])


def delta_kernel(at, other_ref, rest_ref, beside_ref, w_ref, acc_ref, delta_ref, pack_ref):
    part = rest_ref.shape[1]
    sums = acc_ref[...] + dot(rest_ref[...], w_ref[part : 2 * part, :])
    sums = sums + dot(other_ref[...], w_ref[2 * part : 3 * part, :])
    sums = sums + dot(beside_ref[...], w_ref[3 * part : 4 * part, :])
    gu, yh = sums[:, 0:256], sums[:, 256:384]
    low = iota((8, 128), 0) < 4
    zero8 = jnp.zeros((8, 128), F32)
    dgs, dus, dhs, pgs, pus = [], [], [], [], []
    mixed = []
    spans = rest_ref.shape[0] // 40
    for d in range(spans):
        b = 40 * d
        pg, pu = gu[b : b + 24, 0:128], gu[b : b + 24, 128:256]
        hg = jnp.concatenate([yh[b + 24 : b + 40], swap_halves(yh[b + 16 : b + 24])], axis=0)
        s = jax.nn.sigmoid(pg)
        act = pg * s
        hid = act * pu
        gd = hg * pu * s * (1.0 + pg * (1.0 - s))
        ud = hg * act
        dgs += [gd[0:16], jnp.where(low, gd[16:24], 0.0), zero8, zero8]
        dus += [ud[0:16], jnp.where(low, ud[16:24], 0.0), zero8, zero8]
        dhs += [zero8, zero8, jnp.where(low, 0.0, swap_halves(hid[16:24])), hid[0:16]]
        mixed.append((gd, ud))
    for d in range(0, spans, 2):
        for n, parts in ((0, pgs), (1, pus)):
            even, odd = mixed[d][n], mixed[d + 1][n]
            parts += [
                even[0:16],
                jnp.where(low, even[16:24], swap_halves(odd[16:24])),
                odd[0:16],
            ]
    delta_ref[:, 0:128] = jnp.concatenate(dgs, axis=0).astype(BF)
    delta_ref[:, 128:256] = jnp.concatenate(dus, axis=0).astype(BF)
    delta_ref[:, 256:384] = jnp.concatenate(dhs, axis=0).astype(BF)
    pack_ref[:, 0:128] = jnp.concatenate(pgs, axis=0).astype(BF)
    pack_ref[:, 128:256] = jnp.concatenate(pus, axis=0).astype(BF)


def partial_kernel(at, pack_ref, back_ref, out_ref):
    core = at[1]
    nz, ny, rows, _ = out_ref.shape
    lhs = jnp.concatenate([pack_ref[core], pack_ref[1 - core]], axis=1)
    for y in range(0, ny, 2):
        o = dot(lhs, back_ref[:, 128 * y : 128 * y + 256]).astype(BF)
        for z in range(nz):
            out_ref[z, y] = o[z * rows : (z + 1) * rows, 0:128]
            out_ref[z, y + 1] = o[z * rows : (z + 1) * rows, 128:256]


def weight_kernel(at, delta_ref, a_ref, b_ref, c_ref, d_ref, gate_ref, up_ref, down_ref, dt_ref):
    rows, part = a_ref.shape
    for r in range(0, rows, 128):
        dt_ref[:, r : r + 128] = delta_ref[r : r + 128, :].astype(F32).T.astype(BF)
    for n, g_ref in enumerate((a_ref, b_ref, c_ref, d_ref)):
        wide = min(256, part)
        for p in range(0, part, wide):
            o = dot(dt_ref[...], g_ref[:, p : p + wide])
            first = pl.multiple_of(part_at(at, n) * part + p, 128)
            gate_ref[0, pl.ds(first, wide), :] = o[0:128].T.astype(BF)
            up_ref[0, pl.ds(first, wide), :] = o[128:256].T.astype(BF)
            down_ref[0, :, pl.ds(first, wide)] = o[256:384].astype(BF)


def sum_kernel(at, got_ref, out_ref):
    nz, ny, _, _ = got_ref.shape
    for z in range(nz):
        total = got_ref[z, 0].astype(F32)
        for y in range(1, ny):
            total = total + got_ref[z, y].astype(F32)
        for p in range(out_ref.shape[0] // 2):
            b = 40 * p
            out_ref[2 * p, z] = total[b : b + 24].astype(BF)
            out_ref[2 * p + 1, z] = jnp.concatenate(
                [total[b + 24 : b + 40], total[b + 16 : b + 24]], axis=0
            ).astype(BF)


def collect_kernel(at, routes_ref, got_ref, cot_ref, out_ref):
    nx, nz, _, _ = got_ref.shape
    routes = routes_ref[...]
    _, _, s0, s1 = slots_of(routes)
    shift = (at[4] % 2).astype(F32) * 4.0
    cols = nx * nz * 24
    lanes = iota((routes.shape[1], cols), 1).astype(F32)
    hit = None
    for n, s in ((0, s0), (1, s1)):
        half = routes[n : n + 1, :] * 2
        block = (half % nx) * nz + half // nx
        row = block.astype(F32) * 24.0 + s + jnp.where(s >= 16.0, shift, 0.0)
        first = column(row)[:, 0:1]
        match = (lanes == first) | (lanes == first + 24.0 * nz)
        hit = match if hit is None else hit | match
    pick = jnp.where(hit, 1.0, 0.0).astype(BF)
    table = got_ref[...].astype(F32).reshape(cols, 128).astype(BF)
    out_ref[...] = (cot_ref[...].astype(F32) + dot(pick, table)).astype(BF)


def block_of(shape):
    return iota(shape, 1) // BLOCK


def mids_of(gc):
    return [gc[:, b + BLOCK // 2 - 1 : b + BLOCK // 2] for b in range(0, gc.shape[1], BLOCK)]


def growth(gc):
    blocks = block_of(gc.shape)
    mid = jnp.zeros(gc.shape, F32)
    for n, m in enumerate(mids_of(gc)):
        mid = jnp.where(blocks == n, m, mid)
    return jnp.exp(gc - mid)


def causal(tokens):
    return iota((tokens, tokens), 1) <= iota((tokens, tokens), 0)


def in_parts(rows):
    high = rows.astype(BF)
    rest = rows - high.astype(F32)
    mid = rest.astype(BF)
    low = (rest - mid.astype(F32)).astype(BF)
    n = iota(rows.shape, 0)
    parts = jnp.where(n == 0, high.astype(F32), jnp.where(n == 1, mid.astype(F32), low.astype(F32)))
    return jnp.where(n < 3, parts, 0.0).astype(BF)


def columns(rows):
    rows = rows + [jnp.zeros((128 - len(rows), 128), F32)]
    return jnp.concatenate(rows, axis=0).T


def forward_kernel(at, q_ref, k_ref, v_ref, g_ref, s_ref, mixed_ref, p_ref, last_ref, gc_ref, tot_ref):
    width, tokens = q_ref.shape
    g = g_ref[...]
    before = jnp.where(iota((tokens, tokens), 0) <= iota((tokens, tokens), 1), 1.0, 0.0)
    gc = dot(g, before, HI)
    gc_ref[...] = gc
    q = q_ref[...].astype(F32) * (width**-0.5)
    k = k_ref[...].astype(F32)
    v = v_ref[...].astype(F32)
    s0 = s_ref[0, 0]
    qt = q * growth(gc)
    parts = []
    for n, mid in enumerate(mids_of(gc)):
        whole = dot_tn(qt, k * jnp.exp(jnp.minimum(mid - gc, 40.0)), HI)
        parts.append(whole[n * BLOCK : (n + 1) * BLOCK])
    p = jnp.where(causal(tokens), jnp.concatenate(parts, axis=0), 0.0)
    p_ref[...] = p.astype(BF)
    mixed_ref[...] = (dot_tn(q * jnp.exp(gc), s0, HI) + dot(p, v, HI)).astype(BF)
    end = gc[:, tokens - 1 : tokens]
    last_ref[...] = jnp.exp(end) * s0 + dot(k * jnp.exp(end - gc), v, HI)
    row = dot_nt(jnp.ones((8, tokens), F32), g, HI)
    row = jnp.concatenate([row, jnp.zeros((8, 128 - width), F32)], axis=1)
    tot_ref[...] = in_parts(row)


def head_kernel(piece, at, tg_ref, w_ref, q_ref, gc_ref, mixed_ref, tot_ref, rows_ref, send_ref):
    slices = tg_ref.shape[0]
    width = q_ref.shape[0]
    nx = send_ref.shape[0]
    tg = jnp.concatenate([tg_ref[t] for t in range(slices)], axis=1)
    rows = dot(tg, w_ref[...]).astype(BF)
    rows_ref[...] = rows
    qe = q_ref[...].astype(F32) * (width**-0.5) * jnp.exp(gc_ref[...])
    carry = dot(qe, rows.astype(F32), HI).astype(BF)
    own = send_ref.shape[1] - width - 8
    for n in range(nx):
        send_ref[n, own : own + width, :] = carry
        send_ref[n, own + width : own + width + 8, :] = tot_ref[...]
    mixed = mixed_ref[...]
    for t in range(slices):
        o = dot_tn(tg_ref[t], mixed).astype(BF)
        for r in range(0, 128, piece):
            d = (t * 128 + r) // piece
            send_ref[d % nx, (d // nx) * piece : (d // nx + 1) * piece, :] = o[r : r + piece]


def local_kernel(at, rows_ref, q_ref, k_ref, v_ref, gc_ref, s_ref, p_ref, qraw_ref, qq_ref, kl_ref, vl_ref):
    width, tokens = q_ref.shape
    scale = width**-0.5
    rows = rows_ref[...]
    gc = gc_ref[...]
    q = q_ref[...].astype(F32)
    k = k_ref[...].astype(F32)
    a = jnp.where(causal(tokens), dot_nt(rows, v_ref[...]), 0.0)
    grow = growth(gc)
    qt = q * scale * grow
    blocks = block_of(gc.shape)
    inner = jnp.zeros((width, tokens), F32)
    key_local = jnp.zeros((width, tokens), F32)
    for n, mid in enumerate(mids_of(gc)):
        fall = jnp.exp(jnp.minimum(mid - gc, 40.0))
        inner = jnp.where(blocks == n, dot_nt(k * fall, a, HI), inner)
        key_local = key_local + fall * dot(jnp.where(blocks == n, qt, 0.0), a, HI)
    qraw = scale * (jnp.exp(gc) * dot_nt(s_ref[0, 0], rows.astype(F32), HI) + grow * inner)
    qraw_ref[...] = qraw.astype(BF)
    qq_ref[...] = q * qraw
    kl_ref[...] = key_local
    vl_ref[...] = dot_tn(p_ref[...], rows)


def group_kernel(at, got_ref, inside_ref, after_ref, send_ref, token_ref):
    token_ref[...] = jnp.zeros(token_ref.shape, F32)
    nx, rows, _ = got_ref.shape
    nz = send_ref.shape[0]
    width = inside_ref.shape[0]
    own = rows - width - 8
    piece = own // nz
    x = at[4]
    zero = jnp.zeros((1, 128), F32)
    before, later = zero, zero
    weights, wholes = [], []
    for i in range(nx):
        weights.append(jnp.where(x < i, jnp.exp(later), 0.0))
        wholes.append(jnp.exp(before))
        part = got_ref[i, own + width : own + width + 8, :].astype(F32)
        total = jnp.sum(part, axis=0, keepdims=True)
        before = before + total
        later = later + jnp.where(x < i, total, 0.0)
    after_ref[...] = jnp.broadcast_to(later, (8, 128))
    cols = columns(weights + wholes)
    inside = jnp.zeros((width, 128), F32)
    whole = jnp.zeros((width, 128), F32)
    for i in range(nx):
        part = got_ref[i, own : own + width, :].astype(F32)
        inside = inside + cols[0:width, i : i + 1] * part
        whole = whole + cols[0:width, nx + i : nx + i + 1] * part
    inside_ref[...] = inside
    whole = whole.astype(BF)
    parts = in_parts(jnp.broadcast_to(before, (8, 128)))
    for i in range(nz):
        total = got_ref[0, i * piece : (i + 1) * piece, :].astype(F32)
        for j in range(1, nx):
            total = total + got_ref[j, i * piece : (i + 1) * piece, :].astype(F32)
        send_ref[i, 0:piece, :] = total.astype(BF)
        send_ref[i, piece : piece + width, :] = whole
        send_ref[i, piece + width : piece + width + 8, :] = parts


def last_kernel(at, got_ref, inside_ref, after_ref, k_ref, v_ref, gc_ref, last_ref, qq_ref, kl_ref, vl_ref, og_ref, key_ref, value_ref, decay_ref):
    width, tokens = k_ref.shape
    piece = og_ref.shape[0]
    z = at[3]
    sums = after_ref[0:1, :]
    weights = []
    for i in range(got_ref.shape[0]):
        weights.append(jnp.where(z < i, jnp.exp(sums), 0.0))
        part = got_ref[i, piece + width : piece + width + 8, :].astype(F32)
        sums = sums + jnp.where(z < i, jnp.sum(part, axis=0, keepdims=True), 0.0)
    cols = columns(weights)
    incoming = inside_ref[...]
    total = jnp.zeros((piece, 128), F32)
    for i in range(got_ref.shape[0]):
        total = total + got_ref[i, 0:piece, :].astype(F32)
        part = got_ref[i, piece : piece + width, :].astype(F32)
        incoming = incoming + cols[0:width, i : i + 1] * part
    og_ref[...] = total
    gc = gc_ref[...]
    k = k_ref[...].astype(F32)
    rest = jnp.exp(gc[:, tokens - 1 : tokens] - gc)
    key = kl_ref[...] + rest * dot_nt(incoming, v_ref[...].astype(F32), HI)
    key_ref[...] = key.astype(BF)
    value_ref[...] = (vl_ref[...] + dot_tn(k * rest, incoming, HI)).astype(BF)
    later = jnp.where(causal(tokens), 1.0, 0.0)
    cross = jnp.sum(last_ref[...] * incoming, axis=1, keepdims=True)
    decay_ref[...] = dot(qq_ref[...] - k * key, later, HI) + cross


def on_device(
    expert_input,
    cotangent,
    routes,
    route_weight,
    gate_weight,
    up_weight,
    down_weight,
    out_weight,
    queries,
    key_vectors,
    value_rows,
    log_decay,
    start_state,
):
    tokens = expert_input.shape[0]
    nz, nx, ny = lax.axis_size("z"), lax.axis_size("x"), lax.axis_size("y")
    spans = nz * nx
    slices = ny * 2
    core = lax.axis_index("c")
    place = lax.axis_index(("z", "x", "y", "c")).astype(jnp.int32)
    sizes = ((1, slices), (1, 2), (slices, spans), (slices * nx, nz), (slices, nx), (2, 2))
    at = Place(place.reshape(1), sizes)
    width = queries.shape[2]
    piece_rows = slices * 128 // spans
    routes = routes.T
    route_weight = route_weight.T
    q = queries.reshape(tokens, width).T
    k = key_vectors.reshape(tokens, width).T
    v = value_rows.reshape(tokens, 128)
    g = log_decay.reshape(tokens, width).T
    slice_block = ((tokens, 128), lambda i, s: (0, s[0]))
    half = slices * 64
    part = half // 2
    part_block = ((tokens, part), lambda i, s: (0, part_at(s, 0)))

    (sent,) = call(
        dispatch_kernel,
        "dispatch",
        (sds((spans, 40, part), BF),),
        at,
        routes,
        route_weight,
        expert_input,
        cotangent,
        blocks={2: part_block, 3: part_block},
    )
    own = lax.all_to_all(sent, SP, 0, 0, tiled=True).reshape(spans * 40, part)

    weights = jnp.stack([gate_weight[0], up_weight[0]]).reshape(2, ny, 2, 128, 128)
    weights = lax.dynamic_index_in_dim(weights, 1 - core, 2, keepdims=False)
    weights = lax.ppermute(weights, "c", [(0, 1), (1, 0)])
    mixed, p, last, gc, totals = call(
        forward_kernel,
        "forward",
        (
            sds((tokens, 128), BF),
            sds((tokens, tokens), BF),
            sds((width, 128), F32),
            sds((width, tokens), F32),
            sds((8, 128), BF),
        ),
        at,
        q,
        k,
        v,
        g,
        start_state,
        after=(sent,),
    )
    side, back = call(
        layout_kernel,
        "layout",
        (sds((slices * 128, 384), BF), sds((512, half), BF)),
        at,
        gate_weight,
        up_weight,
        down_weight,
        weights,
        after=(mixed,),
    )
    own, mixed, side = lax.optimization_barrier((own, mixed, side))

    rows_all = spans * 40
    swap = [(0, 1), (1, 0)]
    up = [(i, (i + 1) % ny) for i in range(ny)]
    down = [(i, (i - 1) % ny) for i in range(ny)]
    low = lax.ppermute(own[: rows_all // 2], "y", up)
    high = lax.ppermute(own[rows_all // 2 :], "y", down)
    other = lax.ppermute(own, "c", swap)
    tile = rows_all // TILES
    part_rows = ((tile, part), lambda i, s: (i, 0))
    acc_block = ((tile, 384), lambda i, s: (i, 0))
    (acc,) = call(
        first_kernel,
        "first",
        (sds((rows_all, 384), F32),),
        at,
        own,
        side,
        blocks={0: part_rows, 1: ((part, 384), lambda i, s: (0, 0))},
        out_blocks={0: acc_block},
        grid=TILES,
    )
    low, acc, other = lax.optimization_barrier((low, acc, other))
    beside = jnp.concatenate([lax.ppermute(low, "c", swap), lax.ppermute(high, "c", swap)], axis=0)
    rest = jnp.concatenate([low, high], axis=0)
    delta, pack = call(
        delta_kernel,
        "deltas",
        (sds((rows_all, 384), BF), sds((rows_all // 2, 256), BF)),
        at,
        other,
        rest,
        beside,
        side,
        acc,
        blocks={0: part_rows, 1: part_rows, 2: part_rows, 4: acc_block},
        out_blocks={0: acc_block, 1: ((tile // 2, 256), lambda i, s: (i, 0))},
        grid=TILES,
    )
    packs = lax.all_gather(pack, "c", axis=0)
    (terms,) = call(
        partial_kernel,
        "partials",
        (sds((nz, ny, nx * 20, 128), BF),),
        at,
        packs,
        back,
    )
    got = lax.all_to_all(
        terms.reshape(nz * ny, nx * 20, 128), ("z", "y"), 0, 0, tiled=True
    ).reshape(nz, ny, nx * 20, 128)
    (summed,) = call(sum_kernel, "sums", (sds((nx, nz, 24, 128), BF),), at, got)
    returned = lax.all_to_all(summed.reshape(nx, nz * 24, 128), "x", 0, 0, tiled=True)
    (slice_grad,) = call(
        collect_kernel,
        "collect",
        (sds((tokens, 128), BF),),
        at,
        routes,
        returned.reshape(nx, nz, 24, 128),
        cotangent,
        blocks={2: slice_block},
    )
    total_grad = lax.all_gather(slice_grad, TP, axis=0)

    rows, leaving = call(
        partial(head_kernel, piece_rows),
        "head",
        (sds((tokens, 128), BF), sds((nx, nz * piece_rows + width + 8, 128), BF)),
        at,
        total_grad,
        out_weight,
        q,
        gc,
        mixed,
        totals,
    )
    crossing = lax.all_to_all(leaving, "x", 0, 0, tiled=True)
    inside, later, group, token = call(
        group_kernel,
        "group",
        (
            sds((width, 128), F32),
            sds((8, 128), F32),
            sds((nz, piece_rows + width + 8, 128), BF),
            sds((8, 128), F32),
        ),
        at,
        crossing,
    )
    group = lax.all_to_all(group, "z", 0, 0, tiled=True)
    gate_grad, up_grad, down_grad = call(
        weight_kernel,
        "weights",
        (
            sds((1, slices * 128, 128), BF),
            sds((1, slices * 128, 128), BF),
            sds((1, 128, slices * 128), BF),
        ),
        at,
        delta,
        own,
        rest,
        other,
        beside,
        scratch=[pltpu.VMEM((384, spans * 40), BF)],
        after=(token,),
    )
    qraw, qq, key_local, value_local = call(
        local_kernel,
        "local",
        (
            sds((width, tokens), BF),
            sds((width, tokens), F32),
            sds((width, tokens), F32),
            sds((tokens, 128), F32),
        ),
        at,
        rows,
        q,
        k,
        v,
        gc,
        start_state,
        p,
        after=(token,),
    )
    out_grad, key, value, decay = call(
        last_kernel,
        "last",
        (
            sds((piece_rows, 128), F32),
            sds((width, tokens), BF),
            sds((tokens, 128), BF),
            sds((width, tokens), F32),
        ),
        at,
        group,
        inside,
        later,
        k,
        v,
        gc,
        last,
        qq,
        key_local,
        value_local,
    )
    return (
        gate_grad,
        up_grad,
        down_grad,
        out_grad,
        qraw.T[:, None, :],
        key.T[:, None, :],
        value[:, None, :],
        decay.T[:, None, :],
    )


def solution(mesh):
    torus = Mesh(mesh.devices.reshape(8, 4, mesh.shape["tp"] // 2, 2), ("z", "x", "y", "c"))
    in_specs = (
        P(SP, None),
        P(SP, None),
        P(SP, None),
        P(SP, None),
        P(SP, None, TP),
        P(SP, None, TP),
        P(SP, TP, None),
        P(None, TP),
        P(SP, TP, None),
        P(SP, TP, None),
        P(SP, TP, None),
        P(SP, TP, None),
        P(SP, TP, None, None),
    )
    out_specs = (
        P(SP, None, TP),
        P(SP, None, TP),
        P(SP, TP, None),
        P(SP, TP),
        P(SP, TP, None),
        P(SP, TP, None),
        P(SP, TP, None),
        P(SP, TP, None),
    )
    return jax.shard_map(
        on_device, mesh=torus, in_specs=in_specs, out_specs=out_specs, check_vma=False
    )
```
